256 devices in a mesh: grp: 2 (over y), sp: 32 (over z, core), tp: 4 (over x).
Axes of the slice: x: 4, y: 2, z: 16, core: 2. Of those that a mesh axis runs over, the one named last changes fastest.
The devices are a block of a 4x16x16 slice.
Arguments:
- query_plain: bfloat16 [10240, 1024], P(('grp', 'sp'), 'tp'), parts along dimension 0, may hold values from -6 to 6
- query_turn: bfloat16 [10240, 512], P(('grp', 'sp'), 'tp'), parts along dimension 0, may hold values from -40 to 40, as said below
- latent: bfloat16 [10240, 512], P(('grp', 'sp')), parts along dimension 0, may hold values from -6 to 6
- key_turn: bfloat16 [10240, 64], P(('grp', 'sp')), parts along dimension 0, may hold values from -40 to 40, as said below
- latent_norm_scale: bfloat16 [512], replicated, may hold values from 0.099609375 to 1.8984375
- plain_key_matrix: bfloat16 [512, 1024], P(None, 'tp'), may hold values from -0.25 to 0.25
- value_matrix: bfloat16 [512, 1024], P(None, 'tp'), may hold values from -0.25 to 0.25
- residual: bfloat16 [10240, 2048], P(('grp', 'sp', 'tp')), parts along dimension 0, may hold values from -6 to 6
- out_weight: bfloat16 [1024, 2048], replicated, may hold values from -6 to 6
- ffn_gain: bfloat16 [2048], replicated, may hold values from 0.099609375 to 1.8984375
- gate_weight: bfloat16 [32, 2048, 1024], P('sp', None, 'tp'), may hold values from -1 to 1
- up_weight: bfloat16 [32, 2048, 1024], P('sp', None, 'tp'), may hold values from -1 to 1
- down_weight: bfloat16 [32, 1024, 2048], P('sp', 'tp'), may hold values from -0.0625 to 0.0625
- routes: int32 [10240, 4], P(('grp', 'sp', 'tp')), parts along dimension 0, may hold values from 0 to 31, all different within a row; in each aligned block of 40 rows (0 to 39, 40 to 79, ...) at most 7 rows name the same one
- route_weights: float32 [10240, 4], P(('grp', 'sp', 'tp')), parts along dimension 0, may hold values from 0.1 to 0.6
Outputs:
- mixed: bfloat16 [10240, 2048], P(('grp', 'sp', 'tp')), parts along dimension 0
The draws below stay inside these ranges and needn't reach their ends.
There are 2 independent parts, one for each index of `grp`. The reference program is written for one: setup_inputs(seed, part) draws one part's arguments, and reference() takes and returns one part's arrays. A program takes and returns all parts, laid end to end along the dimension named above; an argument that names none is the same for every part. Nothing has to cross between parts.
Inputs may be any that keep to these rules, and one draw needn't show every extreme that they name: `query_turn`: in the hidden draw some rows are large. `key_turn`: in the hidden draw some rows are large. `routes`: each row names 4 different experts. In each aligned block of 40 rows (the rows of one device) no expert is named more than 7 times, a bound that some block reaches.
All inputs are finite; a program needn't handle non-finite values.
Results may differ from the reference program's by a relative error of at most 0.015.
Values may be sent and summed in bfloat16 or wider, within the bound.
No kernel may reach another device: no remote copies, remote signals or barrier semaphores. Data moves between devices by JAX's collectives and lax.ppermute only.
A program may use at most 128 MiB of HBM per device.

```python
import math
import jax
import jax.numpy as jnp
import numpy as np
from jax import lax

D = 2048
ATTENTION_HEADS = 8
PLAIN_HEAD_WIDTH = 128
QK_ROPE = 64
VALUE_WIDTH = 128
LATENT_WIDTH = 512
D_EXPERT = 1024
TOP = 4
GRID_W = 64
ROWS_DEV = 40
SEQUENCE_TOKENS = 5120
EXPERTS = 32
CAP = 7
N_SP = 32
N_TP = 4


def draw_query_turn(key, part):
    base = jnp.clip(jax.random.normal(jax.random.fold_in(key, 1), (SEQUENCE_TOKENS, ATTENTION_HEADS * QK_ROPE), jnp.float32), -6.0, 6.0)
    return base.astype(jnp.bfloat16)


def draw_key_turn(key, part):
    base = jnp.clip(jax.random.normal(jax.random.fold_in(key, 2), (SEQUENCE_TOKENS, QK_ROPE), jnp.float32), -6.0, 6.0)
    return base.astype(jnp.bfloat16)


def block_scale(own_key, extent, cuts, least, high):
    loudness, own = 1.0, jax.random.fold_in(own_key, 6)
    for dim, shards_of in cuts:
        steps = jnp.exp(jax.random.uniform(jax.random.fold_in(own, dim), (shards_of,), jnp.float32, least / len(cuts), high / len(cuts)))
        loudness = loudness * jnp.repeat(steps, extent[dim] // shards_of).reshape([-1 if axis == dim else 1 for axis in range(len(extent))])
    return loudness


def shared_out(stream_key, own, number, rows, count, top, reach, skew):
    ranking = jax.random.permutation(stream_key, count)
    crowded, common = shares(count, rows * top, reach, skew, True), shares(count, rows * top, reach, skew, False)
    places = jnp.arange(count)

    def named(sizes, offset_by):
        used = int((sizes > 0).sum())
        fixed = max(1, used // 4)
        passed = fixed + (places - fixed + offset_by * (used - fixed)) % max(1, count - fixed)
        return jnp.zeros((count,), jnp.int32).at[ranking[jnp.where(places < fixed, places, passed)]].set(jnp.asarray(sizes, jnp.int32))

    sizes = jnp.where(number % 4 == 0, named(crowded, number // 4), named(common, number - number // 4 - 1))
    mixed = jax.random.permutation(jax.random.fold_in(own, 3), count)
    source_of, sink = mixed[0:count // 2 * 2:2], mixed[1:count // 2 * 2:2]
    slack = jnp.minimum(sizes[source_of] - 1, reach - sizes[sink]) // 2
    slack = jnp.where((source_of == ranking[0]) | (sink == ranking[0]) | (sizes[sink] == 0), 0, jnp.maximum(slack, 0))
    passed = jax.random.randint(jax.random.fold_in(own, 4), (count // 2,), 0, 1 << 20) % (slack + 1)
    sizes = sizes.at[source_of].add(-passed).at[sink].add(passed)
    members = jnp.searchsorted(jnp.cumsum(sizes), jnp.arange(rows * top), side="right").astype(jnp.int32)
    grid = members.reshape(top, rows).T
    grid = grid[jax.random.permutation(jax.random.fold_in(own, 1), rows)]
    offset_by = jax.random.randint(jax.random.fold_in(own, 2), (rows, 1), 0, top)
    return jnp.take_along_axis(grid, (jnp.arange(top)[None, :] + offset_by) % top, axis=1)


def shares(count, total, most, lean, full):
    loads = [(1 << 20) // math.isqrt(standing ** lean) + 1 for standing in range(1, count + 1)]
    largest = most if full else min(most, max(-(-total // count), total * loads[0] // sum(loads)))
    least = 1 if total - largest >= count - 1 else 0
    given, surplus = [largest] + [least] * (count - 1), total - largest - least * (count - 1)
    while surplus > 0:
        candidates = [i for i in range(1, count) if given[i] < largest] or [i for i in range(1, count) if given[i] < most]
        whole, budget = sum([loads[i] for i in candidates]), surplus
        for i in candidates:
            more = min(most - given[i], max(1, budget * loads[i] // whole), surplus)
            given[i] = given[i] + more
            surplus = surplus - more
    return np.array(given)


def scatter_about(own_key, dims, scale, bound, shards=(), kind=jnp.bfloat16):
    drawn = jax.random.normal(own_key, dims, jnp.float32) * scale
    if len(shards) > 0:
        drawn = block_scale(own_key, dims, shards, -0.22, 0.18) * drawn
    return jnp.clip(drawn, min=-bound, max=bound).astype(kind)


def setup_inputs(seed: int = 0, part: int = 0) -> dict:
    arg_keys = jax.random.split(jax.random.key(seed), 16)
    part_keys = jax.random.split(jax.random.fold_in(arg_keys[15], part), 16)
    query_plain = scatter_about(part_keys[0], (SEQUENCE_TOKENS, ATTENTION_HEADS * PLAIN_HEAD_WIDTH), 1.0, 6.0, ((0, 32), (1, 4)))
    query_turn = draw_query_turn(jax.random.fold_in(jax.random.fold_in(arg_keys[15], part), 71), part)
    latent = scatter_about(part_keys[2], (SEQUENCE_TOKENS, LATENT_WIDTH), 1.0, 6.0, ((0, 32),))
    key_turn = draw_key_turn(jax.random.fold_in(jax.random.fold_in(arg_keys[15], part), 71), part)
    latent_norm_scale = jnp.clip(1.0 + 0.18 * jax.random.normal(arg_keys[4], (LATENT_WIDTH,), jnp.float32), 0.099609375, 1.8984375).astype(jnp.bfloat16)
    plain_key_matrix = scatter_about(arg_keys[5], (LATENT_WIDTH, ATTENTION_HEADS * PLAIN_HEAD_WIDTH), LATENT_WIDTH ** -0.5, 0.25, ((1, 4),))
    value_matrix = scatter_about(arg_keys[6], (LATENT_WIDTH, ATTENTION_HEADS * VALUE_WIDTH), LATENT_WIDTH ** -0.5, 0.25, ((1, 4),))
    residual = scatter_about(part_keys[7], (SEQUENCE_TOKENS, D), 1.0, 6.0, ((0, 128),))
    out_weight = scatter_about(arg_keys[8], (ATTENTION_HEADS * VALUE_WIDTH, D), (16 * (ATTENTION_HEADS * VALUE_WIDTH) ** -0.5), 6.0)
    ffn_gain = jnp.clip(1.0 + 0.18 * jax.random.normal(arg_keys[9], (D,), jnp.float32), 0.099609375, 1.8984375).astype(jnp.bfloat16)
    gate_weight = scatter_about(arg_keys[10], (EXPERTS, D, D_EXPERT), (3 * D ** -0.5), 1.0, ((0, 32), (2, 4)))
    up_weight = scatter_about(arg_keys[11], (EXPERTS, D, D_EXPERT), (3 * D ** -0.5), 1.0, ((0, 32), (2, 4)))
    down_weight = scatter_about(arg_keys[12], (EXPERTS, D_EXPERT, D), (0.15 * D_EXPERT ** -0.5), 0.0625, ((0, 32), (1, 4)))
    routes_keys = jax.random.split(jax.random.fold_in(part_keys[13], 1), SEQUENCE_TOKENS // ROWS_DEV)
    routes_turns = jax.random.permutation(jax.random.fold_in(part_keys[13], 3), SEQUENCE_TOKENS // ROWS_DEV)
    routes = jax.vmap(lambda own, number: shared_out(jax.random.fold_in(part_keys[13], 2), own, number, ROWS_DEV, EXPERTS, TOP, CAP, 1))(routes_keys, routes_turns).reshape((SEQUENCE_TOKENS, TOP))
    route_weights = jnp.clip(0.1 + 0.5 * jax.random.uniform(part_keys[14], (SEQUENCE_TOKENS, TOP), jnp.float32) ** block_scale(part_keys[14], (SEQUENCE_TOKENS, TOP), ((0, 128),), -0.2, 0.2), 0.1, 0.6)
    return dict(query_plain=query_plain, query_turn=query_turn, latent=latent, key_turn=key_turn, latent_norm_scale=latent_norm_scale, plain_key_matrix=plain_key_matrix, value_matrix=value_matrix, residual=residual, out_weight=out_weight, ffn_gain=ffn_gain, gate_weight=gate_weight, up_weight=up_weight, down_weight=down_weight, routes=routes, route_weights=route_weights)


theta = 10000.0
eps = 1e-06
limit = 7.0
slope = 1.702

def turn(vector, row_shift, col_shift):
    width = vector.shape[-1]
    count = width // 4
    half = width // 2
    freqs = theta ** (-jnp.arange(count, dtype=jnp.float32) / count)
    extra = (1,) * (vector.ndim - 2)
    pieces = []
    for portion, shift in ((vector[..., :half], row_shift), (vector[..., half:], col_shift)):
        angle = (shift.astype(jnp.float32)[:, None] * freqs[None, :]).reshape((shift.shape[0],) + extra + (count,))
        lower = portion[..., :count]
        upper = portion[..., count:]
        pieces.append(jnp.concatenate([lower * jnp.cos(angle) - upper * jnp.sin(angle), lower * jnp.sin(angle) + upper * jnp.cos(angle)], axis=-1))
    return jnp.concatenate(pieces, axis=-1)

def norm_scale(values, gain):
    wide = values.astype(jnp.float32)
    return wide * lax.rsqrt(lax.optimization_barrier(jnp.mean(wide * wide, axis=-1, keepdims=True)) + eps) * gain.astype(jnp.float32)

def expert_apply(operands):
    rows, gate_w, up_w, down_w = operands
    gate_pre = jnp.minimum(jnp.dot(rows, gate_w, preferred_element_type=jnp.float32), limit)
    up_pre = jnp.clip(jnp.dot(rows, up_w, preferred_element_type=jnp.float32), -limit, limit)
    active = ((up_pre + 1.0) * gate_pre * jax.nn.sigmoid(slope * gate_pre)).astype(jnp.bfloat16)
    piece = down_w.shape[0] // N_TP
    groups = jnp.einsum('rnp,npd->nrd', active.reshape(rows.shape[0], N_TP, piece).astype(jnp.float32), down_w.reshape(N_TP, piece, down_w.shape[1]).astype(jnp.float32))
    rounded = lax.optimization_barrier(groups.astype(jnp.bfloat16))
    return lax.optimization_barrier(jnp.sum(rounded.astype(jnp.float32), axis=0)).astype(jnp.bfloat16)

def reference(query_plain, query_turn, latent, key_turn, latent_norm_scale, plain_key_matrix, value_matrix, residual, out_weight, ffn_gain, gate_weight, up_weight, down_weight, routes, route_weights):
    place = jnp.arange(SEQUENCE_TOKENS, dtype=jnp.int32)
    grid_row = place // GRID_W
    grid_col = place % GRID_W
    normed_latent = norm_scale(latent, latent_norm_scale).astype(jnp.bfloat16)
    key_plain = jnp.dot(normed_latent, plain_key_matrix, preferred_element_type=jnp.float32).astype(jnp.bfloat16)
    values = jnp.dot(normed_latent, value_matrix, preferred_element_type=jnp.float32).astype(jnp.bfloat16)
    key_rot = turn(key_turn.astype(jnp.float32), grid_row, grid_col).astype(jnp.bfloat16)
    query_rot = turn(query_turn.astype(jnp.float32).reshape(SEQUENCE_TOKENS, ATTENTION_HEADS, QK_ROPE), grid_row, grid_col).astype(jnp.bfloat16)
    plain_heads = jnp.moveaxis(query_plain.reshape(SEQUENCE_TOKENS, ATTENTION_HEADS, PLAIN_HEAD_WIDTH), 1, 0)
    rot_heads = jnp.moveaxis(query_rot, 1, 0)
    key_heads = jnp.moveaxis(key_plain.reshape(SEQUENCE_TOKENS, ATTENTION_HEADS, PLAIN_HEAD_WIDTH), 1, 0)
    value_heads = jnp.moveaxis(values.reshape(SEQUENCE_TOKENS, ATTENTION_HEADS, VALUE_WIDTH), 1, 0)
    scale = (PLAIN_HEAD_WIDTH + QK_ROPE) ** (-0.5)
    block = math.gcd(SEQUENCE_TOKENS, 512)

    def one_head(operands):
        head_plain, head_rot, head_keys, head_values = operands

        def one_block(start):
            block_plain = lax.dynamic_slice_in_dim(head_plain, start, block, 0)
            block_rot = lax.dynamic_slice_in_dim(head_rot, start, block, 0)
            scores = (jnp.einsum('qd,kd->qk', block_plain, head_keys, preferred_element_type=jnp.float32) + jnp.einsum('qd,kd->qk', block_rot, key_rot, preferred_element_type=jnp.float32)) * scale
            peak = lax.optimization_barrier(jnp.max(scores, axis=1, keepdims=True))
            weights = jnp.exp(scores - peak)
            summed = jnp.dot(weights.astype(jnp.bfloat16), head_values, preferred_element_type=jnp.float32)
            return (summed / lax.optimization_barrier(jnp.sum(weights, axis=1, keepdims=True))).astype(jnp.bfloat16)
        starts = jnp.arange(SEQUENCE_TOKENS // block, dtype=jnp.int32) * block
        return lax.map(one_block, starts).reshape(SEQUENCE_TOKENS, VALUE_WIDTH)
    attended = lax.map(one_head, (plain_heads, rot_heads, key_heads, value_heads))
    attended = jnp.moveaxis(attended, 0, 1).reshape(SEQUENCE_TOKENS, ATTENTION_HEADS * VALUE_WIDTH)
    hidden = (residual.astype(jnp.float32) + jnp.dot(attended, out_weight, preferred_element_type=jnp.float32)).astype(jnp.bfloat16)
    normed = norm_scale(hidden, ffn_gain).astype(jnp.bfloat16)
    blocks = N_SP * N_TP
    per_block = routes.reshape(blocks, ROWS_DEV * TOP)
    marks = (per_block[..., None] == jnp.arange(EXPERTS, dtype=jnp.int32)).astype(jnp.int32)
    earlier = jnp.cumsum(marks, axis=1, dtype=jnp.int32) - marks
    slots = lax.optimization_barrier(jnp.sum(earlier * marks, axis=2, dtype=jnp.int32))
    target = ((per_block * blocks + jnp.arange(blocks, dtype=jnp.int32)[:, None]) * CAP + slots).reshape(SEQUENCE_TOKENS * TOP)
    copies = jnp.repeat(normed, TOP, axis=0)
    buffer = jnp.zeros((EXPERTS * blocks * CAP, D), jnp.bfloat16).at[target].set(copies)
    results = lax.map(expert_apply, (buffer.reshape(EXPERTS, blocks * CAP, D), gate_weight, up_weight, down_weight))
    results = results.reshape(EXPERTS * blocks * CAP, D)
    picked = results[target].reshape(SEQUENCE_TOKENS, TOP, D).astype(jnp.float32)
    return (hidden.astype(jnp.float32) + lax.optimization_barrier(jnp.sum(route_weights[..., None] * picked, axis=1))).astype(jnp.bfloat16)
```

```python
import jax
import jax.numpy as jnp
import numpy as np
from jax import lax
from jax.experimental import pallas as pl
from jax.experimental.pallas import tpu as pltpu
from jax.sharding import Mesh
from jax.sharding import PartitionSpec as P

PLAIN_HEAD_WIDTH = 128
QK_ROPE = 64
VALUE_WIDTH = 128
GRID_W = 64
SP = ("sp_0", "sp_1")
GRP_SP = ("grp", "sp_0", "sp_1")
GRP_SP_TP = ("grp", "sp_0", "sp_1", "tp")


theta = 10000.0
eps = 1e-06
limit = 7.0
slope = 1.702
STAT_LANES = 128


def turn_tables(place):
    count = QK_ROPE // 4
    freqs = theta ** (-jnp.arange(count, dtype=jnp.float32) / count)
    halves_cos, halves_sin = [], []
    for shift in (place // GRID_W, place % GRID_W):
        angle = shift.astype(jnp.float32)[:, None] * freqs[None, :]
        halves_cos += [jnp.cos(angle)] * 2
        halves_sin += [jnp.sin(angle)] * 2
    return jnp.concatenate(halves_cos, axis=1), jnp.concatenate(halves_sin, axis=1)


def partner_matrix(width):
    count = QK_ROPE // 4
    out = np.zeros((width, width), np.float32)
    for at in range(0, width, 2 * count):
        for i in range(count):
            out[at + count + i, at + i] = -1.0
            out[at + i, at + count + i] = 1.0
    return out


def norm_scale(values, gain):
    wide = values.astype(jnp.float32)
    return (
        wide
        * lax.rsqrt(jnp.mean(wide * wide, axis=-1, keepdims=True) + eps)
        * gain.astype(jnp.float32)
    )


def shifted(array, axis, step):
    count = lax.axis_size(axis)
    return lax.ppermute(array, axis, [(i, (i + step) % count) for i in range(count)])


def expert_active(rows, gate_w, up_w):
    gate_pre = jnp.minimum(jnp.dot(rows, gate_w, preferred_element_type=jnp.float32), limit)
    up_pre = jnp.clip(jnp.dot(rows, up_w, preferred_element_type=jnp.float32), -limit, limit)
    return ((up_pre + 1.0) * gate_pre * jax.nn.sigmoid(slope * gate_pre)).astype(jnp.bfloat16)


def expert_whole(rows, quarters):
    total = jnp.zeros((rows.shape[0], quarters[0][2].shape[1]), jnp.float32)
    for gate_w, up_w, down_w in quarters:
        active = expert_active(rows, gate_w, up_w)
        product = jnp.dot(active, down_w, preferred_element_type=jnp.float32)
        total = total + product.astype(jnp.bfloat16).astype(jnp.float32)
    return total.astype(jnp.bfloat16)


def attend_body(near_ref, other_ref, shares_ref, cos_ref, sin_ref, swap_ref, out_ref, kv_ref):
    shards = shares_ref.shape[0]
    width = shares_ref.shape[2]
    near = near_ref.shape[0]
    latent_width = width
    quarter = out_ref.shape[1]
    tokens = shards * quarter
    value_wide = width // 2
    heads = value_wide // PLAIN_HEAD_WIDTH
    scale = (PLAIN_HEAD_WIDTH + QK_ROPE) ** (-0.5)
    near_rot = near_ref[:, latent_width : latent_width + QK_ROPE]
    other_rot = other_ref[:, latent_width : latent_width + QK_ROPE]
    lane = lax.broadcasted_iota(jnp.int32, (tokens, STAT_LANES), 1)
    stats = jnp.zeros((tokens, STAT_LANES), jnp.float32)
    last = (((1,), (1,)), ((), ()))
    for j in range(shards):
        matrix = shares_ref[j, :latent_width, :]
        kv_ref[:near, :] = jnp.dot(
            near_ref[:, :latent_width], matrix, preferred_element_type=jnp.float32
        ).astype(jnp.bfloat16)
        kv_ref[near:, :] = jnp.dot(
            other_ref[:, :latent_width], matrix, preferred_element_type=jnp.float32
        ).astype(jnp.bfloat16)
        at = latent_width
        half = tokens // 2
        plain = jnp.concatenate(
            (
                shares_ref[j, at : at + half, :value_wide],
                shares_ref[j, at : at + half, value_wide:],
            ),
            axis=0,
        )
        at += half
        raw = jnp.concatenate(
            [
                shares_ref[j, at : at + quarter, i * heads * QK_ROPE : (i + 1) * heads * QK_ROPE]
                for i in range(tokens // quarter)
            ],
            axis=0,
        )
        swapped = jnp.dot(raw, swap_ref[...], preferred_element_type=jnp.float32)
        turned = (raw.astype(jnp.float32) * cos_ref[...] + swapped * sin_ref[...]).astype(
            jnp.bfloat16
        )
        for h in range(heads):
            lo = h * PLAIN_HEAD_WIDTH
            query = plain[:, lo : lo + PLAIN_HEAD_WIDTH]
            query_rot = turned[:, h * QK_ROPE : (h + 1) * QK_ROPE]
            keys = kv_ref[:, lo : lo + PLAIN_HEAD_WIDTH]
            rotary = jnp.concatenate(
                (
                    lax.dot_general(query_rot, near_rot, last, preferred_element_type=jnp.float32),
                    lax.dot_general(query_rot, other_rot, last, preferred_element_type=jnp.float32),
                ),
                axis=1,
            )
            scores = (
                lax.dot_general(query, keys, last, preferred_element_type=jnp.float32) + rotary
            ) * scale
            peak = jnp.max(scores, axis=1, keepdims=True)
            weights = jnp.exp(scores - peak)
            total = jnp.sum(weights, axis=1, keepdims=True)
            head_values = kv_ref[:, value_wide + lo : value_wide + lo + VALUE_WIDTH]
            summed = jnp.dot(
                weights.astype(jnp.bfloat16), head_values, preferred_element_type=jnp.float32
            )
            result = (summed / total).astype(jnp.bfloat16)
            head = j * heads + h
            for i in range(shards):
                out_ref[i, :, head * VALUE_WIDTH : (head + 1) * VALUE_WIDTH] = result[
                    i * quarter : (i + 1) * quarter
                ]
            rest = peak + jnp.log(total)
            for part in range(3):
                top = rest.astype(jnp.bfloat16).astype(jnp.float32)
                rest = rest - top
                stats = jnp.where(lane == part * shards * heads + head, top, stats)
    stats = stats.astype(jnp.bfloat16)
    for i in range(shards):
        out_ref[i, :, shards * value_wide :] = stats[i * quarter : (i + 1) * quarter]


def mix_body(parts_ref, weight_ref, residual_ref, gain_ref, table_ref, hidden_ref, outgoing_ref):
    shards = parts_ref.shape[0]
    wide = weight_ref.shape[0]
    heads = wide // VALUE_WIDTH
    sums = []
    for i in range(shards):
        stat = parts_ref[i, :, wide:].astype(jnp.float32)
        sums.append(
            stat[:, :heads] + (stat[:, heads : 2 * heads] + stat[:, 2 * heads : 3 * heads])
        )
    most = sums[0]
    for s in sums[1:]:
        most = jnp.maximum(most, s)
    shares = [jnp.exp(s - most) for s in sums]
    whole = shares[0]
    for s in shares[1:]:
        whole = whole + s
    shares = [s / whole for s in shares]
    pieces = []
    for h in range(heads):
        lo = h * VALUE_WIDTH
        piece = shares[0][:, h : h + 1] * parts_ref[0, :, lo : lo + VALUE_WIDTH].astype(jnp.float32)
        for i in range(1, shards):
            piece = piece + shares[i][:, h : h + 1] * parts_ref[
                i, :, lo : lo + VALUE_WIDTH
            ].astype(jnp.float32)
        pieces.append(piece.astype(jnp.bfloat16))
    attended = jnp.concatenate(pieces, axis=1)
    projected = jnp.dot(attended, weight_ref[...], preferred_element_type=jnp.float32)
    hidden = (residual_ref[...].astype(jnp.float32) + projected).astype(jnp.bfloat16)
    hidden_ref[...] = hidden
    normed = norm_scale(hidden, gain_ref[...]).astype(jnp.bfloat16)
    outgoing_ref[...] = jnp.dot(
        table_ref[...], normed, preferred_element_type=jnp.float32
    ).astype(jnp.bfloat16)


def on_device(
    query_plain,
    query_turn,
    latent,
    key_turn,
    latent_norm_scale,
    plain_key_matrix,
    value_matrix,
    residual,
    out_weight,
    ffn_gain,
    gate_weight,
    up_weight,
    down_weight,
    routes,
    route_weights,
):
    tok_dev = latent.shape[0]
    rows_dev = residual.shape[0]
    model_width = residual.shape[1]
    latent_width = latent.shape[1]
    group = lax.axis_size("tp")
    heads_dev = query_plain.shape[1] // PLAIN_HEAD_WIDTH
    mine = lax.axis_index("tp") * rows_dev

    half = tok_dev // 2
    quarter = query_turn.shape[0] // (latent_width // query_turn.shape[1])
    share = jnp.concatenate(
        (
            jnp.concatenate((plain_key_matrix, value_matrix), axis=1),
            jnp.concatenate((query_plain[:half], query_plain[half:]), axis=1),
            jnp.concatenate(
                [query_turn[i * quarter : (i + 1) * quarter] for i in range(tok_dev // quarter)],
                axis=1,
            ),
        ),
        axis=0,
    )
    shares = lax.all_to_all(
        jnp.broadcast_to(share[None], (group,) + share.shape), "tp", 0, 0, tiled=True
    )

    place = lax.axis_index(SP) * tok_dev + jnp.arange(tok_dev, dtype=jnp.int32)
    cosines, sines = turn_tables(place)
    own_cos = lax.dynamic_slice_in_dim(cosines, mine, rows_dev, 0)
    own_sin = lax.dynamic_slice_in_dim(sines, mine, rows_dev, 0)
    own_latent = lax.dynamic_slice_in_dim(latent, mine, rows_dev, 0)
    own_key = lax.dynamic_slice_in_dim(key_turn, mine, rows_dev, 0)
    normed_latent = norm_scale(own_latent, latent_norm_scale).astype(jnp.bfloat16)
    swap_key = jnp.asarray(partner_matrix(QK_ROPE), jnp.bfloat16)
    key_rot = (
        own_key.astype(jnp.float32) * own_cos
        + jnp.dot(own_key, swap_key, preferred_element_type=jnp.float32) * own_sin
    ).astype(jnp.bfloat16)
    sent = jnp.concatenate((normed_latent, key_rot, jnp.zeros_like(key_rot)), axis=1)
    near = lax.all_gather(sent, "sp_0", axis=0, tiled=True)
    other = shifted(near, "sp_1", 1)

    parts = pl.pallas_call(
        attend_body,
        out_shape=jax.ShapeDtypeStruct(
            (group, rows_dev, group * heads_dev * VALUE_WIDTH + STAT_LANES), jnp.bfloat16
        ),
        scratch_shapes=[pltpu.VMEM((2 * near.shape[0], 2 * heads_dev * VALUE_WIDTH), jnp.bfloat16)],
        compiler_params=pltpu.CompilerParams(vmem_limit_bytes=24 << 20),
        name="attend",
    )(
        near,
        other,
        shares,
        jnp.concatenate([cosines] * heads_dev, axis=1),
        jnp.concatenate([sines] * heads_dev, axis=1),
        jnp.asarray(partner_matrix(heads_dev * QK_ROPE), jnp.bfloat16),
    )
    gathered = lax.all_to_all(parts, "tp", 0, 0, tiled=True)

    top_count = routes.shape[1]
    experts_all = lax.axis_size(SP) * gate_weight.shape[0]
    capacity = min(rows_dev, max(2, rows_dev * top_count * 3 // (2 * experts_all)))
    flat_routes = routes.reshape(rows_dev * top_count)
    marks = (flat_routes[:, None] == jnp.arange(experts_all, dtype=jnp.int32)[None, :]).astype(
        jnp.int32
    )
    earlier = jnp.cumsum(marks, axis=0, dtype=jnp.int32) - marks
    slots = jnp.sum(earlier * marks, axis=1, dtype=jnp.int32)
    target = flat_routes * capacity + slots
    chosen = (
        target.reshape(rows_dev, top_count)[None, :, :]
        == jnp.arange(experts_all * capacity, dtype=jnp.int32)[:, None, None]
    )
    dispatch_table = jnp.sum(chosen.astype(jnp.bfloat16), axis=2)

    hidden, outgoing = pl.pallas_call(
        mix_body,
        out_shape=(
            jax.ShapeDtypeStruct((rows_dev, model_width), jnp.bfloat16),
            jax.ShapeDtypeStruct((experts_all * capacity, model_width), jnp.bfloat16),
        ),
        compiler_params=pltpu.CompilerParams(vmem_limit_bytes=16 << 20),
        name="mix",
    )(gathered, out_weight, residual, ffn_gain.reshape(1, model_width), dispatch_table)
    arrived = lax.all_to_all(
        outgoing.reshape(experts_all, capacity, model_width), SP, 0, 0, tiled=True
    )

    own = (gate_weight[0], up_weight[0], down_weight[0])
    left, right = [], []
    for w in own:
        left.append(shifted(w, "tp", 1))
        right.append(shifted(w, "tp", -1))
    cut = own[2].shape[0] // 2
    far_gate = shifted(left[0], "tp", 1)
    far_up = shifted(right[1], "tp", -1)
    far_down_l = shifted(left[2][:cut], "tp", 1)
    far_down_r = shifted(right[2][cut:], "tp", -1)
    far = (far_gate, far_up, jnp.concatenate((far_down_l, far_down_r), axis=0))

    result_rows = expert_whole(
        arrived.reshape(experts_all * capacity, model_width), (own, left, right, far)
    )
    returned = lax.all_to_all(
        result_rows.reshape(experts_all, capacity, model_width), SP, 0, 0, tiled=True
    )
    picked = returned.reshape(experts_all * capacity, model_width)[target]
    picked = picked.reshape(rows_dev, top_count, model_width).astype(jnp.float32)
    return (
        hidden.astype(jnp.float32) + jnp.sum(route_weights[..., None] * picked, axis=1)
    ).astype(jnp.bfloat16)


def solution(mesh):
    torus = Mesh(
        mesh.devices.reshape(mesh.shape["grp"], 16, 2, mesh.shape["tp"]),
        ("grp", "sp_0", "sp_1", "tp"),
    )
    placed = (
        P(GRP_SP, "tp"),
        P(GRP_SP, "tp"),
        P(GRP_SP, None),
        P(GRP_SP, None),
        P(),
        P(None, "tp"),
        P(None, "tp"),
        P(GRP_SP_TP, None),
        P(),
        P(),
        P(SP, None, "tp"),
        P(SP, None, "tp"),
        P(SP, "tp", None),
        P(GRP_SP_TP, None),
        P(GRP_SP_TP, None),
    )
    return jax.shard_map(
        on_device, mesh=torus, in_specs=placed, out_specs=P(GRP_SP_TP, None), check_vma=False
    )
```

```python
import jax
import jax.numpy as jnp
import numpy as np
from jax import lax
from jax.experimental import pallas as pl
from jax.experimental.pallas import tpu as pltpu
from jax.sharding import Mesh
from jax.sharding import PartitionSpec as P

PLAIN_HEAD_WIDTH = 128
QK_ROPE = 64
VALUE_WIDTH = 128
GRID_W = 64
SP = ("sp_0", "sp_1")
GRP_SP = ("grp", "sp_0", "sp_1")
GRP_SP_TP = ("grp", "sp_0", "sp_1", "tp")


theta = 10000.0
eps = 1e-06
limit = 7.0
slope = 1.702
STAT_LANES = 128


def turn_tables(place, heads):
    count = QK_ROPE // 4
    lane = jnp.arange(heads * QK_ROPE, dtype=jnp.int32)
    freqs = theta ** (-(lane % count).astype(jnp.float32) / count)
    by_row = (lane % QK_ROPE) < QK_ROPE // 2
    shift = jnp.where(by_row[None, :], (place // GRID_W)[:, None], (place % GRID_W)[:, None])
    angle = shift.astype(jnp.float32) * freqs[None, :]
    return jnp.cos(angle), jnp.sin(angle)


def partner_matrix(width):
    count = QK_ROPE // 4
    out = np.zeros((width, width), np.float32)
    for at in range(0, width, 2 * count):
        for i in range(count):
            out[at + count + i, at + i] = -1.0
            out[at + i, at + count + i] = 1.0
    return out


def norm_scale(values, gain):
    wide = values.astype(jnp.float32)
    return (
        wide
        * lax.rsqrt(jnp.mean(wide * wide, axis=-1, keepdims=True) + eps)
        * gain.astype(jnp.float32)
    )


def shifted(array, axis, step):
    count = lax.axis_size(axis)
    return lax.ppermute(array, axis, [(i, (i + step) % count) for i in range(count)])


def prepare_body(
    index_ref,
    latent_ref,
    gain_ref,
    key_ref,
    cos_ref,
    sin_ref,
    swap_ref,
    key_matrix_ref,
    value_matrix_ref,
    plain_ref,
    turn_ref,
    sent_ref,
    shares_ref,
):
    rows, latent_width = latent_ref.shape
    sent_ref[:, :latent_width] = norm_scale(latent_ref[...], gain_ref[...]).astype(jnp.bfloat16)
    tokens = key_ref.shape[1]
    at = lax.broadcasted_iota(jnp.int32, (rows, tokens), 0) + index_ref[0] * rows
    pick = (at == lax.broadcasted_iota(jnp.int32, (rows, tokens), 1)).astype(jnp.bfloat16)
    key = lax.dot_general(
        pick, key_ref[...], (((1,), (1,)), ((), ())), preferred_element_type=jnp.float32
    )
    swapped = jnp.dot(
        key.astype(jnp.bfloat16), swap_ref[...], preferred_element_type=jnp.float32
    )
    turned = (key * cos_ref[...] + swapped * sin_ref[...]).astype(jnp.bfloat16)
    sent_ref[:, latent_width:] = jnp.concatenate((turned, jnp.zeros_like(turned)), axis=1)
    wide = key_matrix_ref.shape[1]
    turn_wide = turn_ref.shape[1]
    half = tokens // 2
    quarter = tokens * turn_wide // (2 * wide)
    for j in range(shares_ref.shape[0]):
        shares_ref[j, :latent_width, :wide] = key_matrix_ref[...]
        shares_ref[j, :latent_width, wide:] = value_matrix_ref[...]
        shares_ref[j, latent_width : latent_width + half, :wide] = plain_ref[:half, :]
        shares_ref[j, latent_width : latent_width + half, wide:] = plain_ref[half:, :]
        for i in range(tokens // quarter):
            shares_ref[
                j, latent_width + half :, i * turn_wide : (i + 1) * turn_wide
            ] = turn_ref[i * quarter : (i + 1) * quarter, :]


def attend_body(near_ref, other_ref, shares_ref, cos_ref, sin_ref, swap_ref, out_ref, kv_ref):
    shards = shares_ref.shape[0]
    width = shares_ref.shape[2]
    near = near_ref.shape[0]
    latent_width = width
    quarter = out_ref.shape[1]
    tokens = shards * quarter
    value_wide = width // 2
    heads = value_wide // PLAIN_HEAD_WIDTH
    scale = (PLAIN_HEAD_WIDTH + QK_ROPE) ** (-0.5)
    near_rot = near_ref[:, latent_width : latent_width + QK_ROPE]
    other_rot = other_ref[:, latent_width : latent_width + QK_ROPE]
    lane = lax.broadcasted_iota(jnp.int32, (tokens, STAT_LANES), 1)
    stats = jnp.zeros((tokens, STAT_LANES), jnp.float32)
    last = (((1,), (1,)), ((), ()))
    for j in range(shards):
        matrix = shares_ref[j, :latent_width, :]
        kv_ref[:near, :] = jnp.dot(
            near_ref[:, :latent_width], matrix, preferred_element_type=jnp.float32
        ).astype(jnp.bfloat16)
        kv_ref[near:, :] = jnp.dot(
            other_ref[:, :latent_width], matrix, preferred_element_type=jnp.float32
        ).astype(jnp.bfloat16)
        at = latent_width
        half = tokens // 2
        plain = jnp.concatenate(
            (
                shares_ref[j, at : at + half, :value_wide],
                shares_ref[j, at : at + half, value_wide:],
            ),
            axis=0,
        )
        at += half
        raw = jnp.concatenate(
            [
                shares_ref[j, at : at + quarter, i * heads * QK_ROPE : (i + 1) * heads * QK_ROPE]
                for i in range(tokens // quarter)
            ],
            axis=0,
        )
        swapped = jnp.dot(raw, swap_ref[...], preferred_element_type=jnp.float32)
        turned = (raw.astype(jnp.float32) * cos_ref[...] + swapped * sin_ref[...]).astype(
            jnp.bfloat16
        )
        for h in range(heads):
            lo = h * PLAIN_HEAD_WIDTH
            query = plain[:, lo : lo + PLAIN_HEAD_WIDTH]
            query_rot = turned[:, h * QK_ROPE : (h + 1) * QK_ROPE]
            keys = kv_ref[:, lo : lo + PLAIN_HEAD_WIDTH]
            rotary = jnp.concatenate(
                (
                    lax.dot_general(query_rot, near_rot, last, preferred_element_type=jnp.float32),
                    lax.dot_general(query_rot, other_rot, last, preferred_element_type=jnp.float32),
                ),
                axis=1,
            )
            scores = (
                lax.dot_general(query, keys, last, preferred_element_type=jnp.float32) + rotary
            ) * scale
            peak = jnp.max(scores, axis=1, keepdims=True)
            weights = jnp.exp(scores - peak)
            total = jnp.sum(weights, axis=1, keepdims=True)
            head_values = kv_ref[:, value_wide + lo : value_wide + lo + VALUE_WIDTH]
            summed = jnp.dot(
                weights.astype(jnp.bfloat16), head_values, preferred_element_type=jnp.float32
            )
            result = (summed / total).astype(jnp.bfloat16)
            head = j * heads + h
            for i in range(shards):
                out_ref[i, :, head * VALUE_WIDTH : (head + 1) * VALUE_WIDTH] = result[
                    i * quarter : (i + 1) * quarter
                ]
            rest = peak + jnp.log(total)
            for part in range(3):
                top = rest.astype(jnp.bfloat16).astype(jnp.float32)
                rest = rest - top
                stats = jnp.where(lane == part * shards * heads + head, top, stats)
    stats = stats.astype(jnp.bfloat16)
    for i in range(shards):
        out_ref[i, :, shards * value_wide :] = stats[i * quarter : (i + 1) * quarter]


GROUP = 8


def lanes_of(index, width):
    return slice(index * width, (index + 1) * width)


def mix_body(
    parts_ref, weight_hbm, residual_ref, gain_ref, routes_ref, hidden_ref, outgoing_ref, weight_ref, sem
):
    load = pltpu.make_async_copy(weight_hbm, weight_ref, sem)
    load.start()
    shards = parts_ref.shape[0]
    rows, model_width = residual_ref.shape
    wide = weight_ref.shape[0]
    heads = wide // VALUE_WIDTH
    sums = []
    for i in range(shards):
        stat = parts_ref[i, :, wide:].astype(jnp.float32)
        sums.append(
            stat[:, :heads] + (stat[:, heads : 2 * heads] + stat[:, 2 * heads : 3 * heads])
        )
    most = sums[0]
    for s in sums[1:]:
        most = jnp.maximum(most, s)
    shares = [jnp.exp(s - most) for s in sums]
    whole = shares[0]
    for s in shares[1:]:
        whole = whole + s
    shares = [s / whole for s in shares]
    pieces = []
    for h in range(heads):
        lo = h * VALUE_WIDTH
        piece = shares[0][:, h : h + 1] * parts_ref[0, :, lo : lo + VALUE_WIDTH].astype(jnp.float32)
        for i in range(1, shards):
            piece = piece + shares[i][:, h : h + 1] * parts_ref[
                i, :, lo : lo + VALUE_WIDTH
            ].astype(jnp.float32)
        pieces.append(piece.astype(jnp.bfloat16))
    attended = jnp.concatenate(pieces, axis=1)

    total_rows = outgoing_ref.shape[0]
    line = lax.broadcasted_iota(jnp.int32, (total_rows, rows), 0)
    named = jnp.zeros((total_rows, rows), jnp.int32)
    for k in range(routes_ref.shape[0]):
        named = named | (routes_ref[k : k + 1, :] == line // GROUP).astype(jnp.int32)
    before = (
        lax.broadcasted_iota(jnp.int32, (rows, rows), 0)
        < lax.broadcasted_iota(jnp.int32, (rows, rows), 1)
    ).astype(jnp.bfloat16)
    rank = jnp.dot(
        named.astype(jnp.float32).astype(jnp.bfloat16), before, preferred_element_type=jnp.float32
    ).astype(jnp.int32)
    table = jnp.where((named > 0) & (rank == line % GROUP), 1.0, 0.0).astype(jnp.bfloat16)

    load.wait()
    projected = jnp.dot(attended, weight_ref[...], preferred_element_type=jnp.float32)
    hidden = (residual_ref[...].astype(jnp.float32) + projected).astype(jnp.bfloat16)
    hidden_ref[...] = hidden
    normed = norm_scale(hidden, gain_ref[...]).astype(jnp.bfloat16)
    tail = model_width - outgoing_ref.shape[1]
    ends = normed[:, model_width - tail :]
    for s in range(GROUP - 1):
        of_last = jnp.where(
            (named > 0) & (rank == s) & (line % GROUP == GROUP - 1), 1.0, 0.0
        ).astype(jnp.bfloat16)
        outgoing_ref[:, lanes_of(s, tail)] = (
            jnp.dot(table, normed[:, lanes_of(s, tail)], preferred_element_type=jnp.float32)
            + jnp.dot(of_last, ends, preferred_element_type=jnp.float32)
        ).astype(jnp.bfloat16)


def expert_body(arrived_ref, *refs):
    count = (len(refs) - 4) // 3
    weights_hbm = refs[: 3 * count]
    out_ref, thin_ref, down_ref, sems = refs[3 * count :]
    gate_up = weights_hbm[0].shape
    loads = []
    for q in range(count):
        for m in range(3):
            dst = down_ref.at[q] if m == 2 else thin_ref.at[q, m]
            loads.append(pltpu.make_async_copy(weights_hbm[3 * q + m], dst, sems.at[q, m]))
            loads[-1].start()
    rows, main = arrived_ref.shape
    model_width = gate_up[0]
    tail = model_width - main
    line = lax.broadcasted_iota(jnp.int32, (rows, rows), 0)
    column = lax.broadcasted_iota(jnp.int32, (rows, rows), 1)
    ends = jnp.zeros((rows, tail), jnp.float32)
    for s in range(GROUP - 1):
        pick = jnp.where(
            (line % GROUP == s) & (column == line - s + GROUP - 1), 1.0, 0.0
        ).astype(jnp.bfloat16)
        ends = ends + jnp.dot(
            pick, arrived_ref[:, lanes_of(s, tail)], preferred_element_type=jnp.float32
        )
    ends = ends.astype(jnp.bfloat16)
    total = jnp.zeros((rows, model_width), jnp.float32)
    for q in range(count):
        loads[3 * q].wait()
        gate_pre = jnp.dot(
            arrived_ref[...], thin_ref[q, 0, :main, :], preferred_element_type=jnp.float32
        ) + jnp.dot(ends, thin_ref[q, 0, main:, :], preferred_element_type=jnp.float32)
        loads[3 * q + 1].wait()
        up_pre = jnp.dot(
            arrived_ref[...], thin_ref[q, 1, :main, :], preferred_element_type=jnp.float32
        ) + jnp.dot(ends, thin_ref[q, 1, main:, :], preferred_element_type=jnp.float32)
        gate_pre = jnp.minimum(gate_pre, limit)
        active = (
            (jnp.clip(up_pre, -limit, limit) + 1.0) * gate_pre * jax.nn.sigmoid(slope * gate_pre)
        ).astype(jnp.bfloat16)
        loads[3 * q + 2].wait()
        product = jnp.dot(active, down_ref[q], preferred_element_type=jnp.float32)
        total = total + product.astype(jnp.bfloat16).astype(jnp.float32)
    result = total.astype(jnp.bfloat16)
    last = result[:, main:]
    group_end = lax.broadcasted_iota(jnp.int32, (rows, tail), 0) % GROUP == GROUP - 1
    for s in range(GROUP - 1):
        pick = jnp.where(
            (line % GROUP == GROUP - 1) & (column == line - (GROUP - 1) + s), 1.0, 0.0
        ).astype(jnp.bfloat16)
        moved = jnp.dot(pick, last, preferred_element_type=jnp.float32).astype(jnp.bfloat16)
        out_ref[:, lanes_of(s, tail)] = jnp.where(
            group_end, moved.astype(jnp.float32), result[:, lanes_of(s, tail)].astype(jnp.float32)
        ).astype(jnp.bfloat16)


def combine_body(returned_ref, hidden_ref, routes_ref, weights_ref, out_ref):
    rows, model_width = hidden_ref.shape
    total_rows, main = returned_ref.shape
    tail = model_width - main
    column = lax.broadcasted_iota(jnp.int32, (rows, total_rows), 1)
    named = jnp.zeros((rows, total_rows), jnp.float32)
    weight = jnp.zeros((rows, total_rows), jnp.float32)
    for k in range(routes_ref.shape[1]):
        here = routes_ref[:, k : k + 1] == column // GROUP
        named = jnp.where(here, 1.0, named)
        weight = jnp.where(here, weights_ref[:, k : k + 1], weight)
    before = (
        lax.broadcasted_iota(jnp.int32, (rows, rows), 1)
        < lax.broadcasted_iota(jnp.int32, (rows, rows), 0)
    ).astype(jnp.bfloat16)
    rank = jnp.dot(
        before, named.astype(jnp.bfloat16), preferred_element_type=jnp.float32
    ).astype(jnp.int32)
    parts = []
    rest = weight
    for _ in range(3):
        top = rest.astype(jnp.bfloat16).astype(jnp.float32)
        rest = rest - top
        parts.append(top)

    def gathered(keep, values):
        table = jnp.concatenate([jnp.where(keep, p, 0.0) for p in parts], axis=0)
        got = jnp.dot(table.astype(jnp.bfloat16), values, preferred_element_type=jnp.float32)
        return got[:rows] + (got[rows : 2 * rows] + got[2 * rows :])

    own = (named > 0) & (rank == column % GROUP)
    out_ref[:, :main] = (
        hidden_ref[:, :main].astype(jnp.float32) + gathered(own, returned_ref[...])
    ).astype(jnp.bfloat16)
    ends = jnp.zeros((rows, tail), jnp.float32)
    for s in range(GROUP - 1):
        keep = (named > 0) & (rank == s) & (column % GROUP == GROUP - 1)
        ends = ends + gathered(keep, returned_ref[:, lanes_of(s, tail)])
    out_ref[:, main:] = (hidden_ref[:, main:].astype(jnp.float32) + ends).astype(jnp.bfloat16)


def on_device(
    query_plain,
    query_turn,
    latent,
    key_turn,
    latent_norm_scale,
    plain_key_matrix,
    value_matrix,
    residual,
    out_weight,
    ffn_gain,
    gate_weight,
    up_weight,
    down_weight,
    routes,
    route_weights,
):
    tok_dev = latent.shape[0]
    rows_dev = residual.shape[0]
    model_width = residual.shape[1]
    latent_width = latent.shape[1]
    group = lax.axis_size("tp")
    heads_dev = query_plain.shape[1] // PLAIN_HEAD_WIDTH
    place = lax.axis_index(SP) * tok_dev + jnp.arange(tok_dev, dtype=jnp.int32)
    at_tp = lax.axis_index("tp")
    own_place = (
        lax.axis_index(SP) * tok_dev
        + at_tp * rows_dev
        + jnp.arange(rows_dev, dtype=jnp.int32)
    )
    own_cos, own_sin = turn_tables(own_place, 1)
    cosines, sines = turn_tables(place, heads_dev)
    share_rows = latent_width + tok_dev // 2 + tok_dev * query_turn.shape[1] // latent_width
    wide = plain_key_matrix.shape[1]
    whole = lambda *shape: pl.BlockSpec(shape, lambda i, at: (0,) * len(shape))
    sent, shares = pl.pallas_call(
        prepare_body,
        out_shape=(
            jax.ShapeDtypeStruct((rows_dev, latent_width + 2 * QK_ROPE), jnp.bfloat16),
            jax.ShapeDtypeStruct((group, share_rows, latent_width), jnp.bfloat16),
        ),
        grid_spec=pltpu.PrefetchScalarGridSpec(
            num_scalar_prefetch=1,
            grid=(1,),
            in_specs=[
                pl.BlockSpec((rows_dev, latent_width), lambda i, at: (at[0], 0)),
                whole(1, latent_width),
                whole(QK_ROPE, tok_dev),
                whole(rows_dev, QK_ROPE),
                whole(rows_dev, QK_ROPE),
                whole(QK_ROPE, QK_ROPE),
                whole(latent_width, wide),
                whole(latent_width, wide),
                whole(tok_dev, query_plain.shape[1]),
                whole(tok_dev, query_turn.shape[1]),
            ],
            out_specs=(
                whole(rows_dev, latent_width + 2 * QK_ROPE),
                whole(group, share_rows, latent_width),
            ),
        ),
        compiler_params=pltpu.CompilerParams(vmem_limit_bytes=16 << 20),
        name="prepare",
    )(
        at_tp.reshape(1),
        latent,
        latent_norm_scale.reshape(1, latent_width),
        key_turn.T,
        own_cos,
        own_sin,
        jnp.asarray(partner_matrix(QK_ROPE), jnp.bfloat16),
        plain_key_matrix,
        value_matrix,
        query_plain,
        query_turn,
    )
    shares = lax.all_to_all(shares, "tp", 0, 0, tiled=True)
    near = lax.all_gather(sent, "sp_0", axis=0, tiled=True)
    other = shifted(near, "sp_1", 1)

    parts = pl.pallas_call(
        attend_body,
        out_shape=jax.ShapeDtypeStruct(
            (group, rows_dev, group * heads_dev * VALUE_WIDTH + STAT_LANES), jnp.bfloat16
        ),
        scratch_shapes=[pltpu.VMEM((2 * near.shape[0], 2 * heads_dev * VALUE_WIDTH), jnp.bfloat16)],
        compiler_params=pltpu.CompilerParams(vmem_limit_bytes=24 << 20),
        name="attend",
    )(
        near,
        other,
        shares,
        cosines,
        sines,
        jnp.asarray(partner_matrix(heads_dev * QK_ROPE), jnp.bfloat16),
    )
    gathered = lax.all_to_all(parts, "tp", 0, 0, tiled=True)

    experts_all = lax.axis_size(SP) * gate_weight.shape[0]
    top_count = routes.shape[1]
    capacity = min(rows_dev, max(2, rows_dev * top_count * 3 // (2 * experts_all)))
    assert capacity == GROUP - 1
    main = model_width * capacity // GROUP
    vmem = pl.BlockSpec(memory_space=pltpu.VMEM)
    hbm = pl.BlockSpec(memory_space=pltpu.HBM)
    hidden, outgoing = pl.pallas_call(
        mix_body,
        out_shape=(
            jax.ShapeDtypeStruct((rows_dev, model_width), jnp.bfloat16),
            jax.ShapeDtypeStruct((experts_all * GROUP, main), jnp.bfloat16),
        ),
        in_specs=[vmem, hbm, vmem, vmem, vmem],
        scratch_shapes=[pltpu.VMEM(out_weight.shape, jnp.bfloat16), pltpu.SemaphoreType.DMA],
        compiler_params=pltpu.CompilerParams(vmem_limit_bytes=16 << 20),
        name="mix",
    )(gathered, out_weight, residual, ffn_gain.reshape(1, model_width), routes.T)
    arrived = lax.all_to_all(outgoing.reshape(experts_all, GROUP, main), SP, 0, 0, tiled=True)

    own = (gate_weight[0], up_weight[0], down_weight[0])
    left, right = [], []
    for w in own:
        left.append(shifted(w, "tp", 1))
        right.append(shifted(w, "tp", -1))
    cut = own[2].shape[0] // 2
    far_gate = shifted(left[0], "tp", 1)
    far_up = shifted(right[1], "tp", -1)
    far_down_l = shifted(left[2][:cut], "tp", 1)
    far_down_r = shifted(right[2][cut:], "tp", -1)
    far = (far_gate, far_up, jnp.concatenate((far_down_l, far_down_r), axis=0))

    weights = []
    for gate_w, up_w, down_w in (own, left, right, far):
        weights += [gate_w, up_w, down_w]
    result_rows = pl.pallas_call(
        expert_body,
        out_shape=jax.ShapeDtypeStruct((experts_all * GROUP, main), jnp.bfloat16),
        in_specs=[vmem] + [hbm] * len(weights),
        scratch_shapes=[
            pltpu.VMEM((group, 2) + own[0].shape, jnp.bfloat16),
            pltpu.VMEM((group,) + own[2].shape, jnp.bfloat16),
            pltpu.SemaphoreType.DMA((group, 3)),
        ],
        compiler_params=pltpu.CompilerParams(vmem_limit_bytes=40 << 20),
        name="expert",
    )(arrived.reshape(experts_all * GROUP, main), *weights)
    returned = lax.all_to_all(result_rows.reshape(experts_all, GROUP, main), SP, 0, 0, tiled=True)
    return pl.pallas_call(
        combine_body,
        out_shape=jax.ShapeDtypeStruct((rows_dev, model_width), jnp.bfloat16),
        compiler_params=pltpu.CompilerParams(vmem_limit_bytes=16 << 20),
        name="combine",
    )(returned.reshape(experts_all * GROUP, main), hidden, routes, route_weights)


def solution(mesh):
    torus = Mesh(
        mesh.devices.reshape(mesh.shape["grp"], 16, 2, mesh.shape["tp"]),
        ("grp", "sp_0", "sp_1", "tp"),
    )
    placed = (
        P(GRP_SP, "tp"),
        P(GRP_SP, "tp"),
        P(GRP_SP, None),
        P(GRP_SP, None),
        P(),
        P(None, "tp"),
        P(None, "tp"),
        P(GRP_SP_TP, None),
        P(),
        P(),
        P(SP, None, "tp"),
        P(SP, None, "tp"),
        P(SP, "tp", None),
        P(GRP_SP_TP, None),
        P(GRP_SP_TP, None),
    )
    return jax.shard_map(
        on_device, mesh=torus, in_specs=placed, out_specs=P(GRP_SP_TP, None), check_vma=False
    )
```

```python
import jax
import jax.numpy as jnp
import numpy as np
from jax import lax
from jax.experimental import pallas as pl
from jax.experimental.pallas import tpu as pltpu
from jax.sharding import Mesh
from jax.sharding import PartitionSpec as P

PLAIN_HEAD_WIDTH = 128
QK_ROPE = 64
VALUE_WIDTH = 128
GRID_W = 64
SP = ("sp_0", "sp_1")
GRP_SP = ("grp", "sp_0", "sp_1")
GRP_SP_TP = ("grp", "sp_0", "sp_1", "tp")


theta = 10000.0
eps = 1e-06
limit = 7.0
slope = 1.702
STAT_LANES = 128


def turn_tables(place, heads):
    count = QK_ROPE // 4
    lane = jnp.arange(heads * QK_ROPE, dtype=jnp.int32)
    freqs = theta ** (-(lane % count).astype(jnp.float32) / count)
    by_row = (lane % QK_ROPE) < QK_ROPE // 2
    shift = jnp.where(by_row[None, :], (place // GRID_W)[:, None], (place % GRID_W)[:, None])
    angle = shift.astype(jnp.float32) * freqs[None, :]
    return jnp.cos(angle), jnp.sin(angle)


def partner_matrix(width):
    count = QK_ROPE // 4
    out = np.zeros((width, width), np.float32)
    for at in range(0, width, 2 * count):
        for i in range(count):
            out[at + count + i, at + i] = -1.0
            out[at + i, at + count + i] = 1.0
    return out


def norm_scale(values, gain):
    wide = values.astype(jnp.float32)
    return (
        wide
        * lax.rsqrt(jnp.mean(wide * wide, axis=-1, keepdims=True) + eps)
        * gain.astype(jnp.float32)
    )


def in_hbm(array):
    return pltpu.with_memory_space_constraint(array, pltpu.HBM)


def shifted(array, axis, step):
    count = lax.axis_size(axis)
    return lax.ppermute(array, axis, [(i, (i + step) % count) for i in range(count)])


GROUP = 8


def lanes_of(index, width):
    return slice(index * width, (index + 1) * width)


def prepare_body(
    index_ref,
    latent_ref,
    gain_ref,
    key_ref,
    cos_ref,
    sin_ref,
    swap_ref,
    key_matrix_ref,
    value_matrix_ref,
    plain_ref,
    turn_ref,
    sent_ref,
    shares_ref,
):
    rows, latent_width = latent_ref.shape
    sent_ref[:, :latent_width] = norm_scale(latent_ref[...], gain_ref[...]).astype(jnp.bfloat16)
    tokens = key_ref.shape[1]
    at = lax.broadcasted_iota(jnp.int32, (rows, tokens), 0) + index_ref[0] * rows
    pick = (at == lax.broadcasted_iota(jnp.int32, (rows, tokens), 1)).astype(jnp.bfloat16)
    key = lax.dot_general(
        pick, key_ref[...], (((1,), (1,)), ((), ())), preferred_element_type=jnp.float32
    )
    swapped = jnp.dot(
        key.astype(jnp.bfloat16), swap_ref[...], preferred_element_type=jnp.float32
    )
    turned = (key * cos_ref[...] + swapped * sin_ref[...]).astype(jnp.bfloat16)
    sent_ref[:, latent_width:] = jnp.concatenate((turned, jnp.zeros_like(turned)), axis=1)
    wide = key_matrix_ref.shape[1]
    depth = latent_width // 2
    matrix = jnp.where(index_ref[1] == 0, key_matrix_ref[...], value_matrix_ref[...])
    turn_wide = turn_ref.shape[1]
    half = tokens // 2
    quarter = tokens * turn_wide // (2 * wide)
    for j in range(shares_ref.shape[0]):
        shares_ref[j, :depth, :wide] = matrix[:depth, :]
        shares_ref[j, :depth, wide:] = matrix[depth:, :]
        shares_ref[j, depth : depth + half, :wide] = plain_ref[:half, :]
        shares_ref[j, depth : depth + half, wide:] = plain_ref[half:, :]
        for i in range(tokens // quarter):
            shares_ref[j, depth + half :, lanes_of(i, turn_wide)] = turn_ref[
                i * quarter : (i + 1) * quarter, :
            ]


def attend_body(
    core_ref, near_ref, other_ref, shares_ref, theirs_ref, cos_ref, sin_ref, swap_ref, out_ref, kv_ref
):
    shards = shares_ref.shape[0]
    width = shares_ref.shape[2]
    near = near_ref.shape[0]
    latent_width = width
    quarter = out_ref.shape[1]
    tokens = shards * quarter
    value_wide = width // 2
    heads = value_wide // PLAIN_HEAD_WIDTH
    scale = (PLAIN_HEAD_WIDTH + QK_ROPE) ** (-0.5)
    near_rot = near_ref[:, latent_width : latent_width + QK_ROPE]
    other_rot = other_ref[:, latent_width : latent_width + QK_ROPE]
    lane = lax.broadcasted_iota(jnp.int32, (tokens, STAT_LANES), 1)
    stats = jnp.zeros((tokens, STAT_LANES), jnp.float32)
    last = (((1,), (1,)), ((), ()))
    for j in range(shards):
        depth = latent_width // 2
        mine = shares_ref[j, :depth, :]
        other = theirs_ref[j, :depth, :]
        for first, second, base in ((mine, other, 0), (other, mine, value_wide)):
            packed = jnp.where(core_ref[0] == 0, first, second)
            matrix = jnp.concatenate((packed[:, :value_wide], packed[:, value_wide:]), axis=0)
            for rows_ref, at in ((near_ref, 0), (other_ref, near)):
                kv_ref[at : at + near, base : base + value_wide] = jnp.dot(
                    rows_ref[:, :latent_width], matrix, preferred_element_type=jnp.float32
                ).astype(jnp.bfloat16)
        at = depth
        half = tokens // 2
        plain = jnp.concatenate(
            (
                shares_ref[j, at : at + half, :value_wide],
                shares_ref[j, at : at + half, value_wide:],
            ),
            axis=0,
        )
        at += half
        raw = jnp.concatenate(
            [
                shares_ref[j, at : at + quarter, i * heads * QK_ROPE : (i + 1) * heads * QK_ROPE]
                for i in range(tokens // quarter)
            ],
            axis=0,
        )
        swapped = jnp.dot(raw, swap_ref[...], preferred_element_type=jnp.float32)
        turned = (raw.astype(jnp.float32) * cos_ref[...] + swapped * sin_ref[...]).astype(
            jnp.bfloat16
        )
        for h in range(heads):
            lo = h * PLAIN_HEAD_WIDTH
            query = plain[:, lo : lo + PLAIN_HEAD_WIDTH]
            query_rot = turned[:, h * QK_ROPE : (h + 1) * QK_ROPE]
            keys = kv_ref[:, lo : lo + PLAIN_HEAD_WIDTH]
            rotary = jnp.concatenate(
                (
                    lax.dot_general(query_rot, near_rot, last, preferred_element_type=jnp.float32),
                    lax.dot_general(query_rot, other_rot, last, preferred_element_type=jnp.float32),
                ),
                axis=1,
            )
            scores = (
                lax.dot_general(query, keys, last, preferred_element_type=jnp.float32) + rotary
            ) * scale
            peak = jnp.max(scores, axis=1, keepdims=True)
            weights = jnp.exp(scores - peak)
            total = jnp.sum(weights, axis=1, keepdims=True)
            head_values = kv_ref[:, value_wide + lo : value_wide + lo + VALUE_WIDTH]
            summed = jnp.dot(
                weights.astype(jnp.bfloat16), head_values, preferred_element_type=jnp.float32
            )
            result = (summed / total).astype(jnp.bfloat16)
            head = j * heads + h
            for i in range(shards):
                out_ref[i, :, head * VALUE_WIDTH : (head + 1) * VALUE_WIDTH] = result[
                    i * quarter : (i + 1) * quarter
                ]
            rest = peak + jnp.log(total)
            for part in range(3):
                top = rest.astype(jnp.bfloat16).astype(jnp.float32)
                rest = rest - top
                stats = jnp.where(lane == part * shards * heads + head, top, stats)
    stats = stats.astype(jnp.bfloat16)
    for i in range(shards):
        out_ref[i, :, shards * value_wide :] = stats[i * quarter : (i + 1) * quarter]


def mix_body(
    parts_ref, weight_hbm, residual_ref, gain_ref, routes_ref, hidden_ref, outgoing_ref, weight_ref, sem
):
    load = pltpu.make_async_copy(weight_hbm, weight_ref, sem)
    load.start()
    shards = parts_ref.shape[0]
    rows, model_width = residual_ref.shape
    wide = weight_ref.shape[0]
    heads = wide // VALUE_WIDTH
    sums = []
    for i in range(shards):
        stat = parts_ref[i, :, wide:].astype(jnp.float32)
        sums.append(
            stat[:, :heads] + (stat[:, heads : 2 * heads] + stat[:, 2 * heads : 3 * heads])
        )
    most = sums[0]
    for s in sums[1:]:
        most = jnp.maximum(most, s)
    shares = [jnp.exp(s - most) for s in sums]
    whole = shares[0]
    for s in shares[1:]:
        whole = whole + s
    shares = [s / whole for s in shares]
    pieces = []
    for h in range(heads):
        lo = h * VALUE_WIDTH
        piece = shares[0][:, h : h + 1] * parts_ref[0, :, lo : lo + VALUE_WIDTH].astype(jnp.float32)
        for i in range(1, shards):
            piece = piece + shares[i][:, h : h + 1] * parts_ref[
                i, :, lo : lo + VALUE_WIDTH
            ].astype(jnp.float32)
        pieces.append(piece.astype(jnp.bfloat16))
    attended = jnp.concatenate(pieces, axis=1)

    total_rows = outgoing_ref.shape[0]
    line = lax.broadcasted_iota(jnp.int32, (total_rows, rows), 0)
    named = jnp.zeros((total_rows, rows), jnp.int32)
    for k in range(routes_ref.shape[0]):
        named = named | (routes_ref[k : k + 1, :] == line // GROUP).astype(jnp.int32)
    before = (
        lax.broadcasted_iota(jnp.int32, (rows, rows), 0)
        < lax.broadcasted_iota(jnp.int32, (rows, rows), 1)
    ).astype(jnp.bfloat16)
    rank = jnp.dot(
        named.astype(jnp.float32).astype(jnp.bfloat16), before, preferred_element_type=jnp.float32
    ).astype(jnp.int32)
    table = jnp.where((named > 0) & (rank == line % GROUP), 1.0, 0.0).astype(jnp.bfloat16)

    load.wait()
    projected = jnp.dot(attended, weight_ref[...], preferred_element_type=jnp.float32)
    hidden = (residual_ref[...].astype(jnp.float32) + projected).astype(jnp.bfloat16)
    hidden_ref[...] = hidden
    normed = norm_scale(hidden, gain_ref[...]).astype(jnp.bfloat16)
    tail = model_width - outgoing_ref.shape[1]
    ends = normed[:, model_width - tail :]
    for s in range(GROUP - 1):
        of_last = jnp.where(
            (named > 0) & (rank == s) & (line % GROUP == GROUP - 1), 1.0, 0.0
        ).astype(jnp.bfloat16)
        outgoing_ref[:, lanes_of(s, tail)] = (
            jnp.dot(table, normed[:, lanes_of(s, tail)], preferred_element_type=jnp.float32)
            + jnp.dot(of_last, ends, preferred_element_type=jnp.float32)
        ).astype(jnp.bfloat16)


def expert_body(arrived_ref, *refs):
    count = (len(refs) - 5) // 3
    weights_hbm = refs[: 3 * count + 1]
    out_ref, thin_ref, down_ref, sems = refs[3 * count + 1 :]
    gate_up = weights_hbm[0].shape
    cut = weights_hbm[-1].shape[0]
    loads = []
    for i, source in enumerate(weights_hbm):
        q, m = divmod(i, 3) if i < 3 * count else (count - 1, 3)
        if m < 2:
            dst = thin_ref.at[q, m]
        elif q < count - 1:
            dst = down_ref.at[q]
        else:
            dst = down_ref.at[q, pl.ds((m - 2) * cut, cut)]
        loads.append(pltpu.make_async_copy(source, dst, sems.at[i]))
        loads[-1].start()
    rows, main = arrived_ref.shape
    model_width = gate_up[0]
    tail = model_width - main
    line = lax.broadcasted_iota(jnp.int32, (rows, rows), 0)
    column = lax.broadcasted_iota(jnp.int32, (rows, rows), 1)
    ends = jnp.zeros((rows, tail), jnp.float32)
    for s in range(GROUP - 1):
        pick = jnp.where(
            (line % GROUP == s) & (column == line - s + GROUP - 1), 1.0, 0.0
        ).astype(jnp.bfloat16)
        ends = ends + jnp.dot(
            pick, arrived_ref[:, lanes_of(s, tail)], preferred_element_type=jnp.float32
        )
    ends = ends.astype(jnp.bfloat16)
    total = jnp.zeros((rows, model_width), jnp.float32)
    for q in range(count):
        loads[3 * q].wait()
        gate_pre = jnp.dot(
            arrived_ref[...], thin_ref[q, 0, :main, :], preferred_element_type=jnp.float32
        ) + jnp.dot(ends, thin_ref[q, 0, main:, :], preferred_element_type=jnp.float32)
        loads[3 * q + 1].wait()
        up_pre = jnp.dot(
            arrived_ref[...], thin_ref[q, 1, :main, :], preferred_element_type=jnp.float32
        ) + jnp.dot(ends, thin_ref[q, 1, main:, :], preferred_element_type=jnp.float32)
        gate_pre = jnp.minimum(gate_pre, limit)
        active = (
            (jnp.clip(up_pre, -limit, limit) + 1.0) * gate_pre * jax.nn.sigmoid(slope * gate_pre)
        ).astype(jnp.bfloat16)
        loads[3 * q + 2].wait()
        if q == count - 1:
            loads[-1].wait()
        product = jnp.dot(active, down_ref[q], preferred_element_type=jnp.float32)
        total = total + product.astype(jnp.bfloat16).astype(jnp.float32)
    result = total.astype(jnp.bfloat16)
    last = result[:, main:]
    group_end = lax.broadcasted_iota(jnp.int32, (rows, tail), 0) % GROUP == GROUP - 1
    for s in range(GROUP - 1):
        pick = jnp.where(
            (line % GROUP == GROUP - 1) & (column == line - (GROUP - 1) + s), 1.0, 0.0
        ).astype(jnp.bfloat16)
        moved = jnp.dot(pick, last, preferred_element_type=jnp.float32).astype(jnp.bfloat16)
        out_ref[:, lanes_of(s, tail)] = jnp.where(
            group_end, moved.astype(jnp.float32), result[:, lanes_of(s, tail)].astype(jnp.float32)
        ).astype(jnp.bfloat16)


def combine_body(returned_ref, hidden_ref, routes_ref, weights_ref, out_ref):
    rows, model_width = hidden_ref.shape
    total_rows, main = returned_ref.shape
    tail = model_width - main
    column = lax.broadcasted_iota(jnp.int32, (rows, total_rows), 1)
    named = jnp.zeros((rows, total_rows), jnp.float32)
    weight = jnp.zeros((rows, total_rows), jnp.float32)
    for k in range(routes_ref.shape[1]):
        here = routes_ref[:, k : k + 1] == column // GROUP
        named = jnp.where(here, 1.0, named)
        weight = jnp.where(here, weights_ref[:, k : k + 1], weight)
    before = (
        lax.broadcasted_iota(jnp.int32, (rows, rows), 1)
        < lax.broadcasted_iota(jnp.int32, (rows, rows), 0)
    ).astype(jnp.bfloat16)
    rank = jnp.dot(
        before, named.astype(jnp.bfloat16), preferred_element_type=jnp.float32
    ).astype(jnp.int32)
    parts = []
    rest = weight
    for _ in range(3):
        top = rest.astype(jnp.bfloat16).astype(jnp.float32)
        rest = rest - top
        parts.append(top)

    def gathered(keep, values):
        table = jnp.concatenate([jnp.where(keep, p, 0.0) for p in parts], axis=0)
        got = jnp.dot(table.astype(jnp.bfloat16), values, preferred_element_type=jnp.float32)
        return got[:rows] + (got[rows : 2 * rows] + got[2 * rows :])

    own = (named > 0) & (rank == column % GROUP)
    out_ref[:, :main] = (
        hidden_ref[:, :main].astype(jnp.float32) + gathered(own, returned_ref[...])
    ).astype(jnp.bfloat16)
    ends = jnp.zeros((rows, tail), jnp.float32)
    for s in range(GROUP - 1):
        keep = (named > 0) & (rank == s) & (column % GROUP == GROUP - 1)
        ends = ends + gathered(keep, returned_ref[:, lanes_of(s, tail)])
    out_ref[:, main:] = (hidden_ref[:, main:].astype(jnp.float32) + ends).astype(jnp.bfloat16)


def on_device(
    query_plain,
    query_turn,
    latent,
    key_turn,
    latent_norm_scale,
    plain_key_matrix,
    value_matrix,
    residual,
    out_weight,
    ffn_gain,
    gate_weight,
    up_weight,
    down_weight,
    routes,
    route_weights,
):
    tok_dev = latent.shape[0]
    rows_dev = residual.shape[0]
    model_width = residual.shape[1]
    latent_width = latent.shape[1]
    group = lax.axis_size("tp")
    heads_dev = query_plain.shape[1] // PLAIN_HEAD_WIDTH
    place = lax.axis_index(SP) * tok_dev + jnp.arange(tok_dev, dtype=jnp.int32)
    at_tp = lax.axis_index("tp")
    at_core = lax.axis_index("sp_1")
    own_place = (
        lax.axis_index(SP) * tok_dev
        + at_tp * rows_dev
        + jnp.arange(rows_dev, dtype=jnp.int32)
    )
    own_cos, own_sin = turn_tables(own_place, 1)
    cosines, sines = turn_tables(place, heads_dev)
    share_rows = latent_width // 2 + tok_dev // 2 + tok_dev * query_turn.shape[1] // latent_width
    wide = plain_key_matrix.shape[1]
    whole = lambda *shape: pl.BlockSpec(shape, lambda i, at: (0,) * len(shape))
    sent, shares = pl.pallas_call(
        prepare_body,
        out_shape=(
            jax.ShapeDtypeStruct((rows_dev, latent_width + 2 * QK_ROPE), jnp.bfloat16),
            jax.ShapeDtypeStruct((group, share_rows, latent_width), jnp.bfloat16),
        ),
        grid_spec=pltpu.PrefetchScalarGridSpec(
            num_scalar_prefetch=1,
            grid=(1,),
            in_specs=[
                pl.BlockSpec((rows_dev, latent_width), lambda i, at: (at[0], 0)),
                whole(1, latent_width),
                whole(QK_ROPE, tok_dev),
                whole(rows_dev, QK_ROPE),
                whole(rows_dev, QK_ROPE),
                whole(QK_ROPE, QK_ROPE),
                whole(latent_width, wide),
                whole(latent_width, wide),
                whole(tok_dev, query_plain.shape[1]),
                whole(tok_dev, query_turn.shape[1]),
            ],
            out_specs=(
                whole(rows_dev, latent_width + 2 * QK_ROPE),
                whole(group, share_rows, latent_width),
            ),
        ),
        compiler_params=pltpu.CompilerParams(vmem_limit_bytes=16 << 20),
        name="prepare",
    )(
        jnp.stack((at_tp, at_core)),
        *map(
            in_hbm,
            (
                latent,
                latent_norm_scale.reshape(1, latent_width),
                key_turn.T,
                own_cos,
                own_sin,
                jnp.asarray(partner_matrix(QK_ROPE), jnp.bfloat16),
                plain_key_matrix,
                value_matrix,
                query_plain,
                query_turn,
            ),
        ),
    )
    shares = lax.all_to_all(shares, "tp", 0, 0, tiled=True)
    theirs = shifted(shares, "sp_1", 1)
    near = lax.all_gather(sent, "sp_0", axis=0, tiled=True)
    other = shifted(near, "sp_1", 1)

    parts = pl.pallas_call(
        attend_body,
        out_shape=jax.ShapeDtypeStruct((group, rows_dev, group * heads_dev * VALUE_WIDTH + STAT_LANES), jnp.bfloat16),
        in_specs=[pl.BlockSpec(memory_space=pltpu.SMEM)]
        + [pl.BlockSpec(memory_space=pltpu.VMEM)] * 7,
        scratch_shapes=[
            pltpu.VMEM((2 * near.shape[0], 2 * heads_dev * VALUE_WIDTH), jnp.bfloat16)
        ],
        compiler_params=pltpu.CompilerParams(vmem_limit_bytes=24 << 20),
        name="attend",
    )(
        at_core.reshape(1),
        near,
        other,
        shares,
        theirs,
        in_hbm(cosines),
        in_hbm(sines),
        in_hbm(jnp.asarray(partner_matrix(heads_dev * QK_ROPE), jnp.bfloat16)),
    )
    gathered = lax.all_to_all(parts, "tp", 0, 0, tiled=True)

    experts_all = lax.axis_size(SP) * gate_weight.shape[0]
    top_count = routes.shape[1]
    capacity = min(rows_dev, max(2, rows_dev * top_count * 3 // (2 * experts_all)))
    assert capacity == GROUP - 1
    main = model_width * capacity // GROUP
    vmem = pl.BlockSpec(memory_space=pltpu.VMEM)
    hbm = pl.BlockSpec(memory_space=pltpu.HBM)
    hidden, outgoing = pl.pallas_call(
        mix_body,
        out_shape=(
            jax.ShapeDtypeStruct((rows_dev, model_width), jnp.bfloat16),
            jax.ShapeDtypeStruct((experts_all * GROUP, main), jnp.bfloat16),
        ),
        in_specs=[vmem, hbm, vmem, vmem, vmem],
        scratch_shapes=[
            pltpu.VMEM(out_weight.shape, jnp.bfloat16),
            pltpu.SemaphoreType.DMA,
        ],
        compiler_params=pltpu.CompilerParams(vmem_limit_bytes=16 << 20),
        name="mix",
    )(gathered, in_hbm(out_weight), in_hbm(residual), in_hbm(ffn_gain.reshape(1, model_width)), in_hbm(routes.T))
    arrived = lax.all_to_all(
        outgoing.reshape(experts_all, GROUP, main), SP, 0, 0, tiled=True
    )

    own = (gate_weight[0], up_weight[0], down_weight[0])
    left, right = [], []
    for w in own:
        left.append(shifted(w, "tp", 1))
        right.append(shifted(w, "tp", -1))
    cut = own[2].shape[0] // 2
    far_gate = shifted(left[0], "tp", 1)
    far_up = shifted(right[1], "tp", -1)
    far_down_l = shifted(left[2][:cut], "tp", 1)
    far_down_r = shifted(right[2][cut:], "tp", -1)

    weights = []
    for quarter_weights in (own, left, right):
        weights += list(quarter_weights)
    weights += [far_gate, far_up, far_down_l, far_down_r]
    result_rows = pl.pallas_call(
        expert_body,
        out_shape=jax.ShapeDtypeStruct((experts_all * GROUP, main), jnp.bfloat16),
        in_specs=[vmem] + [hbm] * len(weights),
        scratch_shapes=[
            pltpu.VMEM((group, 2) + own[0].shape, jnp.bfloat16),
            pltpu.VMEM((group,) + own[2].shape, jnp.bfloat16),
            pltpu.SemaphoreType.DMA((len(weights),)),
        ],
        compiler_params=pltpu.CompilerParams(vmem_limit_bytes=40 << 20),
        name="expert",
    )(arrived.reshape(experts_all * GROUP, main), *map(in_hbm, weights))
    returned = lax.all_to_all(
        result_rows.reshape(experts_all, GROUP, main), SP, 0, 0, tiled=True
    )
    return pl.pallas_call(
        combine_body,
        out_shape=jax.ShapeDtypeStruct((rows_dev, model_width), jnp.bfloat16),
        compiler_params=pltpu.CompilerParams(vmem_limit_bytes=16 << 20),
        name="combine",
    )(returned.reshape(experts_all * GROUP, main), hidden, in_hbm(routes), in_hbm(route_weights))


def solution(mesh):
    torus = Mesh(
        mesh.devices.reshape(mesh.shape["grp"], 16, 2, mesh.shape["tp"]),
        ("grp", "sp_0", "sp_1", "tp"),
    )
    placed = (
        P(GRP_SP, "tp"),
        P(GRP_SP, "tp"),
        P(GRP_SP, None),
        P(GRP_SP, None),
        P(),
        P(None, "tp"),
        P(None, "tp"),
        P(GRP_SP_TP, None),
        P(),
        P(),
        P(SP, None, "tp"),
        P(SP, None, "tp"),
        P(SP, "tp", None),
        P(GRP_SP_TP, None),
        P(GRP_SP_TP, None),
    )
    return jax.shard_map(
        on_device, mesh=torus, in_specs=placed, out_specs=P(GRP_SP_TP, None), check_vma=False
    )
```

```python
import jax
import jax.numpy as jnp
import numpy as np
from jax import lax
from jax.experimental import pallas as pl
from jax.experimental.pallas import tpu as pltpu
from jax.sharding import Mesh
from jax.sharding import PartitionSpec as P

PLAIN_HEAD_WIDTH = 128
QK_ROPE = 64
VALUE_WIDTH = 128
GRID_W = 64
SP = ("sp_0", "sp_1")
GRP_SP = ("grp", "sp_0", "sp_1")
GRP_SP_TP = ("grp", "sp_0", "sp_1", "tp")


theta = 10000.0
eps = 1e-06
limit = 7.0
slope = 1.702
STAT_LANES = 128


def turn_tables(place, heads):
    count = QK_ROPE // 4
    lane = jnp.arange(heads * QK_ROPE, dtype=jnp.int32)
    freqs = theta ** (-(lane % count).astype(jnp.float32) / count)
    by_row = (lane % QK_ROPE) < QK_ROPE // 2
    shift = jnp.where(by_row[None, :], (place // GRID_W)[:, None], (place % GRID_W)[:, None])
    angle = shift.astype(jnp.float32) * freqs[None, :]
    return jnp.cos(angle), jnp.sin(angle)


def partner_matrix(width):
    count = QK_ROPE // 4
    out = np.zeros((width, width), np.float32)
    for at in range(0, width, 2 * count):
        for i in range(count):
            out[at + count + i, at + i] = -1.0
            out[at + i, at + count + i] = 1.0
    return out


def norm_scale(values, gain):
    wide = values.astype(jnp.float32)
    return (
        wide
        * lax.rsqrt(jnp.mean(wide * wide, axis=-1, keepdims=True) + eps)
        * gain.astype(jnp.float32)
    )


def in_hbm(array):
    return pltpu.with_memory_space_constraint(array, pltpu.HBM)


def shifted(array, axis, step):
    count = lax.axis_size(axis)
    return lax.ppermute(array, axis, [(i, (i + step) % count) for i in range(count)])


GROUP = 8


def lanes_of(index, width):
    return slice(index * width, (index + 1) * width)


def prepare_body(
    index_ref,
    latent_ref,
    gain_ref,
    key_ref,
    cos_ref,
    sin_ref,
    swap_ref,
    key_matrix_ref,
    value_matrix_ref,
    plain_ref,
    turn_ref,
    sent_ref,
    shares_ref,
):
    rows, latent_width = latent_ref.shape
    sent_ref[:, :latent_width] = norm_scale(latent_ref[...], gain_ref[...]).astype(jnp.bfloat16)
    tokens = key_ref.shape[1]
    at = lax.broadcasted_iota(jnp.int32, (rows, tokens), 0) + index_ref[0] * rows
    pick = (at == lax.broadcasted_iota(jnp.int32, (rows, tokens), 1)).astype(jnp.bfloat16)
    key = lax.dot_general(
        pick, key_ref[...], (((1,), (1,)), ((), ())), preferred_element_type=jnp.float32
    )
    swapped = jnp.dot(
        key.astype(jnp.bfloat16), swap_ref[...], preferred_element_type=jnp.float32
    )
    turned = (key * cos_ref[...] + swapped * sin_ref[...]).astype(jnp.bfloat16)
    sent_ref[:, latent_width:] = jnp.concatenate((turned, jnp.zeros_like(turned)), axis=1)
    wide = key_matrix_ref.shape[1]
    depth = latent_width // 2
    matrix = jnp.where(index_ref[1] == 0, key_matrix_ref[...], value_matrix_ref[...])
    turn_wide = turn_ref.shape[1]
    half = tokens // 2
    quarter = tokens * turn_wide // (2 * wide)
    for j in range(shares_ref.shape[0]):
        shares_ref[j, :depth, :wide] = matrix[:depth, :]
        shares_ref[j, :depth, wide:] = matrix[depth:, :]
        shares_ref[j, depth : depth + half, :wide] = plain_ref[:half, :]
        shares_ref[j, depth : depth + half, wide:] = plain_ref[half:, :]
        for i in range(tokens // quarter):
            shares_ref[j, depth + half :, lanes_of(i, turn_wide)] = turn_ref[
                i * quarter : (i + 1) * quarter, :
            ]


def attend_body(
    core_ref,
    near_ref,
    other_ref,
    shares_ref,
    theirs_ref,
    cos_ref,
    sin_ref,
    swap_ref,
    out_ref,
    keys_ref,
    values_ref,
):
    shards = shares_ref.shape[0]
    width = shares_ref.shape[2]
    near = near_ref.shape[0]
    latent_width = width
    quarter = out_ref.shape[1]
    tokens = shards * quarter
    value_wide = width // 2
    heads = value_wide // PLAIN_HEAD_WIDTH
    scale = (PLAIN_HEAD_WIDTH + QK_ROPE) ** (-0.5)
    for h in range(heads):
        for rows_ref, at in ((near_ref, 0), (other_ref, near)):
            keys_ref[h, at : at + near, PLAIN_HEAD_WIDTH:] = rows_ref[:, latent_width:]
    lane = lax.broadcasted_iota(jnp.int32, (tokens, STAT_LANES), 1)
    stats = jnp.zeros((tokens, STAT_LANES), jnp.float32)
    last = (((1,), (1,)), ((), ()))
    for j in range(shards):
        depth = latent_width // 2
        mine = shares_ref[j, :depth, :]
        other = theirs_ref[j, :depth, :]
        for first, second, is_key in ((mine, other, True), (other, mine, False)):
            packed = jnp.where(core_ref[0] == 0, first, second)
            matrix = jnp.concatenate((packed[:, :value_wide], packed[:, value_wide:]), axis=0)
            for rows_ref, at in ((near_ref, 0), (other_ref, near)):
                made = jnp.dot(
                    rows_ref[:, :latent_width], matrix, preferred_element_type=jnp.float32
                ).astype(jnp.bfloat16)
                if is_key:
                    for h in range(heads):
                        keys_ref[h, at : at + near, :PLAIN_HEAD_WIDTH] = made[
                            :, lanes_of(h, PLAIN_HEAD_WIDTH)
                        ]
                else:
                    values_ref[at : at + near, :] = made
        at = depth
        half = tokens // 2
        plain = jnp.concatenate(
            (
                shares_ref[j, at : at + half, :value_wide],
                shares_ref[j, at : at + half, value_wide:],
            ),
            axis=0,
        )
        at += half
        raw = jnp.concatenate(
            [
                shares_ref[j, at : at + quarter, i * heads * QK_ROPE : (i + 1) * heads * QK_ROPE]
                for i in range(tokens // quarter)
            ],
            axis=0,
        )
        swapped = jnp.dot(raw, swap_ref[...], preferred_element_type=jnp.float32)
        turned = (raw.astype(jnp.float32) * cos_ref[...] + swapped * sin_ref[...]).astype(
            jnp.bfloat16
        )
        for h in range(heads):
            lo = h * PLAIN_HEAD_WIDTH
            query_rot = turned[:, lanes_of(h, QK_ROPE)]
            query = jnp.concatenate(
                (plain[:, lo : lo + PLAIN_HEAD_WIDTH], query_rot, jnp.zeros_like(query_rot)), axis=1
            )
            scores = lax.dot_general(query, keys_ref[h], last, preferred_element_type=jnp.float32)
            peak = jnp.max(scores, axis=1, keepdims=True)
            weights = jnp.exp((scores - peak) * scale)
            total = jnp.sum(weights, axis=1, keepdims=True)
            summed = jnp.dot(
                weights.astype(jnp.bfloat16),
                values_ref[:, lanes_of(h, VALUE_WIDTH)],
                preferred_element_type=jnp.float32,
            )
            result = (summed / total).astype(jnp.bfloat16)
            head = j * heads + h
            for i in range(shards):
                out_ref[i, :, head * VALUE_WIDTH : (head + 1) * VALUE_WIDTH] = result[
                    i * quarter : (i + 1) * quarter
                ]
            rest = peak * scale + jnp.log(total)
            for part in range(3):
                top = rest.astype(jnp.bfloat16).astype(jnp.float32)
                rest = rest - top
                stats = jnp.where(lane == part * shards * heads + head, top, stats)
    stats = stats.astype(jnp.bfloat16)
    for i in range(shards):
        out_ref[i, :, shards * value_wide :] = stats[i * quarter : (i + 1) * quarter]


def mix_body(
    parts_ref, weight_hbm, residual_ref, gain_ref, routes_ref, hidden_ref, outgoing_ref, weight_ref, sems
):
    pieces = sems.shape[0]
    depth = weight_ref.shape[0] // pieces
    loads = []
    for i in range(pieces):
        part = pl.ds(i * depth, depth)
        loads.append(pltpu.make_async_copy(weight_hbm.at[part], weight_ref.at[part], sems.at[i]))
        loads[-1].start()
    shards = parts_ref.shape[0]
    rows, model_width = residual_ref.shape
    wide = weight_ref.shape[0]
    heads = wide // VALUE_WIDTH
    sums = []
    for i in range(shards):
        stat = parts_ref[i, :, wide:].astype(jnp.float32)
        sums.append(
            stat[:, :heads] + (stat[:, heads : 2 * heads] + stat[:, 2 * heads : 3 * heads])
        )
    most = sums[0]
    for s in sums[1:]:
        most = jnp.maximum(most, s)
    shares = [jnp.exp(s - most) for s in sums]
    whole = shares[0]
    for s in shares[1:]:
        whole = whole + s
    shares = [s / whole for s in shares]
    joined = []
    for h in range(heads):
        lo = h * VALUE_WIDTH
        piece = shares[0][:, h : h + 1] * parts_ref[0, :, lo : lo + VALUE_WIDTH].astype(jnp.float32)
        for i in range(1, shards):
            piece = piece + shares[i][:, h : h + 1] * parts_ref[
                i, :, lo : lo + VALUE_WIDTH
            ].astype(jnp.float32)
        joined.append(piece.astype(jnp.bfloat16))
    attended = jnp.concatenate(joined, axis=1)

    total_rows = outgoing_ref.shape[0]
    line = lax.broadcasted_iota(jnp.int32, (total_rows, rows), 0)
    named = jnp.zeros((total_rows, rows), jnp.int32)
    for k in range(routes_ref.shape[0]):
        named = named | (routes_ref[k : k + 1, :] == line // GROUP).astype(jnp.int32)
    before = (
        lax.broadcasted_iota(jnp.int32, (rows, rows), 0)
        < lax.broadcasted_iota(jnp.int32, (rows, rows), 1)
    ).astype(jnp.bfloat16)
    rank = jnp.dot(
        named.astype(jnp.float32).astype(jnp.bfloat16), before, preferred_element_type=jnp.float32
    ).astype(jnp.int32)
    table = jnp.where((named > 0) & (rank == line % GROUP), 1.0, 0.0).astype(jnp.bfloat16)

    for load in loads:
        load.wait()
    projected = jnp.dot(attended, weight_ref[...], preferred_element_type=jnp.float32)
    hidden = (residual_ref[...].astype(jnp.float32) + projected).astype(jnp.bfloat16)
    hidden_ref[...] = hidden
    normed = norm_scale(hidden, gain_ref[...]).astype(jnp.bfloat16)
    tail = model_width - outgoing_ref.shape[1]
    ends = normed[:, model_width - tail :]
    for s in range(GROUP - 1):
        of_last = jnp.where(
            (named > 0) & (rank == s) & (line % GROUP == GROUP - 1), 1.0, 0.0
        ).astype(jnp.bfloat16)
        outgoing_ref[:, lanes_of(s, tail)] = (
            jnp.dot(table, normed[:, lanes_of(s, tail)], preferred_element_type=jnp.float32)
            + jnp.dot(of_last, ends, preferred_element_type=jnp.float32)
        ).astype(jnp.bfloat16)


def expert_body(arrived_ref, *refs):
    count = (len(refs) - 5) // 3
    weights_hbm = refs[: 3 * count + 1]
    out_ref, thin_ref, down_ref, sems = refs[3 * count + 1 :]
    gate_up = weights_hbm[0].shape
    cut = weights_hbm[-1].shape[0]
    loads = []
    for i, source in enumerate(weights_hbm):
        q, m = divmod(i, 3) if i < 3 * count else (count - 1, 3)
        if m < 2:
            dst = thin_ref.at[q, m]
        elif q < count - 1:
            dst = down_ref.at[q]
        else:
            dst = down_ref.at[q, pl.ds((m - 2) * cut, cut)]
        loads.append(pltpu.make_async_copy(source, dst, sems.at[i]))
        loads[-1].start()
    rows, main = arrived_ref.shape
    model_width = gate_up[0]
    tail = model_width - main
    line = lax.broadcasted_iota(jnp.int32, (rows, rows), 0)
    column = lax.broadcasted_iota(jnp.int32, (rows, rows), 1)
    ends = jnp.zeros((rows, tail), jnp.float32)
    for s in range(GROUP - 1):
        pick = jnp.where(
            (line % GROUP == s) & (column == line - s + GROUP - 1), 1.0, 0.0
        ).astype(jnp.bfloat16)
        ends = ends + jnp.dot(
            pick, arrived_ref[:, lanes_of(s, tail)], preferred_element_type=jnp.float32
        )
    ends = ends.astype(jnp.bfloat16)
    actives = []
    for q in range(count):
        loads[3 * q].wait()
        gate_pre = jnp.dot(
            arrived_ref[...], thin_ref[q, 0, :main, :], preferred_element_type=jnp.float32
        ) + jnp.dot(ends, thin_ref[q, 0, main:, :], preferred_element_type=jnp.float32)
        loads[3 * q + 1].wait()
        up_pre = jnp.dot(
            arrived_ref[...], thin_ref[q, 1, :main, :], preferred_element_type=jnp.float32
        ) + jnp.dot(ends, thin_ref[q, 1, main:, :], preferred_element_type=jnp.float32)
        gate_pre = jnp.minimum(gate_pre, limit)
        actives.append(
            (
                (jnp.clip(up_pre, -limit, limit) + 1.0) * gate_pre * jax.nn.sigmoid(slope * gate_pre)
            ).astype(jnp.bfloat16)
        )
    for q in range(count):
        loads[3 * q + 2].wait()
    loads[-1].wait()

    def result_of(piece):
        total = jnp.zeros((rows, tail), jnp.float32)
        for q in range(count):
            product = jnp.dot(
                actives[q], down_ref[q, :, lanes_of(piece, tail)], preferred_element_type=jnp.float32
            )
            total = total + product.astype(jnp.bfloat16).astype(jnp.float32)
        return total

    last = result_of(GROUP - 1).astype(jnp.bfloat16)
    group_end = lax.broadcasted_iota(jnp.int32, (rows, tail), 0) % GROUP == GROUP - 1
    for s in range(GROUP - 1):
        pick = jnp.where(
            (line % GROUP == GROUP - 1) & (column == line - (GROUP - 1) + s), 1.0, 0.0
        ).astype(jnp.bfloat16)
        moved = jnp.dot(pick, last, preferred_element_type=jnp.float32)
        out_ref[:, lanes_of(s, tail)] = jnp.where(group_end, moved, result_of(s)).astype(
            jnp.bfloat16
        )


def combine_body(returned_ref, hidden_ref, routes_ref, weights_ref, out_ref):
    rows, model_width = hidden_ref.shape
    total_rows, main = returned_ref.shape
    tail = model_width - main
    column = lax.broadcasted_iota(jnp.int32, (rows, total_rows), 1)
    named = jnp.zeros((rows, total_rows), jnp.float32)
    weight = jnp.zeros((rows, total_rows), jnp.float32)
    for k in range(routes_ref.shape[1]):
        here = routes_ref[:, k : k + 1] == column // GROUP
        named = jnp.where(here, 1.0, named)
        weight = jnp.where(here, weights_ref[:, k : k + 1], weight)
    before = (
        lax.broadcasted_iota(jnp.int32, (rows, rows), 1)
        < lax.broadcasted_iota(jnp.int32, (rows, rows), 0)
    ).astype(jnp.bfloat16)
    rank = jnp.dot(
        before, named.astype(jnp.bfloat16), preferred_element_type=jnp.float32
    ).astype(jnp.int32)
    parts = []
    rest = weight
    for _ in range(3):
        top = rest.astype(jnp.bfloat16).astype(jnp.float32)
        rest = rest - top
        parts.append(top)

    def gathered(keep, values):
        table = jnp.concatenate([jnp.where(keep, p, 0.0) for p in parts], axis=0)
        got = jnp.dot(table.astype(jnp.bfloat16), values, preferred_element_type=jnp.float32)
        return got[:rows] + (got[rows : 2 * rows] + got[2 * rows :])

    own = (named > 0) & (rank == column % GROUP)
    out_ref[:, :main] = (
        hidden_ref[:, :main].astype(jnp.float32) + gathered(own, returned_ref[...])
    ).astype(jnp.bfloat16)
    ends = jnp.zeros((rows, tail), jnp.float32)
    for s in range(GROUP - 1):
        keep = (named > 0) & (rank == s) & (column % GROUP == GROUP - 1)
        ends = ends + gathered(keep, returned_ref[:, lanes_of(s, tail)])
    out_ref[:, main:] = (hidden_ref[:, main:].astype(jnp.float32) + ends).astype(jnp.bfloat16)


def on_device(
    query_plain,
    query_turn,
    latent,
    key_turn,
    latent_norm_scale,
    plain_key_matrix,
    value_matrix,
    residual,
    out_weight,
    ffn_gain,
    gate_weight,
    up_weight,
    down_weight,
    routes,
    route_weights,
):
    tok_dev = latent.shape[0]
    rows_dev = residual.shape[0]
    model_width = residual.shape[1]
    latent_width = latent.shape[1]
    group = lax.axis_size("tp")
    heads_dev = query_plain.shape[1] // PLAIN_HEAD_WIDTH
    place = lax.axis_index(SP) * tok_dev + jnp.arange(tok_dev, dtype=jnp.int32)
    at_tp = lax.axis_index("tp")
    at_core = lax.axis_index("sp_1")
    own_place = (
        lax.axis_index(SP) * tok_dev
        + at_tp * rows_dev
        + jnp.arange(rows_dev, dtype=jnp.int32)
    )
    own_cos, own_sin = turn_tables(own_place, 1)
    cosines, sines = turn_tables(place, heads_dev)
    share_rows = latent_width // 2 + tok_dev // 2 + tok_dev * query_turn.shape[1] // latent_width
    wide = plain_key_matrix.shape[1]
    whole = lambda *shape: pl.BlockSpec(shape, lambda i, at: (0,) * len(shape))
    sent, shares = pl.pallas_call(
        prepare_body,
        out_shape=(
            jax.ShapeDtypeStruct((rows_dev, latent_width + 2 * QK_ROPE), jnp.bfloat16),
            jax.ShapeDtypeStruct((group, share_rows, latent_width), jnp.bfloat16),
        ),
        grid_spec=pltpu.PrefetchScalarGridSpec(
            num_scalar_prefetch=1,
            grid=(1,),
            in_specs=[
                pl.BlockSpec((rows_dev, latent_width), lambda i, at: (at[0], 0)),
                whole(1, latent_width),
                whole(QK_ROPE, tok_dev),
                whole(rows_dev, QK_ROPE),
                whole(rows_dev, QK_ROPE),
                whole(QK_ROPE, QK_ROPE),
                whole(latent_width, wide),
                whole(latent_width, wide),
                whole(tok_dev, query_plain.shape[1]),
                whole(tok_dev, query_turn.shape[1]),
            ],
            out_specs=(
                whole(rows_dev, latent_width + 2 * QK_ROPE),
                whole(group, share_rows, latent_width),
            ),
        ),
        compiler_params=pltpu.CompilerParams(vmem_limit_bytes=16 << 20),
        name="prepare",
    )(
        jnp.stack((at_tp, at_core)),
        *map(
            in_hbm,
            (
                latent,
                latent_norm_scale.reshape(1, latent_width),
                key_turn.T,
                own_cos,
                own_sin,
                jnp.asarray(partner_matrix(QK_ROPE), jnp.bfloat16),
                plain_key_matrix,
                value_matrix,
                query_plain,
                query_turn,
            ),
        ),
    )
    shares = lax.all_to_all(shares, "tp", 0, 0, tiled=True)
    theirs = shifted(shares, "sp_1", 1)
    near = lax.all_gather(sent, "sp_0", axis=0, tiled=True)
    other = shifted(near, "sp_1", 1)

    parts = pl.pallas_call(
        attend_body,
        out_shape=jax.ShapeDtypeStruct((group, rows_dev, group * heads_dev * VALUE_WIDTH + STAT_LANES), jnp.bfloat16),
        in_specs=[pl.BlockSpec(memory_space=pltpu.SMEM)]
        + [pl.BlockSpec(memory_space=pltpu.VMEM)] * 7,
        scratch_shapes=[
            pltpu.VMEM((heads_dev, 2 * near.shape[0], PLAIN_HEAD_WIDTH + 2 * QK_ROPE), jnp.bfloat16),
            pltpu.VMEM((2 * near.shape[0], heads_dev * VALUE_WIDTH), jnp.bfloat16),
        ],
        compiler_params=pltpu.CompilerParams(vmem_limit_bytes=24 << 20),
        name="attend",
    )(
        at_core.reshape(1),
        near,
        other,
        shares,
        theirs,
        in_hbm(cosines),
        in_hbm(sines),
        in_hbm(jnp.asarray(partner_matrix(heads_dev * QK_ROPE), jnp.bfloat16)),
    )
    gathered = lax.all_to_all(parts, "tp", 0, 0, tiled=True)

    experts_all = lax.axis_size(SP) * gate_weight.shape[0]
    top_count = routes.shape[1]
    capacity = min(rows_dev, max(2, rows_dev * top_count * 3 // (2 * experts_all)))
    assert capacity == GROUP - 1
    main = model_width * capacity // GROUP
    vmem = pl.BlockSpec(memory_space=pltpu.VMEM)
    hbm = pl.BlockSpec(memory_space=pltpu.HBM)
    hidden, outgoing = pl.pallas_call(
        mix_body,
        out_shape=(
            jax.ShapeDtypeStruct((rows_dev, model_width), jnp.bfloat16),
            jax.ShapeDtypeStruct((experts_all * GROUP, main), jnp.bfloat16),
        ),
        in_specs=[vmem, hbm, vmem, vmem, vmem],
        scratch_shapes=[
            pltpu.VMEM(out_weight.shape, jnp.bfloat16),
            pltpu.SemaphoreType.DMA((8,)),
        ],
        compiler_params=pltpu.CompilerParams(vmem_limit_bytes=16 << 20),
        name="mix",
    )(gathered, in_hbm(out_weight), in_hbm(residual), in_hbm(ffn_gain.reshape(1, model_width)), in_hbm(routes.T))
    arrived = lax.all_to_all(
        outgoing.reshape(experts_all, GROUP, main), SP, 0, 0, tiled=True
    )

    own = (gate_weight[0], up_weight[0], down_weight[0])
    left, right = [], []
    for w in own:
        left.append(shifted(w, "tp", 1))
        right.append(shifted(w, "tp", -1))
    cut = own[2].shape[0] // 2
    far_gate = shifted(left[0], "tp", 1)
    far_up = shifted(right[1], "tp", -1)
    far_down_l = shifted(left[2][:cut], "tp", 1)
    far_down_r = shifted(right[2][cut:], "tp", -1)

    weights = []
    for quarter_weights in (own, left, right):
        weights += list(quarter_weights)
    weights += [far_gate, far_up, far_down_l, far_down_r]
    result_rows = pl.pallas_call(
        expert_body,
        out_shape=jax.ShapeDtypeStruct((experts_all * GROUP, main), jnp.bfloat16),
        in_specs=[vmem] + [hbm] * len(weights),
        scratch_shapes=[
            pltpu.VMEM((group, 2) + own[0].shape, jnp.bfloat16),
            pltpu.VMEM((group,) + own[2].shape, jnp.bfloat16),
            pltpu.SemaphoreType.DMA((len(weights),)),
        ],
        compiler_params=pltpu.CompilerParams(vmem_limit_bytes=40 << 20),
        name="expert",
    )(arrived.reshape(experts_all * GROUP, main), *map(in_hbm, weights[:-4]), *weights[-4:])
    returned = lax.all_to_all(
        result_rows.reshape(experts_all, GROUP, main), SP, 0, 0, tiled=True
    )
    return pl.pallas_call(
        combine_body,
        out_shape=jax.ShapeDtypeStruct((rows_dev, model_width), jnp.bfloat16),
        compiler_params=pltpu.CompilerParams(vmem_limit_bytes=16 << 20),
        name="combine",
    )(returned.reshape(experts_all * GROUP, main), hidden, in_hbm(routes), in_hbm(route_weights))


def solution(mesh):
    torus = Mesh(
        mesh.devices.reshape(mesh.shape["grp"], 16, 2, mesh.shape["tp"]),
        ("grp", "sp_0", "sp_1", "tp"),
    )
    placed = (
        P(GRP_SP, "tp"),
        P(GRP_SP, "tp"),
        P(GRP_SP, None),
        P(GRP_SP, None),
        P(),
        P(None, "tp"),
        P(None, "tp"),
        P(GRP_SP_TP, None),
        P(),
        P(),
        P(SP, None, "tp"),
        P(SP, None, "tp"),
        P(SP, "tp", None),
        P(GRP_SP_TP, None),
        P(GRP_SP_TP, None),
    )
    return jax.shard_map(
        on_device, mesh=torus, in_specs=placed, out_specs=P(GRP_SP_TP, None), check_vma=False
    )
```

```python
import jax
import jax.numpy as jnp
import numpy as np
from jax import lax
from jax.experimental import pallas as pl
from jax.experimental.pallas import tpu as pltpu
from jax.sharding import Mesh
from jax.sharding import PartitionSpec as P

PLAIN_HEAD_WIDTH = 128
QK_ROPE = 64
VALUE_WIDTH = 128
GRID_W = 64
SP = ("sp_0", "sp_1")
GRP_SP = ("grp", "sp_0", "sp_1")
GRP_SP_TP = ("grp", "sp_0", "sp_1", "tp")


theta = 10000.0
eps = 1e-06
limit = 7.0
slope = 1.702
STAT_LANES = 128


def turn_tables(place, heads):
    count = QK_ROPE // 4
    lane = jnp.arange(heads * QK_ROPE, dtype=jnp.int32)
    freqs = theta ** (-(lane % count).astype(jnp.float32) / count)
    by_row = (lane % QK_ROPE) < QK_ROPE // 2
    shift = jnp.where(by_row[None, :], (place // GRID_W)[:, None], (place % GRID_W)[:, None])
    angle = shift.astype(jnp.float32) * freqs[None, :]
    return jnp.cos(angle), jnp.sin(angle)


def partner_matrix(width):
    count = QK_ROPE // 4
    out = np.zeros((width, width), np.float32)
    for at in range(0, width, 2 * count):
        for i in range(count):
            out[at + count + i, at + i] = -1.0
            out[at + i, at + count + i] = 1.0
    return out


def norm_scale(values, gain):
    wide = values.astype(jnp.float32)
    return (
        wide
        * lax.rsqrt(jnp.mean(wide * wide, axis=-1, keepdims=True) + eps)
        * gain.astype(jnp.float32)
    )


def in_hbm(array):
    return pltpu.with_memory_space_constraint(array, pltpu.HBM)


def shifted(array, axis, step):
    count = lax.axis_size(axis)
    return lax.ppermute(array, axis, [(i, (i + step) % count) for i in range(count)])


GROUP = 8


def lanes_of(index, width):
    return slice(index * width, (index + 1) * width)


def prepare_body(
    index_ref,
    latent_ref,
    gain_ref,
    key_ref,
    cos_ref,
    sin_ref,
    swap_ref,
    key_matrix_ref,
    value_matrix_ref,
    plain_ref,
    turn_ref,
    sent_ref,
    shares_ref,
):
    rows, latent_width = latent_ref.shape
    sent_ref[:, :latent_width] = norm_scale(latent_ref[...], gain_ref[...]).astype(jnp.bfloat16)
    tokens = key_ref.shape[1]
    at = lax.broadcasted_iota(jnp.int32, (rows, tokens), 0) + index_ref[0] * rows
    pick = (at == lax.broadcasted_iota(jnp.int32, (rows, tokens), 1)).astype(jnp.bfloat16)
    key = lax.dot_general(
        pick, key_ref[...], (((1,), (1,)), ((), ())), preferred_element_type=jnp.float32
    )
    swapped = jnp.dot(
        key.astype(jnp.bfloat16), swap_ref[...], preferred_element_type=jnp.float32
    )
    turned = (key * cos_ref[...] + swapped * sin_ref[...]).astype(jnp.bfloat16)
    sent_ref[:, latent_width:] = jnp.concatenate((turned, jnp.zeros_like(turned)), axis=1)
    wide = key_matrix_ref.shape[1]
    depth = latent_width // 2
    matrix = jnp.where(index_ref[1] == 0, key_matrix_ref[...], value_matrix_ref[...])
    turn_wide = turn_ref.shape[1]
    half = tokens // 2
    quarter = tokens * turn_wide // (2 * wide)
    for j in range(shares_ref.shape[0]):
        shares_ref[j, :depth, :wide] = matrix[:depth, :]
        shares_ref[j, :depth, wide:] = matrix[depth:, :]
        shares_ref[j, depth : depth + half, :wide] = plain_ref[:half, :]
        shares_ref[j, depth : depth + half, wide:] = plain_ref[half:, :]
        for i in range(tokens // quarter):
            shares_ref[j, depth + half :, lanes_of(i, turn_wide)] = turn_ref[
                i * quarter : (i + 1) * quarter, :
            ]


def attend_body(
    core_ref,
    near_ref,
    other_ref,
    shares_ref,
    theirs_ref,
    cos_ref,
    sin_ref,
    swap_ref,
    out_ref,
    keys_ref,
    values_ref,
):
    shards = shares_ref.shape[0]
    width = shares_ref.shape[2]
    near = near_ref.shape[0]
    latent_width = width
    quarter = out_ref.shape[1]
    tokens = shards * quarter
    value_wide = width // 2
    heads = value_wide // PLAIN_HEAD_WIDTH
    scale = (PLAIN_HEAD_WIDTH + QK_ROPE) ** (-0.5)
    for h in range(heads):
        for rows_ref, at in ((near_ref, 0), (other_ref, near)):
            keys_ref[h, at : at + near, PLAIN_HEAD_WIDTH:] = rows_ref[:, latent_width:]
    lane = lax.broadcasted_iota(jnp.int32, (tokens, STAT_LANES), 1)
    stats = jnp.zeros((tokens, STAT_LANES), jnp.float32)
    last = (((1,), (1,)), ((), ()))
    for j in range(shards):
        depth = latent_width // 2
        mine = shares_ref[j, :depth, :]
        other = theirs_ref[j, :depth, :]
        for first, second, is_key in ((mine, other, True), (other, mine, False)):
            packed = jnp.where(core_ref[0] == 0, first, second)
            matrix = jnp.concatenate((packed[:, :value_wide], packed[:, value_wide:]), axis=0)
            for rows_ref, at in ((near_ref, 0), (other_ref, near)):
                made = jnp.dot(
                    rows_ref[:, :latent_width], matrix, preferred_element_type=jnp.float32
                ).astype(jnp.bfloat16)
                if is_key:
                    for h in range(heads):
                        keys_ref[h, at : at + near, :PLAIN_HEAD_WIDTH] = made[
                            :, lanes_of(h, PLAIN_HEAD_WIDTH)
                        ]
                else:
                    values_ref[at : at + near, :] = made
        at = depth
        half = tokens // 2
        plain = jnp.concatenate(
            (
                shares_ref[j, at : at + half, :value_wide],
                shares_ref[j, at : at + half, value_wide:],
            ),
            axis=0,
        )
        at += half
        raw = jnp.concatenate(
            [
                shares_ref[j, at : at + quarter, i * heads * QK_ROPE : (i + 1) * heads * QK_ROPE]
                for i in range(tokens // quarter)
            ],
            axis=0,
        )
        swapped = jnp.dot(raw, swap_ref[...], preferred_element_type=jnp.float32)
        turned = (raw.astype(jnp.float32) * cos_ref[...] + swapped * sin_ref[...]).astype(
            jnp.bfloat16
        )
        for h in range(heads):
            lo = h * PLAIN_HEAD_WIDTH
            query_rot = turned[:, lanes_of(h, QK_ROPE)]
            query = jnp.concatenate(
                (plain[:, lo : lo + PLAIN_HEAD_WIDTH], query_rot, jnp.zeros_like(query_rot)), axis=1
            )
            scores = lax.dot_general(query, keys_ref[h], last, preferred_element_type=jnp.float32)
            peak = jnp.max(scores, axis=1, keepdims=True)
            weights = jnp.exp((scores - peak) * scale)
            total = jnp.sum(weights, axis=1, keepdims=True)
            summed = jnp.dot(
                weights.astype(jnp.bfloat16),
                values_ref[:, lanes_of(h, VALUE_WIDTH)],
                preferred_element_type=jnp.float32,
            )
            result = (summed / total).astype(jnp.bfloat16)
            head = j * heads + h
            for i in range(shards):
                out_ref[i, :, head * VALUE_WIDTH : (head + 1) * VALUE_WIDTH] = result[
                    i * quarter : (i + 1) * quarter
                ]
            rest = peak * scale + jnp.log(total)
            for part in range(3):
                top = rest.astype(jnp.bfloat16).astype(jnp.float32)
                rest = rest - top
                stats = jnp.where(lane == part * shards * heads + head, top, stats)
    stats = stats.astype(jnp.bfloat16)
    for i in range(shards):
        out_ref[i, :, shards * value_wide :] = stats[i * quarter : (i + 1) * quarter]


def mix_body(
    parts_ref, weight_hbm, residual_ref, gain_ref, routes_ref, hidden_ref, outgoing_ref, weight_ref, sems
):
    pieces = sems.shape[0]
    depth = weight_ref.shape[0] // pieces
    loads = []
    for i in range(pieces):
        part = pl.ds(i * depth, depth)
        loads.append(pltpu.make_async_copy(weight_hbm.at[part], weight_ref.at[part], sems.at[i]))
        loads[-1].start()
    shards = parts_ref.shape[0]
    rows, model_width = residual_ref.shape
    wide = weight_ref.shape[0]
    heads = wide // VALUE_WIDTH
    sums = []
    for i in range(shards):
        stat = parts_ref[i, :, wide:].astype(jnp.float32)
        sums.append(
            stat[:, :heads] + (stat[:, heads : 2 * heads] + stat[:, 2 * heads : 3 * heads])
        )
    most = sums[0]
    for s in sums[1:]:
        most = jnp.maximum(most, s)
    shares = [jnp.exp(s - most) for s in sums]
    whole = shares[0]
    for s in shares[1:]:
        whole = whole + s
    shares = [s / whole for s in shares]
    joined = []
    for h in range(heads):
        lo = h * VALUE_WIDTH
        piece = shares[0][:, h : h + 1] * parts_ref[0, :, lo : lo + VALUE_WIDTH].astype(jnp.float32)
        for i in range(1, shards):
            piece = piece + shares[i][:, h : h + 1] * parts_ref[
                i, :, lo : lo + VALUE_WIDTH
            ].astype(jnp.float32)
        joined.append(piece.astype(jnp.bfloat16))
    attended = jnp.concatenate(joined, axis=1)

    total_rows = outgoing_ref.shape[0]
    line = lax.broadcasted_iota(jnp.int32, (total_rows, rows), 0)
    named = jnp.zeros((total_rows, rows), jnp.int32)
    for k in range(routes_ref.shape[0]):
        named = named | (routes_ref[k : k + 1, :] == line // GROUP).astype(jnp.int32)
    before = (
        lax.broadcasted_iota(jnp.int32, (rows, rows), 0)
        < lax.broadcasted_iota(jnp.int32, (rows, rows), 1)
    ).astype(jnp.bfloat16)
    rank = jnp.dot(
        named.astype(jnp.float32).astype(jnp.bfloat16), before, preferred_element_type=jnp.float32
    ).astype(jnp.int32)
    table = jnp.where((named > 0) & (rank == line % GROUP), 1.0, 0.0).astype(jnp.bfloat16)

    for load in loads:
        load.wait()
    projected = jnp.dot(attended, weight_ref[...], preferred_element_type=jnp.float32)
    hidden = (residual_ref[...].astype(jnp.float32) + projected).astype(jnp.bfloat16)
    hidden_ref[...] = hidden
    normed = norm_scale(hidden, gain_ref[...]).astype(jnp.bfloat16)
    tail = model_width - outgoing_ref.shape[1]
    ends = normed[:, model_width - tail :]
    for s in range(GROUP - 1):
        of_last = jnp.where(
            (named > 0) & (rank == s) & (line % GROUP == GROUP - 1), 1.0, 0.0
        ).astype(jnp.bfloat16)
        outgoing_ref[:, lanes_of(s, tail)] = (
            jnp.dot(table, normed[:, lanes_of(s, tail)], preferred_element_type=jnp.float32)
            + jnp.dot(of_last, ends, preferred_element_type=jnp.float32)
        ).astype(jnp.bfloat16)


def expert_body(arrived_ref, *refs):
    count = (len(refs) - 5) // 3
    weights_hbm = refs[: 3 * count + 1]
    out_ref, thin_ref, down_ref, sems = refs[3 * count + 1 :]
    gate_up = weights_hbm[0].shape
    cut = weights_hbm[-1].shape[0]
    loads = []
    for i, source in enumerate(weights_hbm):
        q, m = divmod(i, 3) if i < 3 * count else (count - 1, 3)
        if m < 2:
            dst = thin_ref.at[q, m]
        elif q < count - 1:
            dst = down_ref.at[q]
        else:
            dst = down_ref.at[q, pl.ds((m - 2) * cut, cut)]
        loads.append(pltpu.make_async_copy(source, dst, sems.at[i]))
        loads[-1].start()
    rows, main = arrived_ref.shape
    model_width = gate_up[0]
    tail = model_width - main
    line = lax.broadcasted_iota(jnp.int32, (rows, rows), 0)
    column = lax.broadcasted_iota(jnp.int32, (rows, rows), 1)
    ends = jnp.zeros((rows, tail), jnp.float32)
    for s in range(GROUP - 1):
        pick = jnp.where(
            (line % GROUP == s) & (column == line - s + GROUP - 1), 1.0, 0.0
        ).astype(jnp.bfloat16)
        ends = ends + jnp.dot(
            pick, arrived_ref[:, lanes_of(s, tail)], preferred_element_type=jnp.float32
        )
    ends = ends.astype(jnp.bfloat16)
    actives = []
    for q in range(count):
        loads[3 * q].wait()
        gate_pre = jnp.dot(
            arrived_ref[...], thin_ref[q, 0, :main, :], preferred_element_type=jnp.float32
        ) + jnp.dot(ends, thin_ref[q, 0, main:, :], preferred_element_type=jnp.float32)
        loads[3 * q + 1].wait()
        up_pre = jnp.dot(
            arrived_ref[...], thin_ref[q, 1, :main, :], preferred_element_type=jnp.float32
        ) + jnp.dot(ends, thin_ref[q, 1, main:, :], preferred_element_type=jnp.float32)
        gate_pre = jnp.minimum(gate_pre, limit)
        actives.append(
            (
                (jnp.clip(up_pre, -limit, limit) + 1.0) * gate_pre * jax.nn.sigmoid(slope * gate_pre)
            ).astype(jnp.bfloat16)
        )
    for q in range(count):
        loads[3 * q + 2].wait()
    loads[-1].wait()

    def result_of(piece):
        total = jnp.zeros((rows, tail), jnp.float32)
        for q in range(count):
            product = jnp.dot(
                actives[q], down_ref[q, :, lanes_of(piece, tail)], preferred_element_type=jnp.float32
            )
            total = total + product.astype(jnp.bfloat16).astype(jnp.float32)
        return total

    last = result_of(GROUP - 1).astype(jnp.bfloat16)
    group_end = lax.broadcasted_iota(jnp.int32, (rows, tail), 0) % GROUP == GROUP - 1
    for s in range(GROUP - 1):
        pick = jnp.where(
            (line % GROUP == GROUP - 1) & (column == line - (GROUP - 1) + s), 1.0, 0.0
        ).astype(jnp.bfloat16)
        moved = jnp.dot(pick, last, preferred_element_type=jnp.float32)
        out_ref[:, lanes_of(s, tail)] = jnp.where(group_end, moved, result_of(s)).astype(
            jnp.bfloat16
        )


def combine_body(returned_ref, hidden_ref, routes_ref, weights_ref, out_ref):
    rows, model_width = hidden_ref.shape
    total_rows, main = returned_ref.shape
    tail = model_width - main
    column = lax.broadcasted_iota(jnp.int32, (rows, total_rows), 1)
    named = jnp.zeros((rows, total_rows), jnp.float32)
    weight = jnp.zeros((rows, total_rows), jnp.float32)
    for k in range(routes_ref.shape[1]):
        here = routes_ref[:, k : k + 1] == column // GROUP
        named = jnp.where(here, 1.0, named)
        weight = jnp.where(here, weights_ref[:, k : k + 1], weight)
    before = (
        lax.broadcasted_iota(jnp.int32, (rows, rows), 1)
        < lax.broadcasted_iota(jnp.int32, (rows, rows), 0)
    ).astype(jnp.bfloat16)
    rank = jnp.dot(
        before, named.astype(jnp.bfloat16), preferred_element_type=jnp.float32
    ).astype(jnp.int32)
    parts = []
    rest = weight
    for _ in range(3):
        top = rest.astype(jnp.bfloat16).astype(jnp.float32)
        rest = rest - top
        parts.append(top)

    def gathered(keep, values):
        table = jnp.concatenate([jnp.where(keep, p, 0.0) for p in parts], axis=0)
        got = jnp.dot(table.astype(jnp.bfloat16), values, preferred_element_type=jnp.float32)
        return got[:rows] + (got[rows : 2 * rows] + got[2 * rows :])

    own = (named > 0) & (rank == column % GROUP)
    out_ref[:, :main] = (
        hidden_ref[:, :main].astype(jnp.float32) + gathered(own, returned_ref[...])
    ).astype(jnp.bfloat16)
    ends = jnp.zeros((rows, tail), jnp.float32)
    for s in range(GROUP - 1):
        keep = (named > 0) & (rank == s) & (column % GROUP == GROUP - 1)
        ends = ends + gathered(keep, returned_ref[:, lanes_of(s, tail)])
    out_ref[:, main:] = (hidden_ref[:, main:].astype(jnp.float32) + ends).astype(jnp.bfloat16)


def on_device(
    query_plain,
    query_turn,
    latent,
    key_turn,
    latent_norm_scale,
    plain_key_matrix,
    value_matrix,
    residual,
    out_weight,
    ffn_gain,
    gate_weight,
    up_weight,
    down_weight,
    routes,
    route_weights,
):
    tok_dev = latent.shape[0]
    rows_dev = residual.shape[0]
    model_width = residual.shape[1]
    latent_width = latent.shape[1]
    group = lax.axis_size("tp")
    heads_dev = query_plain.shape[1] // PLAIN_HEAD_WIDTH
    place = lax.axis_index(SP) * tok_dev + jnp.arange(tok_dev, dtype=jnp.int32)
    at_tp = lax.axis_index("tp")
    at_core = lax.axis_index("sp_1")
    own_place = (
        lax.axis_index(SP) * tok_dev
        + at_tp * rows_dev
        + jnp.arange(rows_dev, dtype=jnp.int32)
    )
    own_cos, own_sin = turn_tables(own_place, 1)
    cosines, sines = turn_tables(place, heads_dev)
    share_rows = latent_width // 2 + tok_dev // 2 + tok_dev * query_turn.shape[1] // latent_width
    wide = plain_key_matrix.shape[1]
    whole = lambda *shape: pl.BlockSpec(shape, lambda i, at: (0,) * len(shape))
    sent, shares = pl.pallas_call(
        prepare_body,
        out_shape=(
            jax.ShapeDtypeStruct((rows_dev, latent_width + 2 * QK_ROPE), jnp.bfloat16),
            jax.ShapeDtypeStruct((group, share_rows, latent_width), jnp.bfloat16),
        ),
        grid_spec=pltpu.PrefetchScalarGridSpec(
            num_scalar_prefetch=1,
            grid=(1,),
            in_specs=[
                pl.BlockSpec((rows_dev, latent_width), lambda i, at: (at[0], 0)),
                whole(latent_width),
                whole(QK_ROPE, tok_dev),
                whole(rows_dev, QK_ROPE),
                whole(rows_dev, QK_ROPE),
                whole(QK_ROPE, QK_ROPE),
                whole(latent_width, wide),
                whole(latent_width, wide),
                whole(tok_dev, query_plain.shape[1]),
                whole(tok_dev, query_turn.shape[1]),
            ],
            out_specs=(
                whole(rows_dev, latent_width + 2 * QK_ROPE),
                whole(group, share_rows, latent_width),
            ),
        ),
        compiler_params=pltpu.CompilerParams(vmem_limit_bytes=16 << 20),
        name="prepare",
    )(
        jnp.stack((at_tp, at_core)),
        *map(
            in_hbm,
            (
                latent,
                latent_norm_scale,
                key_turn.T,
                own_cos,
                own_sin,
                jnp.asarray(partner_matrix(QK_ROPE), jnp.bfloat16),
                plain_key_matrix,
                value_matrix,
                query_plain,
                query_turn,
            ),
        ),
    )
    shares = lax.all_to_all(shares, "tp", 0, 0, tiled=True)
    theirs = shifted(shares, "sp_1", 1)
    near = lax.all_gather(sent, "sp_0", axis=0, tiled=True)
    other = shifted(near, "sp_1", 1)

    parts = pl.pallas_call(
        attend_body,
        out_shape=pltpu.HBM(
            (group, rows_dev, group * heads_dev * VALUE_WIDTH + STAT_LANES), jnp.bfloat16
        ),
        in_specs=[pl.BlockSpec(memory_space=pltpu.SMEM)]
        + [pl.BlockSpec(memory_space=pltpu.VMEM)] * 7,
        scratch_shapes=[
            pltpu.VMEM((heads_dev, 2 * near.shape[0], PLAIN_HEAD_WIDTH + 2 * QK_ROPE), jnp.bfloat16),
            pltpu.VMEM((2 * near.shape[0], heads_dev * VALUE_WIDTH), jnp.bfloat16),
        ],
        compiler_params=pltpu.CompilerParams(vmem_limit_bytes=24 << 20),
        name="attend",
    )(
        at_core.reshape(1),
        near,
        other,
        shares,
        theirs,
        in_hbm(cosines),
        in_hbm(sines),
        in_hbm(jnp.asarray(partner_matrix(heads_dev * QK_ROPE), jnp.bfloat16)),
    )
    gathered = lax.all_to_all(parts, "tp", 0, 0, tiled=True)

    experts_all = lax.axis_size(SP) * gate_weight.shape[0]
    top_count = routes.shape[1]
    capacity = min(rows_dev, max(2, rows_dev * top_count * 3 // (2 * experts_all)))
    assert capacity == GROUP - 1
    main = model_width * capacity // GROUP
    vmem = pl.BlockSpec(memory_space=pltpu.VMEM)
    hbm = pl.BlockSpec(memory_space=pltpu.HBM)
    hidden, outgoing = pl.pallas_call(
        mix_body,
        out_shape=(
            jax.ShapeDtypeStruct((rows_dev, model_width), jnp.bfloat16),
            pltpu.HBM((experts_all * GROUP, main), jnp.bfloat16),
        ),
        in_specs=[vmem, hbm, vmem, vmem, vmem],
        scratch_shapes=[
            pltpu.VMEM(out_weight.shape, jnp.bfloat16),
            pltpu.SemaphoreType.DMA((8,)),
        ],
        compiler_params=pltpu.CompilerParams(vmem_limit_bytes=16 << 20),
        name="mix",
    )(
        gathered,
        in_hbm(out_weight),
        in_hbm(residual),
        in_hbm(ffn_gain),
        in_hbm(routes.T),
    )
    arrived = lax.all_to_all(
        outgoing.reshape(experts_all, GROUP, main), SP, 0, 0, tiled=True
    )

    own = (gate_weight[0], up_weight[0], down_weight[0])
    left, right = [], []
    for w in own:
        left.append(shifted(w, "tp", 1))
        right.append(shifted(w, "tp", -1))
    cut = own[2].shape[0] // 2
    far_gate = shifted(left[0], "tp", 1)
    far_up = shifted(right[1], "tp", -1)
    far_down_l = shifted(left[2][:cut], "tp", 1)
    far_down_r = shifted(right[2][cut:], "tp", -1)

    weights = []
    for gate_w, up_w, down_w in (own, left, right):
        weights += [gate_w, up_w, down_w]
    weights += [far_gate, far_up, far_down_l, far_down_r]
    result_rows = pl.pallas_call(
        expert_body,
        out_shape=pltpu.HBM((experts_all * GROUP, main), jnp.bfloat16),
        in_specs=[vmem] + [hbm] * len(weights),
        scratch_shapes=[
            pltpu.VMEM((group, 2) + own[0].shape, jnp.bfloat16),
            pltpu.VMEM((group,) + own[2].shape, jnp.bfloat16),
            pltpu.SemaphoreType.DMA((len(weights),)),
        ],
        compiler_params=pltpu.CompilerParams(vmem_limit_bytes=40 << 20),
        name="expert",
    )(arrived.reshape(experts_all * GROUP, main), *map(in_hbm, weights))
    returned = lax.all_to_all(
        result_rows.reshape(experts_all, GROUP, main), SP, 0, 0, tiled=True
    )
    return pl.pallas_call(
        combine_body,
        out_shape=jax.ShapeDtypeStruct((rows_dev, model_width), jnp.bfloat16),
        compiler_params=pltpu.CompilerParams(vmem_limit_bytes=16 << 20),
        name="combine",
    )(returned.reshape(experts_all * GROUP, main), hidden, in_hbm(routes), in_hbm(route_weights))


def solution(mesh):
    torus = Mesh(
        mesh.devices.reshape(mesh.shape["grp"], 16, 2, mesh.shape["tp"]),
        ("grp", "sp_0", "sp_1", "tp"),
    )
    placed = (
        P(GRP_SP, "tp"),
        P(GRP_SP, "tp"),
        P(GRP_SP, None),
        P(GRP_SP, None),
        P(),
        P(None, "tp"),
        P(None, "tp"),
        P(GRP_SP_TP, None),
        P(),
        P(),
        P(SP, None, "tp"),
        P(SP, None, "tp"),
        P(SP, "tp", None),
        P(GRP_SP_TP, None),
        P(GRP_SP_TP, None),
    )
    return jax.shard_map(
        on_device, mesh=torus, in_specs=placed, out_specs=P(GRP_SP_TP, None), check_vma=False
    )
```

```python
import jax
import jax.numpy as jnp
import numpy as np
from jax import lax
from jax.experimental import pallas as pl
from jax.experimental.pallas import tpu as pltpu
from jax.sharding import Mesh
from jax.sharding import PartitionSpec as P

PLAIN_HEAD_WIDTH = 128
QK_ROPE = 64
VALUE_WIDTH = 128
GRID_W = 64
SP = ("sp_0", "sp_1")
GRP_SP = ("grp", "sp_0", "sp_1")
GRP_SP_TP = ("grp", "sp_0", "sp_1", "tp")


theta = 10000.0
eps = 1e-06
limit = 7.0
slope = 1.702
STAT_LANES = 128


def turn_tables(place, heads):
    count = QK_ROPE // 4
    lane = jnp.arange(heads * QK_ROPE, dtype=jnp.int32)
    freqs = theta ** (-(lane % count).astype(jnp.float32) / count)
    by_row = (lane % QK_ROPE) < QK_ROPE // 2
    shift = jnp.where(by_row[None, :], (place // GRID_W)[:, None], (place % GRID_W)[:, None])
    angle = shift.astype(jnp.float32) * freqs[None, :]
    return jnp.cos(angle), jnp.sin(angle)


def partner_matrix(width):
    count = QK_ROPE // 4
    out = np.zeros((width, width), np.float32)
    for at in range(0, width, 2 * count):
        for i in range(count):
            out[at + count + i, at + i] = -1.0
            out[at + i, at + count + i] = 1.0
    return out


def norm_scale(values, gain):
    wide = values.astype(jnp.float32)
    return (
        wide
        * lax.rsqrt(jnp.mean(wide * wide, axis=-1, keepdims=True) + eps)
        * gain.astype(jnp.float32)
    )


def in_hbm(array):
    return pltpu.with_memory_space_constraint(array, pltpu.HBM)


def shifted(array, axis, step):
    count = lax.axis_size(axis)
    return lax.ppermute(array, axis, [(i, (i + step) % count) for i in range(count)])


GROUP = 8


def lanes_of(index, width):
    return slice(index * width, (index + 1) * width)


def stage_body(*refs):
    count = (len(refs) - 1) // 2
    sems = refs[-1]
    pieces = sems.shape[1]
    loads = []
    for n in range(count):
        depth = refs[count + n].shape[0] // pieces
        for i in range(pieces):
            part = pl.ds(i * depth, depth)
            loads.append(
                pltpu.make_async_copy(refs[n].at[part], refs[count + n].at[part], sems.at[n, i])
            )
            loads[-1].start()
    for load in loads:
        load.wait()


def staged(arrays, rows):
    hbm = pl.BlockSpec(memory_space=pltpu.HBM)
    vmem = pl.BlockSpec(memory_space=pltpu.VMEM)
    return pl.pallas_call(
        stage_body,
        out_shape=tuple(pltpu.VMEM((rows,) + a.shape[1:], a.dtype) for a in arrays),
        in_specs=[hbm] * len(arrays),
        out_specs=(vmem,) * len(arrays),
        scratch_shapes=[pltpu.SemaphoreType.DMA((len(arrays), 4))],
        compiler_params=pltpu.CompilerParams(vmem_limit_bytes=16 << 20),
    )(*map(in_hbm, arrays))


def prepare_body(
    index_ref,
    latent_ref,
    gain_ref,
    key_ref,
    cos_ref,
    sin_ref,
    swap_ref,
    key_matrix_ref,
    value_matrix_ref,
    plain_ref,
    turn_ref,
    sent_ref,
    shares_ref,
):
    rows, latent_width = latent_ref.shape
    sent_ref[:, :latent_width] = norm_scale(latent_ref[...], gain_ref[...]).astype(jnp.bfloat16)
    tokens = key_ref.shape[1]
    at = lax.broadcasted_iota(jnp.int32, (rows, tokens), 0) + index_ref[0] * rows
    pick = (at == lax.broadcasted_iota(jnp.int32, (rows, tokens), 1)).astype(jnp.bfloat16)
    key = lax.dot_general(
        pick, key_ref[...], (((1,), (1,)), ((), ())), preferred_element_type=jnp.float32
    )
    swapped = jnp.dot(
        key.astype(jnp.bfloat16), swap_ref[...], preferred_element_type=jnp.float32
    )
    turned = (key * cos_ref[...] + swapped * sin_ref[...]).astype(jnp.bfloat16)
    sent_ref[:, latent_width:] = jnp.concatenate((turned, jnp.zeros_like(turned)), axis=1)
    wide = key_matrix_ref.shape[1]
    depth = latent_width // 2
    matrix = jnp.where(index_ref[1] == 0, key_matrix_ref[...], value_matrix_ref[...])
    turn_wide = turn_ref.shape[1]
    half = tokens // 2
    quarter = tokens * turn_wide // (2 * wide)
    for j in range(shares_ref.shape[0]):
        shares_ref[j, :depth, :wide] = matrix[:depth, :]
        shares_ref[j, :depth, wide:] = matrix[depth:, :]
        shares_ref[j, depth : depth + half, :wide] = plain_ref[:half, :]
        shares_ref[j, depth : depth + half, wide:] = plain_ref[half:, :]
        for i in range(tokens // quarter):
            shares_ref[j, depth + half :, lanes_of(i, turn_wide)] = turn_ref[
                i * quarter : (i + 1) * quarter, :
            ]


def attend_body(
    core_ref,
    near_ref,
    other_ref,
    shares_ref,
    theirs_ref,
    cos_ref,
    sin_ref,
    swap_ref,
    out_ref,
    keys_ref,
    values_ref,
):
    shards = shares_ref.shape[0]
    width = shares_ref.shape[2]
    near = near_ref.shape[0]
    latent_width = width
    quarter = out_ref.shape[1]
    tokens = shards * quarter
    value_wide = width // 2
    heads = value_wide // PLAIN_HEAD_WIDTH
    scale = (PLAIN_HEAD_WIDTH + QK_ROPE) ** (-0.5)
    for h in range(heads):
        for rows_ref, at in ((near_ref, 0), (other_ref, near)):
            keys_ref[h, at : at + near, PLAIN_HEAD_WIDTH:] = rows_ref[:, latent_width:]
    lane = lax.broadcasted_iota(jnp.int32, (tokens, STAT_LANES), 1)
    stats = jnp.zeros((tokens, STAT_LANES), jnp.float32)
    last = (((1,), (1,)), ((), ()))
    for j in range(shards):
        depth = latent_width // 2
        mine = shares_ref[j, :depth, :]
        other = theirs_ref[j, :depth, :]
        for first, second, is_key in ((mine, other, True), (other, mine, False)):
            packed = jnp.where(core_ref[0] == 0, first, second)
            matrix = jnp.concatenate((packed[:, :value_wide], packed[:, value_wide:]), axis=0)
            for rows_ref, at in ((near_ref, 0), (other_ref, near)):
                made = jnp.dot(
                    rows_ref[:, :latent_width], matrix, preferred_element_type=jnp.float32
                ).astype(jnp.bfloat16)
                if is_key:
                    for h in range(heads):
                        keys_ref[h, at : at + near, :PLAIN_HEAD_WIDTH] = made[
                            :, lanes_of(h, PLAIN_HEAD_WIDTH)
                        ]
                else:
                    values_ref[at : at + near, :] = made
        at = depth
        half = tokens // 2
        plain = jnp.concatenate(
            (
                shares_ref[j, at : at + half, :value_wide],
                shares_ref[j, at : at + half, value_wide:],
            ),
            axis=0,
        )
        at += half
        raw = jnp.concatenate(
            [
                shares_ref[j, at : at + quarter, i * heads * QK_ROPE : (i + 1) * heads * QK_ROPE]
                for i in range(tokens // quarter)
            ],
            axis=0,
        )
        swapped = jnp.dot(raw, swap_ref[...], preferred_element_type=jnp.float32)
        turned = (raw.astype(jnp.float32) * cos_ref[...] + swapped * sin_ref[...]).astype(
            jnp.bfloat16
        )
        for h in range(heads):
            lo = h * PLAIN_HEAD_WIDTH
            query_rot = turned[:, lanes_of(h, QK_ROPE)]
            query = jnp.concatenate(
                (plain[:, lo : lo + PLAIN_HEAD_WIDTH], query_rot, jnp.zeros_like(query_rot)), axis=1
            )
            scores = lax.dot_general(query, keys_ref[h], last, preferred_element_type=jnp.float32)
            peak = jnp.max(scores, axis=1, keepdims=True)
            weights = jnp.exp((scores - peak) * scale)
            total = jnp.sum(weights, axis=1, keepdims=True)
            summed = jnp.dot(
                weights.astype(jnp.bfloat16),
                values_ref[:, lanes_of(h, VALUE_WIDTH)],
                preferred_element_type=jnp.float32,
            )
            result = (summed / total).astype(jnp.bfloat16)
            head = j * heads + h
            for i in range(shards):
                out_ref[i, :, head * VALUE_WIDTH : (head + 1) * VALUE_WIDTH] = result[
                    i * quarter : (i + 1) * quarter
                ]
            rest = peak * scale + jnp.log(total)
            for part in range(3):
                top = rest.astype(jnp.bfloat16).astype(jnp.float32)
                rest = rest - top
                stats = jnp.where(lane == part * shards * heads + head, top, stats)
    stats = stats.astype(jnp.bfloat16)
    for i in range(shards):
        out_ref[i, :, shards * value_wide :] = stats[i * quarter : (i + 1) * quarter]


def mix_body(
    parts_ref,
    near_ref,
    weight_hbm,
    residual_ref,
    gain_ref,
    routes_ref,
    hidden_ref,
    outgoing_ref,
    weight_ref,
    sems,
):
    pieces = sems.shape[0]
    depth = weight_ref.shape[0] // pieces
    above = near_ref.shape[0]
    loads = []
    for i in range(pieces):
        source = weight_hbm.at[pl.ds(above + i * depth, depth)]
        loads.append(
            pltpu.make_async_copy(source, weight_ref.at[pl.ds(i * depth, depth)], sems.at[i])
        )
        loads[-1].start()
    shards = parts_ref.shape[0]
    rows, model_width = residual_ref.shape
    wide = weight_hbm.shape[0]
    heads = wide // VALUE_WIDTH
    sums = []
    for i in range(shards):
        stat = parts_ref[i, :, wide:].astype(jnp.float32)
        sums.append(
            stat[:, :heads] + (stat[:, heads : 2 * heads] + stat[:, 2 * heads : 3 * heads])
        )
    most = sums[0]
    for s in sums[1:]:
        most = jnp.maximum(most, s)
    shares = [jnp.exp(s - most) for s in sums]
    whole = shares[0]
    for s in shares[1:]:
        whole = whole + s
    shares = [s / whole for s in shares]
    joined = []
    for h in range(heads):
        lo = h * VALUE_WIDTH
        piece = shares[0][:, h : h + 1] * parts_ref[0, :, lo : lo + VALUE_WIDTH].astype(jnp.float32)
        for i in range(1, shards):
            piece = piece + shares[i][:, h : h + 1] * parts_ref[
                i, :, lo : lo + VALUE_WIDTH
            ].astype(jnp.float32)
        joined.append(piece.astype(jnp.bfloat16))
    attended = jnp.concatenate(joined, axis=1)

    total_rows = outgoing_ref.shape[0]
    line = lax.broadcasted_iota(jnp.int32, (total_rows, rows), 0)
    named = jnp.zeros((total_rows, rows), jnp.int32)
    for k in range(routes_ref.shape[0]):
        named = named | (routes_ref[k : k + 1, :] == line // GROUP).astype(jnp.int32)
    before = (
        lax.broadcasted_iota(jnp.int32, (rows, rows), 0)
        < lax.broadcasted_iota(jnp.int32, (rows, rows), 1)
    ).astype(jnp.bfloat16)
    rank = jnp.dot(
        named.astype(jnp.float32).astype(jnp.bfloat16), before, preferred_element_type=jnp.float32
    ).astype(jnp.int32)
    table = jnp.where((named > 0) & (rank == line % GROUP), 1.0, 0.0).astype(jnp.bfloat16)

    projected = jnp.dot(attended[:, :above], near_ref[...], preferred_element_type=jnp.float32)
    for load in loads:
        load.wait()
    projected = projected + jnp.dot(
        attended[:, above:], weight_ref[...], preferred_element_type=jnp.float32
    )
    hidden = (residual_ref[...].astype(jnp.float32) + projected).astype(jnp.bfloat16)
    hidden_ref[...] = hidden
    normed = norm_scale(hidden, gain_ref[...]).astype(jnp.bfloat16)
    tail = model_width - outgoing_ref.shape[1]
    ends = normed[:, model_width - tail :]
    for s in range(GROUP - 1):
        of_last = jnp.where(
            (named > 0) & (rank == s) & (line % GROUP == GROUP - 1), 1.0, 0.0
        ).astype(jnp.bfloat16)
        outgoing_ref[:, lanes_of(s, tail)] = (
            jnp.dot(table, normed[:, lanes_of(s, tail)], preferred_element_type=jnp.float32)
            + jnp.dot(of_last, ends, preferred_element_type=jnp.float32)
        ).astype(jnp.bfloat16)


def expert_body(arrived_ref, *refs):
    out_ref, gates_ref, ups_ref, down_ref, sems = refs[-5:]
    own_gate_ref, own_up_ref, *sources = refs[:-5]
    count = down_ref.shape[0]
    wanted = []
    for q in range(count):
        wanted.append((gates_ref.at[q - 1], ups_ref.at[q - 1], down_ref.at[q]))
    cut = sources[7].shape[0]
    long = sources[8].shape[0]
    short = sources[9].shape[0]
    targets = [
        ("down", 0, wanted[0][2]),
        ("gate", 1, wanted[1][0]),
        ("down", 1, wanted[1][2]),
        ("gate", 2, wanted[2][0]),
        ("down", 2, wanted[2][2]),
        ("gate", 3, wanted[3][0]),
        ("down", 3, down_ref.at[3, pl.ds(0, cut)]),
        ("down", 3, down_ref.at[3, pl.ds(cut, cut)]),
    ]
    for q in range(1, count):
        targets.append(("up", q, ups_ref.at[q - 1, pl.ds(0, long)]))
        targets.append(("up", q, ups_ref.at[q - 1, pl.ds(long, short)]))
    loads = {}
    for i, (source, (kind, q, target)) in enumerate(zip(sources, targets, strict=True)):
        load = pltpu.make_async_copy(source, target, sems.at[i])
        load.start()
        loads.setdefault((kind, q), []).append(load)

    def ready(kind, q):
        for load in loads.pop((kind, q), ()):
            load.wait()

    rows, main = arrived_ref.shape
    model_width = own_gate_ref.shape[0]
    tail = model_width - main
    line = lax.broadcasted_iota(jnp.int32, (rows, rows), 0)
    column = lax.broadcasted_iota(jnp.int32, (rows, rows), 1)
    ends = jnp.zeros((rows, tail), jnp.float32)
    for s in range(GROUP - 1):
        pick = jnp.where(
            (line % GROUP == s) & (column == line - s + GROUP - 1), 1.0, 0.0
        ).astype(jnp.bfloat16)
        ends = ends + jnp.dot(
            pick, arrived_ref[:, lanes_of(s, tail)], preferred_element_type=jnp.float32
        )
    ends = ends.astype(jnp.bfloat16)
    actives = []
    for q in range(count):
        gate_ref = gates_ref.at[q - 1] if q else own_gate_ref
        up_ref = ups_ref.at[q - 1] if q else own_up_ref
        ready("gate", q)
        gate_pre = jnp.dot(
            arrived_ref[...], gate_ref[:main, :], preferred_element_type=jnp.float32
        ) + jnp.dot(ends, gate_ref[main:, :], preferred_element_type=jnp.float32)
        ready("up", q)
        up_pre = jnp.dot(
            arrived_ref[...], up_ref[:main, :], preferred_element_type=jnp.float32
        ) + jnp.dot(ends, up_ref[main:, :], preferred_element_type=jnp.float32)
        gate_pre = jnp.minimum(gate_pre, limit)
        actives.append(
            (
                (jnp.clip(up_pre, -limit, limit) + 1.0) * gate_pre * jax.nn.sigmoid(slope * gate_pre)
            ).astype(jnp.bfloat16)
        )
    for q in range(count):
        ready("down", q)

    def result_of(piece):
        total = jnp.zeros((rows, tail), jnp.float32)
        for q in range(count):
            product = jnp.dot(
                actives[q], down_ref[q, :, lanes_of(piece, tail)], preferred_element_type=jnp.float32
            )
            total = total + product.astype(jnp.bfloat16).astype(jnp.float32)
        return total

    last = result_of(GROUP - 1).astype(jnp.bfloat16)
    group_end = lax.broadcasted_iota(jnp.int32, (rows, tail), 0) % GROUP == GROUP - 1
    for s in range(GROUP - 1):
        pick = jnp.where(
            (line % GROUP == GROUP - 1) & (column == line - (GROUP - 1) + s), 1.0, 0.0
        ).astype(jnp.bfloat16)
        moved = jnp.dot(pick, last, preferred_element_type=jnp.float32)
        out_ref[:, lanes_of(s, tail)] = jnp.where(group_end, moved, result_of(s)).astype(
            jnp.bfloat16
        )


def combine_body(returned_ref, hidden_ref, routes_ref, weights_ref, out_ref):
    rows, model_width = hidden_ref.shape
    total_rows, main = returned_ref.shape
    tail = model_width - main
    column = lax.broadcasted_iota(jnp.int32, (rows, total_rows), 1)
    named = jnp.zeros((rows, total_rows), jnp.float32)
    weight = jnp.zeros((rows, total_rows), jnp.float32)
    for k in range(routes_ref.shape[1]):
        here = routes_ref[:, k : k + 1] == column // GROUP
        named = jnp.where(here, 1.0, named)
        weight = jnp.where(here, weights_ref[:, k : k + 1], weight)
    before = (
        lax.broadcasted_iota(jnp.int32, (rows, rows), 1)
        < lax.broadcasted_iota(jnp.int32, (rows, rows), 0)
    ).astype(jnp.bfloat16)
    rank = jnp.dot(
        before, named.astype(jnp.bfloat16), preferred_element_type=jnp.float32
    ).astype(jnp.int32)
    parts = []
    rest = weight
    for _ in range(3):
        top = rest.astype(jnp.bfloat16).astype(jnp.float32)
        rest = rest - top
        parts.append(top)

    def gathered(keep, values):
        table = jnp.concatenate([jnp.where(keep, p, 0.0) for p in parts], axis=0)
        got = jnp.dot(table.astype(jnp.bfloat16), values, preferred_element_type=jnp.float32)
        return got[:rows] + (got[rows : 2 * rows] + got[2 * rows :])

    own = (named > 0) & (rank == column % GROUP)
    out_ref[:, :main] = (
        hidden_ref[:, :main].astype(jnp.float32) + gathered(own, returned_ref[...])
    ).astype(jnp.bfloat16)
    ends = jnp.zeros((rows, tail), jnp.float32)
    for s in range(GROUP - 1):
        keep = (named > 0) & (rank == s) & (column % GROUP == GROUP - 1)
        ends = ends + gathered(keep, returned_ref[:, lanes_of(s, tail)])
    out_ref[:, main:] = (hidden_ref[:, main:].astype(jnp.float32) + ends).astype(jnp.bfloat16)


def on_device(
    query_plain,
    query_turn,
    latent,
    key_turn,
    latent_norm_scale,
    plain_key_matrix,
    value_matrix,
    residual,
    out_weight,
    ffn_gain,
    gate_weight,
    up_weight,
    down_weight,
    routes,
    route_weights,
):
    tok_dev = latent.shape[0]
    rows_dev = residual.shape[0]
    model_width = residual.shape[1]
    latent_width = latent.shape[1]
    group = lax.axis_size("tp")
    heads_dev = query_plain.shape[1] // PLAIN_HEAD_WIDTH
    place = lax.axis_index(SP) * tok_dev + jnp.arange(tok_dev, dtype=jnp.int32)
    at_tp = lax.axis_index("tp")
    at_core = lax.axis_index("sp_1")
    own_place = (
        lax.axis_index(SP) * tok_dev
        + at_tp * rows_dev
        + jnp.arange(rows_dev, dtype=jnp.int32)
    )
    own_cos, own_sin = turn_tables(own_place, 1)
    cosines, sines = turn_tables(place, heads_dev)
    share_rows = latent_width // 2 + tok_dev // 2 + tok_dev * query_turn.shape[1] // latent_width
    wide = plain_key_matrix.shape[1]
    whole = lambda *shape: pl.BlockSpec(shape, lambda i, at: (0,) * len(shape))
    sent, shares = pl.pallas_call(
        prepare_body,
        out_shape=(
            jax.ShapeDtypeStruct((rows_dev, latent_width + 2 * QK_ROPE), jnp.bfloat16),
            jax.ShapeDtypeStruct((group, share_rows, latent_width), jnp.bfloat16),
        ),
        grid_spec=pltpu.PrefetchScalarGridSpec(
            num_scalar_prefetch=1,
            grid=(1,),
            in_specs=[
                pl.BlockSpec((rows_dev, latent_width), lambda i, at: (at[0], 0)),
                whole(latent_width),
                whole(QK_ROPE, tok_dev),
                whole(rows_dev, QK_ROPE),
                whole(rows_dev, QK_ROPE),
                whole(QK_ROPE, QK_ROPE),
                whole(latent_width, wide),
                whole(latent_width, wide),
                whole(tok_dev, query_plain.shape[1]),
                whole(tok_dev, query_turn.shape[1]),
            ],
            out_specs=(
                whole(rows_dev, latent_width + 2 * QK_ROPE),
                whole(group, share_rows, latent_width),
            ),
        ),
        compiler_params=pltpu.CompilerParams(vmem_limit_bytes=16 << 20),
        name="prepare",
    )(
        jnp.stack((at_tp, at_core)),
        *map(
            in_hbm,
            (
                latent,
                latent_norm_scale,
                key_turn.T,
                own_cos,
                own_sin,
                jnp.asarray(partner_matrix(QK_ROPE), jnp.bfloat16),
                plain_key_matrix,
                value_matrix,
                query_plain,
                query_turn,
            ),
        ),
    )
    shares = lax.all_to_all(shares, "tp", 0, 0, tiled=True)
    theirs = shifted(shares, "sp_1", 1)
    near = lax.all_gather(sent, "sp_0", axis=0, tiled=True)
    other = shifted(near, "sp_1", 1)

    parts = pl.pallas_call(
        attend_body,
        out_shape=pltpu.HBM(
            (group, rows_dev, group * heads_dev * VALUE_WIDTH + STAT_LANES), jnp.bfloat16
        ),
        in_specs=[pl.BlockSpec(memory_space=pltpu.SMEM)]
        + [pl.BlockSpec(memory_space=pltpu.VMEM)] * 7,
        scratch_shapes=[
            pltpu.VMEM((heads_dev, 2 * near.shape[0], PLAIN_HEAD_WIDTH + 2 * QK_ROPE), jnp.bfloat16),
            pltpu.VMEM((2 * near.shape[0], heads_dev * VALUE_WIDTH), jnp.bfloat16),
        ],
        compiler_params=pltpu.CompilerParams(vmem_limit_bytes=24 << 20),
        name="attend",
    )(
        at_core.reshape(1),
        near,
        other,
        shares,
        theirs,
        in_hbm(cosines),
        in_hbm(sines),
        in_hbm(jnp.asarray(partner_matrix(heads_dev * QK_ROPE), jnp.bfloat16)),
    )
    gathered = lax.all_to_all(parts, "tp", 0, 0, tiled=True)

    experts_all = lax.axis_size(SP) * gate_weight.shape[0]
    top_count = routes.shape[1]
    capacity = min(rows_dev, max(2, rows_dev * top_count * 3 // (2 * experts_all)))
    assert capacity == GROUP - 1
    main = model_width * capacity // GROUP
    vmem = pl.BlockSpec(memory_space=pltpu.VMEM)
    hbm = pl.BlockSpec(memory_space=pltpu.HBM)
    half_wide = out_weight.shape[0] // 2
    (weight_near,) = staged((out_weight,), half_wide)
    hidden, outgoing = pl.pallas_call(
        mix_body,
        out_shape=(
            jax.ShapeDtypeStruct((rows_dev, model_width), jnp.bfloat16),
            pltpu.HBM((experts_all * GROUP, main), jnp.bfloat16),
        ),
        in_specs=[vmem, vmem, hbm, vmem, vmem, vmem],
        scratch_shapes=[
            pltpu.VMEM((half_wide, model_width), jnp.bfloat16),
            pltpu.SemaphoreType.DMA((4,)),
        ],
        compiler_params=pltpu.CompilerParams(vmem_limit_bytes=16 << 20),
        name="mix",
    )(
        gathered,
        weight_near,
        in_hbm(out_weight),
        in_hbm(residual),
        in_hbm(ffn_gain),
        in_hbm(routes.T),
    )
    arrived = lax.all_to_all(outgoing.reshape(experts_all, GROUP, main), SP, 0, 0, tiled=True)

    gate_own, up_own, down_own = gate_weight[0], up_weight[0], down_weight[0]
    own_near = staged((gate_own, up_own), model_width)
    long = model_width * 11 // 16
    names = ("gate", "up", "more", "down")
    left, right = {}, {}
    for name, w in zip(names, (gate_own, up_own[:long], up_own[long:], down_own)):
        left[name] = shifted(w, "tp", 1)
        right[name] = shifted(w, "tp", -1)
    cut = down_own.shape[0] // 2
    far_gate = shifted(left["gate"], "tp", 1)
    far_up = shifted(right["up"], "tp", -1)
    far_more = shifted(right["more"], "tp", -1)
    far_down_l = shifted(left["down"][:cut], "tp", 1)
    far_down_r = shifted(right["down"][cut:], "tp", -1)
    weights = (
        down_own,
        left["gate"],
        left["down"],
        right["gate"],
        right["down"],
        far_gate,
        far_down_l,
        far_down_r,
        left["up"],
        left["more"],
        right["up"],
        right["more"],
        far_up,
        far_more,
    )
    result_rows = pl.pallas_call(
        expert_body,
        out_shape=pltpu.HBM((experts_all * GROUP, main), jnp.bfloat16),
        in_specs=[vmem] * 3 + [hbm] * len(weights),
        scratch_shapes=[
            pltpu.VMEM((group - 1,) + gate_own.shape, jnp.bfloat16),
            pltpu.VMEM((group - 1,) + gate_own.shape, jnp.bfloat16),
            pltpu.VMEM((group,) + down_own.shape, jnp.bfloat16),
            pltpu.SemaphoreType.DMA((len(weights),)),
        ],
        compiler_params=pltpu.CompilerParams(vmem_limit_bytes=40 << 20),
        name="expert",
    )(arrived.reshape(experts_all * GROUP, main), *own_near, *map(in_hbm, weights))
    returned = lax.all_to_all(result_rows.reshape(experts_all, GROUP, main), SP, 0, 0, tiled=True)
    return pl.pallas_call(
        combine_body,
        out_shape=jax.ShapeDtypeStruct((rows_dev, model_width), jnp.bfloat16),
        compiler_params=pltpu.CompilerParams(vmem_limit_bytes=16 << 20),
        name="combine",
    )(returned.reshape(experts_all * GROUP, main), hidden, in_hbm(routes), in_hbm(route_weights))


def solution(mesh):
    torus = Mesh(
        mesh.devices.reshape(mesh.shape["grp"], 16, 2, mesh.shape["tp"]),
        ("grp", "sp_0", "sp_1", "tp"),
    )
    placed = (
        P(GRP_SP, "tp"),
        P(GRP_SP, "tp"),
        P(GRP_SP, None),
        P(GRP_SP, None),
        P(),
        P(None, "tp"),
        P(None, "tp"),
        P(GRP_SP_TP, None),
        P(),
        P(),
        P(SP, None, "tp"),
        P(SP, None, "tp"),
        P(SP, "tp", None),
        P(GRP_SP_TP, None),
        P(GRP_SP_TP, None),
    )
    return jax.shard_map(
        on_device, mesh=torus, in_specs=placed, out_specs=P(GRP_SP_TP, None), check_vma=False
    )
```

```python
import jax
import jax.numpy as jnp
import numpy as np
from jax import lax
from jax.experimental import pallas as pl
from jax.experimental.pallas import tpu as pltpu
from jax.sharding import Mesh
from jax.sharding import PartitionSpec as P

PLAIN_HEAD_WIDTH = 128
QK_ROPE = 64
VALUE_WIDTH = 128
GRID_W = 64
SP = ("sp_0", "sp_1")
GRP_SP = ("grp", "sp_0", "sp_1")
GRP_SP_TP = ("grp", "sp_0", "sp_1", "tp")


theta = 10000.0
eps = 1e-06
limit = 7.0
slope = 1.702
STAT_LANES = 128


def turn_tables(place, heads):
    count = QK_ROPE // 4
    lane = jnp.arange(heads * QK_ROPE, dtype=jnp.int32)
    freqs = theta ** (-(lane % count).astype(jnp.float32) / count)
    by_row = (lane % QK_ROPE) < QK_ROPE // 2
    shift = jnp.where(by_row[None, :], (place // GRID_W)[:, None], (place % GRID_W)[:, None])
    angle = shift.astype(jnp.float32) * freqs[None, :]
    return jnp.cos(angle), jnp.sin(angle)


def partner_matrix(width):
    count = QK_ROPE // 4
    out = np.zeros((width, width), np.float32)
    for at in range(0, width, 2 * count):
        for i in range(count):
            out[at + count + i, at + i] = -1.0
            out[at + i, at + count + i] = 1.0
    return out


def norm_scale(values, gain):
    wide = values.astype(jnp.float32)
    return (
        wide
        * lax.rsqrt(jnp.mean(wide * wide, axis=-1, keepdims=True) + eps)
        * gain.astype(jnp.float32)
    )


def in_hbm(array):
    return pltpu.with_memory_space_constraint(array, pltpu.HBM)


def shifted(array, axis, step):
    count = lax.axis_size(axis)
    return lax.ppermute(array, axis, [(i, (i + step) % count) for i in range(count)])


GROUP = 8


def lanes_of(index, width):
    return slice(index * width, (index + 1) * width)


def prepare_body(
    index_ref,
    latent_ref,
    gain_ref,
    key_ref,
    cos_ref,
    sin_ref,
    swap_ref,
    key_matrix_ref,
    value_matrix_ref,
    plain_ref,
    turn_ref,
    sent_ref,
    shares_ref,
):
    rows, latent_width = latent_ref.shape
    sent_ref[:, :latent_width] = norm_scale(latent_ref[...], gain_ref[...]).astype(jnp.bfloat16)
    tokens = key_ref.shape[1]
    at = lax.broadcasted_iota(jnp.int32, (rows, tokens), 0) + index_ref[0] * rows
    pick = (at == lax.broadcasted_iota(jnp.int32, (rows, tokens), 1)).astype(jnp.bfloat16)
    key = lax.dot_general(
        pick, key_ref[...], (((1,), (1,)), ((), ())), preferred_element_type=jnp.float32
    )
    swapped = jnp.dot(
        key.astype(jnp.bfloat16), swap_ref[...], preferred_element_type=jnp.float32
    )
    turned = (key * cos_ref[...] + swapped * sin_ref[...]).astype(jnp.bfloat16)
    sent_ref[:, latent_width:] = jnp.concatenate((turned, jnp.zeros_like(turned)), axis=1)
    wide = key_matrix_ref.shape[1]
    depth = latent_width // 2
    matrix = jnp.where(index_ref[1] == 0, key_matrix_ref[...], value_matrix_ref[...])
    turn_wide = turn_ref.shape[1]
    half = tokens // 2
    quarter = tokens * turn_wide // (2 * wide)
    for j in range(shares_ref.shape[0]):
        shares_ref[j, :depth, :wide] = matrix[:depth, :]
        shares_ref[j, :depth, wide:] = matrix[depth:, :]
        shares_ref[j, depth : depth + half, :wide] = plain_ref[:half, :]
        shares_ref[j, depth : depth + half, wide:] = plain_ref[half:, :]
        for i in range(tokens // quarter):
            shares_ref[j, depth + half :, lanes_of(i, turn_wide)] = turn_ref[
                i * quarter : (i + 1) * quarter, :
            ]


def attend_body(
    core_ref,
    near_ref,
    other_ref,
    shares_ref,
    theirs_ref,
    cos_ref,
    sin_ref,
    swap_ref,
    out_ref,
    keys_ref,
    values_ref,
):
    shards = shares_ref.shape[0]
    width = shares_ref.shape[2]
    near = near_ref.shape[0]
    latent_width = width
    quarter = out_ref.shape[1]
    tokens = shards * quarter
    value_wide = width // 2
    heads = value_wide // PLAIN_HEAD_WIDTH
    scale = (PLAIN_HEAD_WIDTH + QK_ROPE) ** (-0.5)
    for h in range(heads):
        for rows_ref, at in ((near_ref, 0), (other_ref, near)):
            keys_ref[h, at : at + near, PLAIN_HEAD_WIDTH:] = rows_ref[:, latent_width:]
    lane = lax.broadcasted_iota(jnp.int32, (tokens, STAT_LANES), 1)
    stats = jnp.zeros((tokens, STAT_LANES), jnp.float32)
    last = (((1,), (1,)), ((), ()))
    for j in range(shards):
        depth = latent_width // 2
        mine = shares_ref[j, :depth, :]
        other = theirs_ref[j, :depth, :]
        for first, second, is_key in ((mine, other, True), (other, mine, False)):
            packed = jnp.where(core_ref[0] == 0, first, second)
            matrix = jnp.concatenate((packed[:, :value_wide], packed[:, value_wide:]), axis=0)
            for rows_ref, at in ((near_ref, 0), (other_ref, near)):
                made = jnp.dot(
                    rows_ref[:, :latent_width], matrix, preferred_element_type=jnp.float32
                ).astype(jnp.bfloat16)
                if is_key:
                    for h in range(heads):
                        keys_ref[h, at : at + near, :PLAIN_HEAD_WIDTH] = made[
                            :, lanes_of(h, PLAIN_HEAD_WIDTH)
                        ]
                else:
                    values_ref[at : at + near, :] = made
        at = depth
        half = tokens // 2
        plain = jnp.concatenate(
            (
                shares_ref[j, at : at + half, :value_wide],
                shares_ref[j, at : at + half, value_wide:],
            ),
            axis=0,
        )
        at += half
        raw = jnp.concatenate(
            [
                shares_ref[j, at : at + quarter, i * heads * QK_ROPE : (i + 1) * heads * QK_ROPE]
                for i in range(tokens // quarter)
            ],
            axis=0,
        )
        swapped = jnp.dot(raw, swap_ref[...], preferred_element_type=jnp.float32)
        turned = (raw.astype(jnp.float32) * cos_ref[...] + swapped * sin_ref[...]).astype(
            jnp.bfloat16
        )
        for h in range(heads):
            lo = h * PLAIN_HEAD_WIDTH
            query_rot = turned[:, lanes_of(h, QK_ROPE)]
            query = jnp.concatenate(
                (plain[:, lo : lo + PLAIN_HEAD_WIDTH], query_rot, jnp.zeros_like(query_rot)), axis=1
            )
            scores = lax.dot_general(query, keys_ref[h], last, preferred_element_type=jnp.float32)
            peak = jnp.max(scores, axis=1, keepdims=True)
            weights = jnp.exp((scores - peak) * scale)
            total = jnp.sum(weights, axis=1, keepdims=True)
            summed = jnp.dot(
                weights.astype(jnp.bfloat16),
                values_ref[:, lanes_of(h, VALUE_WIDTH)],
                preferred_element_type=jnp.float32,
            )
            result = (summed / total).astype(jnp.bfloat16)
            head = j * heads + h
            for i in range(shards):
                out_ref[i, :, head * VALUE_WIDTH : (head + 1) * VALUE_WIDTH] = result[
                    i * quarter : (i + 1) * quarter
                ]
            rest = peak * scale + jnp.log(total)
            for part in range(3):
                top = rest.astype(jnp.bfloat16).astype(jnp.float32)
                rest = rest - top
                stats = jnp.where(lane == part * shards * heads + head, top, stats)
    stats = stats.astype(jnp.bfloat16)
    for i in range(shards):
        out_ref[i, :, shards * value_wide :] = stats[i * quarter : (i + 1) * quarter]


def mix_body(
    parts_ref, weight_hbm, residual_ref, gain_ref, routes_ref, hidden_ref, outgoing_ref, weight_ref, sems
):
    pieces = sems.shape[0]
    depth = weight_ref.shape[0] // pieces
    loads = []
    for i in range(pieces):
        part = pl.ds(i * depth, depth)
        loads.append(pltpu.make_async_copy(weight_hbm.at[part], weight_ref.at[part], sems.at[i]))
        loads[-1].start()
    shards = parts_ref.shape[0]
    rows, model_width = residual_ref.shape
    wide = weight_ref.shape[0]
    heads = wide // VALUE_WIDTH
    sums = []
    for i in range(shards):
        stat = parts_ref[i, :, wide:].astype(jnp.float32)
        sums.append(
            stat[:, :heads] + (stat[:, heads : 2 * heads] + stat[:, 2 * heads : 3 * heads])
        )
    most = sums[0]
    for s in sums[1:]:
        most = jnp.maximum(most, s)
    shares = [jnp.exp(s - most) for s in sums]
    whole = shares[0]
    for s in shares[1:]:
        whole = whole + s
    shares = [s / whole for s in shares]
    joined = []
    for h in range(heads):
        lo = h * VALUE_WIDTH
        piece = shares[0][:, h : h + 1] * parts_ref[0, :, lo : lo + VALUE_WIDTH].astype(jnp.float32)
        for i in range(1, shards):
            piece = piece + shares[i][:, h : h + 1] * parts_ref[
                i, :, lo : lo + VALUE_WIDTH
            ].astype(jnp.float32)
        joined.append(piece.astype(jnp.bfloat16))
    attended = jnp.concatenate(joined, axis=1)

    total_rows = outgoing_ref.shape[0]
    line = lax.broadcasted_iota(jnp.int32, (total_rows, rows), 0)
    named = jnp.zeros((total_rows, rows), jnp.int32)
    for k in range(routes_ref.shape[0]):
        named = named | (routes_ref[k : k + 1, :] == line // GROUP).astype(jnp.int32)
    before = (
        lax.broadcasted_iota(jnp.int32, (rows, rows), 0)
        < lax.broadcasted_iota(jnp.int32, (rows, rows), 1)
    ).astype(jnp.bfloat16)
    rank = jnp.dot(
        named.astype(jnp.float32).astype(jnp.bfloat16), before, preferred_element_type=jnp.float32
    ).astype(jnp.int32)
    table = jnp.where((named > 0) & (rank == line % GROUP), 1.0, 0.0).astype(jnp.bfloat16)

    for load in loads:
        load.wait()
    projected = jnp.dot(attended, weight_ref[...], preferred_element_type=jnp.float32)
    hidden = (residual_ref[...].astype(jnp.float32) + projected).astype(jnp.bfloat16)
    hidden_ref[...] = hidden
    normed = norm_scale(hidden, gain_ref[...]).astype(jnp.bfloat16)
    tail = model_width - outgoing_ref.shape[1]
    ends = normed[:, model_width - tail :]
    for s in range(GROUP - 1):
        of_last = jnp.where(
            (named > 0) & (rank == s) & (line % GROUP == GROUP - 1), 1.0, 0.0
        ).astype(jnp.bfloat16)
        outgoing_ref[:, lanes_of(s, tail)] = (
            jnp.dot(table, normed[:, lanes_of(s, tail)], preferred_element_type=jnp.float32)
            + jnp.dot(of_last, ends, preferred_element_type=jnp.float32)
        ).astype(jnp.bfloat16)


def expert_body(parity_ref, arrived_ref, *refs):
    out_ref, gate_up_ref, down_ref, sems = refs[-4:]
    sources = refs[:-4]
    count = down_ref.shape[0]
    far = count - 1
    long = sources[4].shape[0]
    short = sources[5].shape[0]
    cut = sources[13].shape[0]
    part = sources[15].shape[0]
    parity = parity_ref[0]
    targets = [
        ("gate", 0, gate_up_ref.at[0, 0]),
        ("up", 0, gate_up_ref.at[0, 1]),
        ("down", 0, down_ref.at[0]),
    ]
    for q in range(1, far):
        targets += [
            ("gate", q, gate_up_ref.at[q, 0]),
            ("up", q, gate_up_ref.at[q, 1, pl.ds(0, long)]),
            ("up", q, gate_up_ref.at[q, 1, pl.ds(long, short)]),
            ("down", q, down_ref.at[q]),
        ]
    targets += [
        ("gate", far, gate_up_ref.at[far, 0, pl.ds(long, short)]),
        ("up", far, gate_up_ref.at[far, 1, pl.ds(long, short)]),
        ("down", far, down_ref.at[far, pl.ds(0, cut)]),
        ("down", far, down_ref.at[far, pl.ds(cut, cut)]),
        ("gate", far, gate_up_ref.at[far, parity, pl.ds(0, part)]),
        ("gate", far, gate_up_ref.at[far, parity, pl.ds(part, part)]),
        ("gate", far, gate_up_ref.at[far, 1 - parity, pl.ds(0, part)]),
        ("gate", far, gate_up_ref.at[far, 1 - parity, pl.ds(part, part)]),
    ]
    loads = {}
    for i, (source, (kind, q, target)) in enumerate(zip(sources, targets, strict=True)):
        load = pltpu.make_async_copy(source, target, sems.at[i])
        load.start()
        loads.setdefault((kind, q), []).append(load)

    def ready(kind, q):
        for load in loads.pop((kind, q), ()):
            load.wait()

    rows, main = arrived_ref.shape
    model_width = gate_up_ref.shape[2]
    tail = model_width - main
    line = lax.broadcasted_iota(jnp.int32, (rows, rows), 0)
    column = lax.broadcasted_iota(jnp.int32, (rows, rows), 1)
    ends = jnp.zeros((rows, tail), jnp.float32)
    for s in range(GROUP - 1):
        pick = jnp.where(
            (line % GROUP == s) & (column == line - s + GROUP - 1), 1.0, 0.0
        ).astype(jnp.bfloat16)
        ends = ends + jnp.dot(
            pick, arrived_ref[:, lanes_of(s, tail)], preferred_element_type=jnp.float32
        )
    ends = ends.astype(jnp.bfloat16)
    actives = []
    for q in range(count):
        gate_ref, up_ref = gate_up_ref.at[q, 0], gate_up_ref.at[q, 1]
        ready("gate", q)
        gate_pre = jnp.dot(
            arrived_ref[...], gate_ref[:main, :], preferred_element_type=jnp.float32
        ) + jnp.dot(ends, gate_ref[main:, :], preferred_element_type=jnp.float32)
        ready("up", q)
        up_pre = jnp.dot(
            arrived_ref[...], up_ref[:main, :], preferred_element_type=jnp.float32
        ) + jnp.dot(ends, up_ref[main:, :], preferred_element_type=jnp.float32)
        gate_pre = jnp.minimum(gate_pre, limit)
        actives.append(
            (
                (jnp.clip(up_pre, -limit, limit) + 1.0) * gate_pre * jax.nn.sigmoid(slope * gate_pre)
            ).astype(jnp.bfloat16)
        )
    for q in range(count):
        ready("down", q)

    def result_of(piece):
        total = jnp.zeros((rows, tail), jnp.float32)
        for q in range(count):
            product = jnp.dot(
                actives[q], down_ref[q, :, lanes_of(piece, tail)], preferred_element_type=jnp.float32
            )
            total = total + product.astype(jnp.bfloat16).astype(jnp.float32)
        return total

    last = result_of(GROUP - 1).astype(jnp.bfloat16)
    group_end = lax.broadcasted_iota(jnp.int32, (rows, tail), 0) % GROUP == GROUP - 1
    for s in range(GROUP - 1):
        pick = jnp.where(
            (line % GROUP == GROUP - 1) & (column == line - (GROUP - 1) + s), 1.0, 0.0
        ).astype(jnp.bfloat16)
        moved = jnp.dot(pick, last, preferred_element_type=jnp.float32)
        out_ref[:, lanes_of(s, tail)] = jnp.where(group_end, moved, result_of(s)).astype(
            jnp.bfloat16
        )


def combine_body(returned_ref, hidden_ref, routes_ref, weights_ref, out_ref):
    rows, model_width = hidden_ref.shape
    total_rows, main = returned_ref.shape
    tail = model_width - main
    column = lax.broadcasted_iota(jnp.int32, (rows, total_rows), 1)
    named = jnp.zeros((rows, total_rows), jnp.float32)
    weight = jnp.zeros((rows, total_rows), jnp.float32)
    for k in range(routes_ref.shape[1]):
        here = routes_ref[:, k : k + 1] == column // GROUP
        named = jnp.where(here, 1.0, named)
        weight = jnp.where(here, weights_ref[:, k : k + 1], weight)
    before = (
        lax.broadcasted_iota(jnp.int32, (rows, rows), 1)
        < lax.broadcasted_iota(jnp.int32, (rows, rows), 0)
    ).astype(jnp.bfloat16)
    rank = jnp.dot(
        before, named.astype(jnp.bfloat16), preferred_element_type=jnp.float32
    ).astype(jnp.int32)
    parts = []
    rest = weight
    for _ in range(3):
        top = rest.astype(jnp.bfloat16).astype(jnp.float32)
        rest = rest - top
        parts.append(top)

    def gathered(keep, values):
        table = jnp.concatenate([jnp.where(keep, p, 0.0) for p in parts], axis=0)
        got = jnp.dot(table.astype(jnp.bfloat16), values, preferred_element_type=jnp.float32)
        return got[:rows] + (got[rows : 2 * rows] + got[2 * rows :])

    own = (named > 0) & (rank == column % GROUP)
    out_ref[:, :main] = (
        hidden_ref[:, :main].astype(jnp.float32) + gathered(own, returned_ref[...])
    ).astype(jnp.bfloat16)
    ends = jnp.zeros((rows, tail), jnp.float32)
    for s in range(GROUP - 1):
        keep = (named > 0) & (rank == s) & (column % GROUP == GROUP - 1)
        ends = ends + gathered(keep, returned_ref[:, lanes_of(s, tail)])
    out_ref[:, main:] = (hidden_ref[:, main:].astype(jnp.float32) + ends).astype(jnp.bfloat16)


def on_device(
    query_plain,
    query_turn,
    latent,
    key_turn,
    latent_norm_scale,
    plain_key_matrix,
    value_matrix,
    residual,
    out_weight,
    ffn_gain,
    gate_weight,
    up_weight,
    down_weight,
    routes,
    route_weights,
):
    tok_dev = latent.shape[0]
    rows_dev = residual.shape[0]
    model_width = residual.shape[1]
    latent_width = latent.shape[1]
    group = lax.axis_size("tp")
    heads_dev = query_plain.shape[1] // PLAIN_HEAD_WIDTH
    place = lax.axis_index(SP) * tok_dev + jnp.arange(tok_dev, dtype=jnp.int32)
    at_tp = lax.axis_index("tp")
    at_core = lax.axis_index("sp_1")
    own_place = (
        lax.axis_index(SP) * tok_dev
        + at_tp * rows_dev
        + jnp.arange(rows_dev, dtype=jnp.int32)
    )
    own_cos, own_sin = turn_tables(own_place, 1)
    cosines, sines = turn_tables(place, heads_dev)
    share_rows = latent_width // 2 + tok_dev // 2 + tok_dev * query_turn.shape[1] // latent_width
    wide = plain_key_matrix.shape[1]
    whole = lambda *shape: pl.BlockSpec(shape, lambda i, at: (0,) * len(shape))
    sent, shares = pl.pallas_call(
        prepare_body,
        out_shape=(
            jax.ShapeDtypeStruct((rows_dev, latent_width + 2 * QK_ROPE), jnp.bfloat16),
            jax.ShapeDtypeStruct((group, share_rows, latent_width), jnp.bfloat16),
        ),
        grid_spec=pltpu.PrefetchScalarGridSpec(
            num_scalar_prefetch=1,
            grid=(1,),
            in_specs=[
                pl.BlockSpec((rows_dev, latent_width), lambda i, at: (at[0], 0)),
                whole(latent_width),
                whole(QK_ROPE, tok_dev),
                whole(rows_dev, QK_ROPE),
                whole(rows_dev, QK_ROPE),
                whole(QK_ROPE, QK_ROPE),
                whole(latent_width, wide),
                whole(latent_width, wide),
                whole(tok_dev, query_plain.shape[1]),
                whole(tok_dev, query_turn.shape[1]),
            ],
            out_specs=(
                whole(rows_dev, latent_width + 2 * QK_ROPE),
                whole(group, share_rows, latent_width),
            ),
        ),
        compiler_params=pltpu.CompilerParams(vmem_limit_bytes=16 << 20),
        name="prepare",
    )(
        jnp.stack((at_tp, at_core)),
        *map(
            in_hbm,
            (
                latent,
                latent_norm_scale,
                key_turn.T,
                own_cos,
                own_sin,
                jnp.asarray(partner_matrix(QK_ROPE), jnp.bfloat16),
                plain_key_matrix,
                value_matrix,
                query_plain,
                query_turn,
            ),
        ),
    )
    shares = lax.all_to_all(shares, "tp", 0, 0, tiled=True)
    theirs = shifted(shares, "sp_1", 1)
    near = lax.all_gather(sent, "sp_0", axis=0, tiled=True)
    other = shifted(near, "sp_1", 1)

    parts = pl.pallas_call(
        attend_body,
        out_shape=pltpu.HBM(
            (group, rows_dev, group * heads_dev * VALUE_WIDTH + STAT_LANES), jnp.bfloat16
        ),
        in_specs=[pl.BlockSpec(memory_space=pltpu.SMEM)]
        + [pl.BlockSpec(memory_space=pltpu.VMEM)] * 7,
        scratch_shapes=[
            pltpu.VMEM((heads_dev, 2 * near.shape[0], PLAIN_HEAD_WIDTH + 2 * QK_ROPE), jnp.bfloat16),
            pltpu.VMEM((2 * near.shape[0], heads_dev * VALUE_WIDTH), jnp.bfloat16),
        ],
        compiler_params=pltpu.CompilerParams(vmem_limit_bytes=24 << 20),
        name="attend",
    )(
        at_core.reshape(1),
        near,
        other,
        shares,
        theirs,
        in_hbm(cosines),
        in_hbm(sines),
        in_hbm(jnp.asarray(partner_matrix(heads_dev * QK_ROPE), jnp.bfloat16)),
    )
    gathered = lax.all_to_all(parts, "tp", 0, 0, tiled=True)

    experts_all = lax.axis_size(SP) * gate_weight.shape[0]
    top_count = routes.shape[1]
    capacity = min(rows_dev, max(2, rows_dev * top_count * 3 // (2 * experts_all)))
    assert capacity == GROUP - 1
    main = model_width * capacity // GROUP
    vmem = pl.BlockSpec(memory_space=pltpu.VMEM)
    hbm = pl.BlockSpec(memory_space=pltpu.HBM)
    hidden, outgoing = pl.pallas_call(
        mix_body,
        out_shape=(
            jax.ShapeDtypeStruct((rows_dev, model_width), jnp.bfloat16),
            pltpu.HBM((experts_all * GROUP, main), jnp.bfloat16),
        ),
        in_specs=[vmem, hbm, vmem, vmem, vmem],
        scratch_shapes=[
            pltpu.VMEM(out_weight.shape, jnp.bfloat16),
            pltpu.SemaphoreType.DMA((8,)),
        ],
        compiler_params=pltpu.CompilerParams(vmem_limit_bytes=16 << 20),
        name="mix",
    )(
        gathered,
        in_hbm(out_weight),
        in_hbm(residual),
        in_hbm(ffn_gain),
        in_hbm(routes.T),
    )
    arrived = lax.all_to_all(
        outgoing.reshape(experts_all, GROUP, main), SP, 0, 0, tiled=True
    )

    gate_own, up_own, down_own = gate_weight[0], up_weight[0], down_weight[0]
    long = model_width * 11 // 16
    names = ("gate", "up", "more", "down")
    left, right = {}, {}
    for name, w in zip(names, (gate_own, up_own[:long], up_own[long:], down_own)):
        left[name] = shifted(w, "tp", 1)
        right[name] = shifted(w, "tp", -1)
    cut = down_own.shape[0] // 2
    part = long // 2
    parity = lax.axis_index("grp") % 2
    even = parity == 0
    relay_l = jnp.where(even, left["gate"][:part], left["up"][:part])
    relay_r = jnp.where(even, right["gate"][part:long], right["up"][part:])
    far_l = shifted(relay_l, "tp", 1)
    far_r = shifted(relay_r, "tp", -1)
    pairs = [(i, i ^ 1) for i in range(lax.axis_size("grp"))]
    pair_l = lax.ppermute(far_l, "grp", pairs)
    pair_r = lax.ppermute(far_r, "grp", pairs)
    far_gate = shifted(left["gate"][long:], "tp", 1)
    far_more = shifted(right["more"], "tp", -1)
    far_down_l = shifted(left["down"][:cut], "tp", 1)
    far_down_r = shifted(right["down"][cut:], "tp", -1)
    weights = [gate_own, up_own, down_own]
    for side in (left, right):
        weights += [side["gate"], side["up"], side["more"], side["down"]]
    weights += [far_gate, far_more, far_down_l, far_down_r, far_l, far_r, pair_l, pair_r]
    result_rows = pl.pallas_call(
        expert_body,
        out_shape=pltpu.HBM((experts_all * GROUP, main), jnp.bfloat16),
        in_specs=[pl.BlockSpec(memory_space=pltpu.SMEM), vmem] + [hbm] * len(weights),
        scratch_shapes=[
            pltpu.VMEM((group, 2) + gate_own.shape, jnp.bfloat16),
            pltpu.VMEM((group,) + down_own.shape, jnp.bfloat16),
            pltpu.SemaphoreType.DMA((len(weights),)),
        ],
        compiler_params=pltpu.CompilerParams(vmem_limit_bytes=40 << 20),
        name="expert",
    )(
        parity.reshape(1),
        arrived.reshape(experts_all * GROUP, main),
        *map(in_hbm, weights),
    )
    returned = lax.all_to_all(
        result_rows.reshape(experts_all, GROUP, main), SP, 0, 0, tiled=True
    )
    return pl.pallas_call(
        combine_body,
        out_shape=jax.ShapeDtypeStruct((rows_dev, model_width), jnp.bfloat16),
        compiler_params=pltpu.CompilerParams(vmem_limit_bytes=16 << 20),
        name="combine",
    )(returned.reshape(experts_all * GROUP, main), hidden, in_hbm(routes), in_hbm(route_weights))


def solution(mesh):
    torus = Mesh(
        mesh.devices.reshape(mesh.shape["grp"], 16, 2, mesh.shape["tp"]),
        ("grp", "sp_0", "sp_1", "tp"),
    )
    placed = (
        P(GRP_SP, "tp"),
        P(GRP_SP, "tp"),
        P(GRP_SP, None),
        P(GRP_SP, None),
        P(),
        P(None, "tp"),
        P(None, "tp"),
        P(GRP_SP_TP, None),
        P(),
        P(),
        P(SP, None, "tp"),
        P(SP, None, "tp"),
        P(SP, "tp", None),
        P(GRP_SP_TP, None),
        P(GRP_SP_TP, None),
    )
    return jax.shard_map(
        on_device, mesh=torus, in_specs=placed, out_specs=P(GRP_SP_TP, None), check_vma=False
    )
```

```python
import jax
import jax.numpy as jnp
import numpy as np
from jax import lax
from jax.experimental import pallas as pl
from jax.experimental.pallas import tpu as pltpu
from jax.sharding import Mesh
from jax.sharding import PartitionSpec as P

PLAIN_HEAD_WIDTH = 128
QK_ROPE = 64
VALUE_WIDTH = 128
GRID_W = 64
SP = ("sp_0", "sp_1")
GRP_SP = ("grp", "sp_0", "sp_1")
GRP_SP_TP = ("grp", "sp_0", "sp_1", "tp")


theta = 10000.0
eps = 1e-06
limit = 7.0
slope = 1.702
STAT_LANES = 128
LOG2_E = 1.4426950408889634


def turn_tables(place, heads):
    count = QK_ROPE // 4
    lane = jnp.arange(heads * QK_ROPE, dtype=jnp.int32)
    freqs = theta ** (-(lane % count).astype(jnp.float32) / count)
    by_row = (lane % QK_ROPE) < QK_ROPE // 2
    shift = jnp.where(by_row[None, :], (place // GRID_W)[:, None], (place % GRID_W)[:, None])
    angle = shift.astype(jnp.float32) * freqs[None, :]
    return jnp.cos(angle), jnp.sin(angle)


def partner_matrix(width):
    count = QK_ROPE // 4
    out = np.zeros((width, width), np.float32)
    for at in range(0, width, 2 * count):
        for i in range(count):
            out[at + count + i, at + i] = -1.0
            out[at + i, at + count + i] = 1.0
    return out


def norm_scale(values, gain):
    wide = values.astype(jnp.float32)
    return (
        wide
        * lax.rsqrt(jnp.mean(wide * wide, axis=-1, keepdims=True) + eps)
        * gain.astype(jnp.float32)
    )


def in_hbm(array):
    return pltpu.with_memory_space_constraint(array, pltpu.HBM)


def in_vmem(array):
    return pltpu.with_memory_space_constraint(array, pltpu.VMEM)


def shifted(array, axis, step):
    count = lax.axis_size(axis)
    return lax.ppermute(array, axis, [(i, (i + step) % count) for i in range(count)])


GROUP = 8


def lanes_of(index, width):
    return slice(index * width, (index + 1) * width)


def stage_body(*refs):
    count = (len(refs) - 1) // 2
    sems = refs[-1]
    pieces = sems.shape[1]
    loads = []
    for n in range(count):
        depth = refs[count + n].shape[0] // pieces
        for i in range(pieces):
            part = pl.ds(i * depth, depth)
            loads.append(
                pltpu.make_async_copy(refs[n].at[part], refs[count + n].at[part], sems.at[n, i])
            )
            loads[-1].start()
    for load in loads:
        load.wait()


def staged(arrays, rows):
    hbm = pl.BlockSpec(memory_space=pltpu.HBM)
    vmem = pl.BlockSpec(memory_space=pltpu.VMEM)
    return pl.pallas_call(
        stage_body,
        out_shape=tuple(pltpu.VMEM((rows,) + a.shape[1:], a.dtype) for a in arrays),
        in_specs=[hbm] * len(arrays),
        out_specs=(vmem,) * len(arrays),
        scratch_shapes=[pltpu.SemaphoreType.DMA((len(arrays), 4))],
        compiler_params=pltpu.CompilerParams(vmem_limit_bytes=16 << 20),
    )(*map(in_hbm, arrays))


def prepare_body(
    index_ref,
    latent_ref,
    gain_ref,
    key_ref,
    cos_ref,
    sin_ref,
    swap_ref,
    key_matrix_ref,
    value_matrix_ref,
    plain_ref,
    turn_ref,
    sent_ref,
    shares_ref,
):
    rows, latent_width = latent_ref.shape
    sent_ref[:, :latent_width] = norm_scale(latent_ref[...], gain_ref[...]).astype(jnp.bfloat16)
    tokens = key_ref.shape[1]
    at = lax.broadcasted_iota(jnp.int32, (rows, tokens), 0) + index_ref[0] * rows
    pick = (at == lax.broadcasted_iota(jnp.int32, (rows, tokens), 1)).astype(jnp.bfloat16)
    key = lax.dot_general(
        pick, key_ref[...], (((1,), (1,)), ((), ())), preferred_element_type=jnp.float32
    )
    swapped = jnp.dot(
        key.astype(jnp.bfloat16), swap_ref[...], preferred_element_type=jnp.float32
    )
    turned = (key * cos_ref[...] + swapped * sin_ref[...]).astype(jnp.bfloat16)
    sent_ref[:, latent_width:] = jnp.concatenate((turned, jnp.zeros_like(turned)), axis=1)
    wide = key_matrix_ref.shape[1]
    depth = latent_width // 2
    matrix = jnp.where(index_ref[1] == 0, key_matrix_ref[...], value_matrix_ref[...])
    turn_wide = turn_ref.shape[1]
    half = tokens // 2
    quarter = tokens * turn_wide // (2 * wide)
    for j in range(shares_ref.shape[0]):
        shares_ref[j, :depth, :wide] = matrix[:depth, :]
        shares_ref[j, :depth, wide:] = matrix[depth:, :]
        shares_ref[j, depth : depth + half, :wide] = plain_ref[:half, :]
        shares_ref[j, depth : depth + half, wide:] = plain_ref[half:, :]
        for i in range(tokens // quarter):
            shares_ref[j, depth + half :, lanes_of(i, turn_wide)] = turn_ref[
                i * quarter : (i + 1) * quarter, :
            ]


def attend_body(
    core_ref,
    near_ref,
    other_ref,
    shares_ref,
    theirs_ref,
    cos_ref,
    sin_ref,
    swap_ref,
    out_ref,
    keys_ref,
    values_ref,
):
    shards = shares_ref.shape[0]
    width = shares_ref.shape[2]
    near = near_ref.shape[0]
    latent_width = width
    quarter = out_ref.shape[1]
    tokens = shards * quarter
    value_wide = width // 2
    heads = value_wide // PLAIN_HEAD_WIDTH
    scale = (PLAIN_HEAD_WIDTH + QK_ROPE) ** (-0.5)
    for h in range(heads):
        for rows_ref, at in ((near_ref, 0), (other_ref, near)):
            keys_ref[h, at : at + near, PLAIN_HEAD_WIDTH:] = rows_ref[:, latent_width:]
    lane = lax.broadcasted_iota(jnp.int32, (tokens, STAT_LANES), 1)
    stats = jnp.zeros((tokens, STAT_LANES), jnp.float32)
    last = (((1,), (1,)), ((), ()))
    for j in range(shards):
        depth = latent_width // 2
        mine = shares_ref[j, :depth, :]
        other = theirs_ref[j, :depth, :]
        for first, second, is_key in ((mine, other, True), (other, mine, False)):
            packed = jnp.where(core_ref[0] == 0, first, second)
            matrix = jnp.concatenate((packed[:, :value_wide], packed[:, value_wide:]), axis=0)
            for rows_ref, at in ((near_ref, 0), (other_ref, near)):
                made = jnp.dot(
                    rows_ref[:, :latent_width], matrix, preferred_element_type=jnp.float32
                ).astype(jnp.bfloat16)
                if is_key:
                    for h in range(heads):
                        keys_ref[h, at : at + near, :PLAIN_HEAD_WIDTH] = made[
                            :, lanes_of(h, PLAIN_HEAD_WIDTH)
                        ]
                else:
                    values_ref[at : at + near, :] = made
        at = depth
        half = tokens // 2
        plain = jnp.concatenate(
            (
                shares_ref[j, at : at + half, :value_wide],
                shares_ref[j, at : at + half, value_wide:],
            ),
            axis=0,
        )
        at += half
        raw = jnp.concatenate(
            [
                shares_ref[j, at : at + quarter, i * heads * QK_ROPE : (i + 1) * heads * QK_ROPE]
                for i in range(tokens // quarter)
            ],
            axis=0,
        )
        swapped = jnp.dot(raw, swap_ref[...], preferred_element_type=jnp.float32)
        turned = (raw.astype(jnp.float32) * cos_ref[...] + swapped * sin_ref[...]).astype(
            jnp.bfloat16
        )
        all_weights, peaks, totals = [], [], []
        for h in range(heads):
            query_rot = turned[:, lanes_of(h, QK_ROPE)]
            query = jnp.concatenate(
                (plain[:, lanes_of(h, PLAIN_HEAD_WIDTH)], query_rot, jnp.zeros_like(query_rot)),
                axis=1,
            )
            scores = lax.dot_general(query, keys_ref[h], last, preferred_element_type=jnp.float32)
            peak = jnp.max(scores, axis=1, keepdims=True)
            weights = jnp.exp2((scores - peak) * (scale * LOG2_E))
            peaks.append(peak)
            totals.append(jnp.sum(weights, axis=1, keepdims=True))
            all_weights.append(weights.astype(jnp.bfloat16))
        crossed = jnp.dot(
            jnp.concatenate(all_weights, axis=0), values_ref[...], preferred_element_type=jnp.float32
        )
        for h in range(heads):
            peak, total = peaks[h], totals[h]
            summed = crossed[h * tokens : (h + 1) * tokens, lanes_of(h, VALUE_WIDTH)]
            result = (summed / total).astype(jnp.bfloat16)
            head = j * heads + h
            for i in range(shards):
                out_ref[i, :, head * VALUE_WIDTH : (head + 1) * VALUE_WIDTH] = result[
                    i * quarter : (i + 1) * quarter
                ]
            rest = peak * scale + jnp.log(total)
            for part in range(3):
                top = rest.astype(jnp.bfloat16).astype(jnp.float32)
                rest = rest - top
                stats = jnp.where(lane == part * shards * heads + head, top, stats)
    stats = stats.astype(jnp.bfloat16)
    for i in range(shards):
        out_ref[i, :, shards * value_wide :] = stats[i * quarter : (i + 1) * quarter]


def mix_body(
    parts_ref,
    near_ref,
    weight_hbm,
    residual_ref,
    gain_ref,
    routes_ref,
    hidden_ref,
    outgoing_ref,
    weight_ref,
    sems,
):
    pieces = sems.shape[0]
    depth = weight_ref.shape[0] // pieces
    above = near_ref.shape[0]
    loads = []
    for i in range(pieces):
        source = weight_hbm.at[pl.ds(above + i * depth, depth)]
        loads.append(
            pltpu.make_async_copy(source, weight_ref.at[pl.ds(i * depth, depth)], sems.at[i])
        )
        loads[-1].start()
    shards = parts_ref.shape[0]
    rows, model_width = residual_ref.shape
    wide = weight_hbm.shape[0]
    heads = wide // VALUE_WIDTH
    sums = []
    for i in range(shards):
        stat = parts_ref[i, :, wide:].astype(jnp.float32)
        sums.append(
            stat[:, :heads] + (stat[:, heads : 2 * heads] + stat[:, 2 * heads : 3 * heads])
        )
    most = sums[0]
    for s in sums[1:]:
        most = jnp.maximum(most, s)
    shares = [jnp.exp(s - most) for s in sums]
    whole = shares[0]
    for s in shares[1:]:
        whole = whole + s
    shares = [s / whole for s in shares]
    joined = []
    for h in range(heads):
        lo = h * VALUE_WIDTH
        piece = shares[0][:, h : h + 1] * parts_ref[0, :, lo : lo + VALUE_WIDTH].astype(jnp.float32)
        for i in range(1, shards):
            piece = piece + shares[i][:, h : h + 1] * parts_ref[
                i, :, lo : lo + VALUE_WIDTH
            ].astype(jnp.float32)
        joined.append(piece.astype(jnp.bfloat16))
    attended = jnp.concatenate(joined, axis=1)

    total_rows = outgoing_ref.shape[0]
    line = lax.broadcasted_iota(jnp.int32, (total_rows, rows), 0)
    named = jnp.zeros((total_rows, rows), jnp.int32)
    for k in range(routes_ref.shape[0]):
        named = named | (routes_ref[k : k + 1, :] == line // GROUP).astype(jnp.int32)
    before = (
        lax.broadcasted_iota(jnp.int32, (rows, rows), 0)
        < lax.broadcasted_iota(jnp.int32, (rows, rows), 1)
    ).astype(jnp.bfloat16)
    rank = jnp.dot(
        named.astype(jnp.float32).astype(jnp.bfloat16), before, preferred_element_type=jnp.float32
    ).astype(jnp.int32)
    table = jnp.where((named > 0) & (rank == line % GROUP), 1.0, 0.0).astype(jnp.bfloat16)

    projected = jnp.dot(attended[:, :above], near_ref[...], preferred_element_type=jnp.float32)
    for load in loads:
        load.wait()
    projected = projected + jnp.dot(
        attended[:, above:], weight_ref[...], preferred_element_type=jnp.float32
    )
    hidden = (residual_ref[...].astype(jnp.float32) + projected).astype(jnp.bfloat16)
    hidden_ref[...] = hidden
    normed = norm_scale(hidden, gain_ref[...]).astype(jnp.bfloat16)
    tail = model_width - outgoing_ref.shape[1]
    ends = normed[:, model_width - tail :]
    for s in range(GROUP - 1):
        of_last = jnp.where(
            (named > 0) & (rank == s) & (line % GROUP == GROUP - 1), 1.0, 0.0
        ).astype(jnp.bfloat16)
        outgoing_ref[:, lanes_of(s, tail)] = (
            jnp.dot(table, normed[:, lanes_of(s, tail)], preferred_element_type=jnp.float32)
            + jnp.dot(of_last, ends, preferred_element_type=jnp.float32)
        ).astype(jnp.bfloat16)


def begin_loads(sources, targets, sems):
    loads = {}
    for i, (source, (name, target)) in enumerate(zip(sources, targets, strict=True)):
        load = pltpu.make_async_copy(source, target, sems.at[i])
        load.start()
        loads.setdefault(name, []).append(load)

    def ready(name):
        for load in loads.pop(name):
            load.wait()

    return ready


def activation(gate_pre, up_pre):
    gate_pre = jnp.minimum(gate_pre, limit)
    return (
        (jnp.clip(up_pre, -limit, limit) + 1.0) * gate_pre * jax.nn.sigmoid(slope * gate_pre)
    ).astype(jnp.bfloat16)


def active_units(rows_ref, ends, gate_ref, up_ref, ready, q):
    main = rows_ref.shape[1]
    ready(("gate", q))
    gate_pre = jnp.dot(
        rows_ref[...], gate_ref[:main, :], preferred_element_type=jnp.float32
    ) + jnp.dot(ends, gate_ref[main:, :], preferred_element_type=jnp.float32)
    ready(("up", q))
    up_pre = jnp.dot(
        rows_ref[...], up_ref[:main, :], preferred_element_type=jnp.float32
    ) + jnp.dot(ends, up_ref[main:, :], preferred_element_type=jnp.float32)
    return activation(gate_pre, up_pre)


def near_body(arrived_ref, *refs):
    total_ref, ends_ref, gate_up_ref, down_ref, sems = refs[-5:]
    sources = refs[:-5]
    count = down_ref.shape[0]
    long, short = sources[4].shape[0], sources[5].shape[0]
    targets = [
        (("gate", 0), gate_up_ref.at[0, 0]),
        (("up", 0), gate_up_ref.at[0, 1]),
        (("down", 0), down_ref.at[0]),
    ]
    for q in range(1, count):
        targets += [
            (("gate", q), gate_up_ref.at[q, 0]),
            (("up", q), gate_up_ref.at[q, 1, pl.ds(0, long)]),
            (("up", q), gate_up_ref.at[q, 1, pl.ds(long, short)]),
            (("down", q), down_ref.at[q]),
        ]
    ready = begin_loads(sources, targets, sems)
    rows, main = arrived_ref.shape
    tail = total_ref.shape[1] - main
    line = lax.broadcasted_iota(jnp.int32, (rows, rows), 0)
    column = lax.broadcasted_iota(jnp.int32, (rows, rows), 1)
    ends = jnp.zeros((rows, tail), jnp.float32)
    for s in range(GROUP - 1):
        pick = jnp.where(
            (line % GROUP == s) & (column == line - s + GROUP - 1), 1.0, 0.0
        ).astype(jnp.bfloat16)
        ends = ends + jnp.dot(
            pick, arrived_ref[:, lanes_of(s, tail)], preferred_element_type=jnp.float32
        )
    ends = ends.astype(jnp.bfloat16)
    ends_ref[...] = ends
    actives = [
        active_units(arrived_ref, ends, gate_up_ref.at[q, 0], gate_up_ref.at[q, 1], ready, q)
        for q in range(count)
    ]
    for q in range(count):
        ready(("down", q))
    for piece in range(GROUP):
        at = lanes_of(piece, tail)
        total = jnp.zeros((rows, tail), jnp.float32)
        for q in range(count):
            product = jnp.dot(actives[q], down_ref[q, :, at], preferred_element_type=jnp.float32)
            total = total + product.astype(jnp.bfloat16).astype(jnp.float32)
        total_ref[:, at] = total


def far_body(
    arrived_ref,
    ends_ref,
    total_ref,
    gate_ref,
    up_ref,
    down_l_ref,
    more_hbm,
    down_r_hbm,
    out_ref,
    more_ref,
    down_r_ref,
    sems,
):
    ready = begin_loads(
        (more_hbm, down_r_hbm), (("more", more_ref), ("down", down_r_ref)), sems
    )
    rows, main = out_ref.shape
    tail = ends_ref.shape[1]
    line = lax.broadcasted_iota(jnp.int32, (rows, rows), 0)
    column = lax.broadcasted_iota(jnp.int32, (rows, rows), 1)
    long = up_ref.shape[0]
    rest = main - long
    ends = ends_ref[...]
    gate_pre = jnp.dot(
        arrived_ref[...], gate_ref[:main, :], preferred_element_type=jnp.float32
    ) + jnp.dot(ends, gate_ref[main:, :], preferred_element_type=jnp.float32)
    up_pre = jnp.dot(arrived_ref[:, :long], up_ref[...], preferred_element_type=jnp.float32)
    ready("more")
    up_pre = (
        up_pre
        + jnp.dot(arrived_ref[:, long:], more_ref[:rest, :], preferred_element_type=jnp.float32)
        + jnp.dot(ends, more_ref[rest:, :], preferred_element_type=jnp.float32)
    )
    active = activation(gate_pre, up_pre)
    ready("down")
    cut = down_l_ref.shape[0]

    def result_of(piece):
        at = lanes_of(piece, tail)
        product = jnp.dot(
            active[:, :cut], down_l_ref[:, at], preferred_element_type=jnp.float32
        ) + jnp.dot(active[:, cut:], down_r_ref[:, at], preferred_element_type=jnp.float32)
        return total_ref[:, at] + product.astype(jnp.bfloat16).astype(jnp.float32)

    last = result_of(GROUP - 1).astype(jnp.bfloat16)
    group_end = lax.broadcasted_iota(jnp.int32, (rows, tail), 0) % GROUP == GROUP - 1
    for s in range(GROUP - 1):
        pick = jnp.where(
            (line % GROUP == GROUP - 1) & (column == line - (GROUP - 1) + s), 1.0, 0.0
        ).astype(jnp.bfloat16)
        moved = jnp.dot(pick, last, preferred_element_type=jnp.float32)
        out_ref[:, lanes_of(s, tail)] = jnp.where(group_end, moved, result_of(s)).astype(
            jnp.bfloat16
        )


def combine_body(returned_ref, hidden_ref, routes_ref, weights_ref, out_ref):
    rows, model_width = hidden_ref.shape
    total_rows, main = returned_ref.shape
    tail = model_width - main
    column = lax.broadcasted_iota(jnp.int32, (rows, total_rows), 1)
    named = jnp.zeros((rows, total_rows), jnp.float32)
    weight = jnp.zeros((rows, total_rows), jnp.float32)
    for k in range(routes_ref.shape[1]):
        here = routes_ref[:, k : k + 1] == column // GROUP
        named = jnp.where(here, 1.0, named)
        weight = jnp.where(here, weights_ref[:, k : k + 1], weight)
    before = (
        lax.broadcasted_iota(jnp.int32, (rows, rows), 1)
        < lax.broadcasted_iota(jnp.int32, (rows, rows), 0)
    ).astype(jnp.bfloat16)
    rank = jnp.dot(
        before, named.astype(jnp.bfloat16), preferred_element_type=jnp.float32
    ).astype(jnp.int32)
    parts = []
    rest = weight
    for _ in range(3):
        top = rest.astype(jnp.bfloat16).astype(jnp.float32)
        rest = rest - top
        parts.append(top)

    def gathered(keep, values):
        table = jnp.concatenate([jnp.where(keep, p, 0.0) for p in parts], axis=0)
        got = jnp.dot(table.astype(jnp.bfloat16), values, preferred_element_type=jnp.float32)
        return got[:rows] + (got[rows : 2 * rows] + got[2 * rows :])

    own = (named > 0) & (rank == column % GROUP)
    out_ref[:, :main] = (
        hidden_ref[:, :main].astype(jnp.float32) + gathered(own, returned_ref[...])
    ).astype(jnp.bfloat16)
    ends = jnp.zeros((rows, tail), jnp.float32)
    for s in range(GROUP - 1):
        keep = (named > 0) & (rank == s) & (column % GROUP == GROUP - 1)
        ends = ends + gathered(keep, returned_ref[:, lanes_of(s, tail)])
    out_ref[:, main:] = (hidden_ref[:, main:].astype(jnp.float32) + ends).astype(jnp.bfloat16)


def on_device(
    query_plain,
    query_turn,
    latent,
    key_turn,
    latent_norm_scale,
    plain_key_matrix,
    value_matrix,
    residual,
    out_weight,
    ffn_gain,
    gate_weight,
    up_weight,
    down_weight,
    routes,
    route_weights,
):
    tok_dev = latent.shape[0]
    rows_dev = residual.shape[0]
    model_width = residual.shape[1]
    latent_width = latent.shape[1]
    group = lax.axis_size("tp")
    heads_dev = query_plain.shape[1] // PLAIN_HEAD_WIDTH
    place = lax.axis_index(SP) * tok_dev + jnp.arange(tok_dev, dtype=jnp.int32)
    at_tp = lax.axis_index("tp")
    at_core = lax.axis_index("sp_1")
    own_place = (
        lax.axis_index(SP) * tok_dev
        + at_tp * rows_dev
        + jnp.arange(rows_dev, dtype=jnp.int32)
    )
    own_cos, own_sin = turn_tables(own_place, 1)
    cosines, sines = turn_tables(place, heads_dev)
    share_rows = latent_width // 2 + tok_dev // 2 + tok_dev * query_turn.shape[1] // latent_width
    wide = plain_key_matrix.shape[1]
    whole = lambda *shape: pl.BlockSpec(shape, lambda i, at: (0,) * len(shape))
    sent, shares = pl.pallas_call(
        prepare_body,
        out_shape=(
            jax.ShapeDtypeStruct((rows_dev, latent_width + 2 * QK_ROPE), jnp.bfloat16),
            jax.ShapeDtypeStruct((group, share_rows, latent_width), jnp.bfloat16),
        ),
        grid_spec=pltpu.PrefetchScalarGridSpec(
            num_scalar_prefetch=1,
            grid=(1,),
            in_specs=[
                pl.BlockSpec((rows_dev, latent_width), lambda i, at: (at[0], 0)),
                whole(latent_width),
                whole(QK_ROPE, tok_dev),
                whole(rows_dev, QK_ROPE),
                whole(rows_dev, QK_ROPE),
                whole(QK_ROPE, QK_ROPE),
                whole(latent_width, wide),
                whole(latent_width, wide),
                whole(tok_dev, query_plain.shape[1]),
                whole(tok_dev, query_turn.shape[1]),
            ],
            out_specs=(
                whole(rows_dev, latent_width + 2 * QK_ROPE),
                whole(group, share_rows, latent_width),
            ),
        ),
        compiler_params=pltpu.CompilerParams(vmem_limit_bytes=16 << 20),
        name="prepare",
    )(
        jnp.stack((at_tp, at_core)),
        *map(
            in_hbm,
            (
                latent,
                latent_norm_scale,
                key_turn.T,
                own_cos,
                own_sin,
                jnp.asarray(partner_matrix(QK_ROPE), jnp.bfloat16),
                plain_key_matrix,
                value_matrix,
                query_plain,
                query_turn,
            ),
        ),
    )
    shares = lax.all_to_all(shares, "tp", 0, 0, tiled=True)
    theirs = shifted(shares, "sp_1", 1)
    near = lax.all_gather(sent, "sp_0", axis=0, tiled=True)
    other = shifted(near, "sp_1", 1)

    parts = pl.pallas_call(
        attend_body,
        out_shape=pltpu.HBM(
            (group, rows_dev, group * heads_dev * VALUE_WIDTH + STAT_LANES), jnp.bfloat16
        ),
        in_specs=[pl.BlockSpec(memory_space=pltpu.SMEM)]
        + [pl.BlockSpec(memory_space=pltpu.VMEM)] * 7,
        scratch_shapes=[
            pltpu.VMEM((heads_dev, 2 * near.shape[0], PLAIN_HEAD_WIDTH + 2 * QK_ROPE), jnp.bfloat16),
            pltpu.VMEM((2 * near.shape[0], heads_dev * VALUE_WIDTH), jnp.bfloat16),
        ],
        compiler_params=pltpu.CompilerParams(vmem_limit_bytes=24 << 20),
        name="attend",
    )(
        at_core.reshape(1),
        near,
        other,
        shares,
        theirs,
        in_hbm(cosines),
        in_hbm(sines),
        in_hbm(jnp.asarray(partner_matrix(heads_dev * QK_ROPE), jnp.bfloat16)),
    )
    gathered = lax.all_to_all(parts, "tp", 0, 0, tiled=True)

    experts_all = lax.axis_size(SP) * gate_weight.shape[0]
    top_count = routes.shape[1]
    capacity = min(rows_dev, max(2, rows_dev * top_count * 3 // (2 * experts_all)))
    assert capacity == GROUP - 1
    main = model_width * capacity // GROUP
    vmem = pl.BlockSpec(memory_space=pltpu.VMEM)
    hbm = pl.BlockSpec(memory_space=pltpu.HBM)
    half_wide = out_weight.shape[0] // 2
    (weight_near,) = staged((out_weight,), half_wide)
    hidden, outgoing = pl.pallas_call(
        mix_body,
        out_shape=(
            jax.ShapeDtypeStruct((rows_dev, model_width), jnp.bfloat16),
            pltpu.HBM((experts_all * GROUP, main), jnp.bfloat16),
        ),
        in_specs=[vmem, vmem, hbm, vmem, vmem, vmem],
        scratch_shapes=[
            pltpu.VMEM((half_wide, model_width), jnp.bfloat16),
            pltpu.SemaphoreType.DMA((4,)),
        ],
        compiler_params=pltpu.CompilerParams(vmem_limit_bytes=16 << 20),
        name="mix",
    )(
        gathered,
        weight_near,
        in_hbm(out_weight),
        in_hbm(residual),
        in_hbm(ffn_gain),
        in_hbm(routes.T),
    )
    arrived = lax.all_to_all(outgoing.reshape(experts_all, GROUP, main), SP, 0, 0, tiled=True)

    gate_own, up_own, down_own = gate_weight[0], up_weight[0], down_weight[0]
    long = model_width * 11 // 16
    names = ("gate", "up", "more", "down")
    left, right = {}, {}
    for name, w in zip(names, (gate_own, up_own[:long], up_own[long:], down_own)):
        left[name] = shifted(w, "tp", 1)
        right[name] = shifted(w, "tp", -1)
    cut = down_own.shape[0] // 2
    far_gate = shifted(left["gate"], "tp", 1)
    far_up = shifted(right["up"], "tp", -1)
    far_more = shifted(right["more"], "tp", -1)
    far_down_l = shifted(left["down"][:cut], "tp", 1)
    far_down_r = shifted(right["down"][cut:], "tp", -1)
    arrived_rows = arrived.reshape(experts_all * GROUP, main)
    near_weights = [gate_own, up_own, down_own]
    for side in (left, right):
        near_weights += [side["gate"], side["up"], side["more"], side["down"]]
    total, ends = pl.pallas_call(
        near_body,
        out_shape=(
            pltpu.VMEM((experts_all * GROUP, model_width), jnp.float32),
            pltpu.VMEM((experts_all * GROUP, model_width - main), jnp.bfloat16),
        ),
        in_specs=[vmem] + [hbm] * len(near_weights),
        out_specs=(vmem, vmem),
        scratch_shapes=[
            pltpu.VMEM((group - 1, 2) + gate_own.shape, jnp.bfloat16),
            pltpu.VMEM((group - 1,) + down_own.shape, jnp.bfloat16),
            pltpu.SemaphoreType.DMA((len(near_weights),)),
        ],
        compiler_params=pltpu.CompilerParams(vmem_limit_bytes=32 << 20),
        name="near_quarters",
    )(arrived_rows, *map(in_hbm, near_weights))
    result_rows = pl.pallas_call(
        far_body,
        out_shape=pltpu.HBM((experts_all * GROUP, main), jnp.bfloat16),
        in_specs=[vmem] * 6 + [hbm] * 2,
        scratch_shapes=[
            pltpu.VMEM(far_more.shape, jnp.bfloat16),
            pltpu.VMEM(far_down_r.shape, jnp.bfloat16),
            pltpu.SemaphoreType.DMA((2,)),
        ],
        compiler_params=pltpu.CompilerParams(vmem_limit_bytes=24 << 20),
        name="far_quarter",
    )(
        arrived_rows,
        ends,
        total,
        *map(in_vmem, (far_gate, far_up, far_down_l)),
        *map(in_hbm, (far_more, far_down_r)),
    )
    returned = lax.all_to_all(result_rows.reshape(experts_all, GROUP, main), SP, 0, 0, tiled=True)
    return pl.pallas_call(
        combine_body,
        out_shape=jax.ShapeDtypeStruct((rows_dev, model_width), jnp.bfloat16),
        compiler_params=pltpu.CompilerParams(vmem_limit_bytes=16 << 20),
        name="combine",
    )(returned.reshape(experts_all * GROUP, main), hidden, in_hbm(routes), in_hbm(route_weights))


def solution(mesh):
    torus = Mesh(
        mesh.devices.reshape(mesh.shape["grp"], 16, 2, mesh.shape["tp"]),
        ("grp", "sp_0", "sp_1", "tp"),
    )
    placed = (
        P(GRP_SP, "tp"),
        P(GRP_SP, "tp"),
        P(GRP_SP, None),
        P(GRP_SP, None),
        P(),
        P(None, "tp"),
        P(None, "tp"),
        P(GRP_SP_TP, None),
        P(),
        P(),
        P(SP, None, "tp"),
        P(SP, None, "tp"),
        P(SP, "tp", None),
        P(GRP_SP_TP, None),
        P(GRP_SP_TP, None),
    )
    return jax.shard_map(
        on_device, mesh=torus, in_specs=placed, out_specs=P(GRP_SP_TP, None), check_vma=False
    )
```
